32 devices in a mesh: sp: 16 (over z, y, core), tp: 2 (over x).
Axes of the slice: x: 2, y: 2, z: 4, core: 2. Of those that a mesh axis runs over, the one named last changes fastest.
Arguments:
- tokens: bfloat16 [16384, 2048], P('sp'), may hold values from -6 to 6
- norm_gain: float32 [2048], replicated, may hold values from 0.1 to 1.9
- w_query: bfloat16 [2048, 512], P(None, 'tp'), may hold values from -0.79549513 to 0.79549513
- w_key: bfloat16 [2048, 128], P('sp'), may hold values from -0.79549513 to 0.79549513
- w_value: bfloat16 [2048, 128], P('sp'), may hold values from -0.125 to 0.125
- w_pool_in: bfloat16 [2048, 512], P(None, 'tp'), may hold values from -0.125 to 0.125
- sink_logit: float32 [8], P('tp'), may hold values from 3 to 7
- pool_scale: float32 [512], P('tp'), may hold values from 0.05 to 0.5
- w_out: bfloat16 [1024, 2048], P('tp', 'sp'), may hold values from -0.75 to 0.75
Outputs:
- mixed_out: bfloat16 [16384, 2048], P(('sp', 'tp'))
The draws below stay inside these ranges and needn't reach their ends.
All inputs are finite; a program needn't handle non-finite values.
Results may differ from the reference program's by a relative error of at most 0.03.
The reference program's roundings to bfloat16 on the way (of `normed`, `query`, `key`, `value`, `pool_in`, `weights`, `attended` and `pooled`) count: a program that leaves them out, or rounds other values in their place, can miss the bound.
Values may be sent and summed in bfloat16 or wider, within the bound.
A program may use at most 64 MiB of HBM per device.

```python
import math
import jax
import jax.numpy as jnp
from jax import lax

D = 2048
HEAD = 64
QH = 8
KVH = 2
POOL_CH = 128
POOL_W = 512
WINDOW = 128
QB = 128
SEQ = 16384


def projection_draw(key, shape):
    values = jax.random.truncated_normal(key, -6.0, 6.0, shape, jnp.float32) * D ** (-0.5)
    return values.astype(jnp.bfloat16)


def draw_w_query(key, part):
    return projection_draw(jax.random.fold_in(key, 11), (D, QH * HEAD))


def draw_w_key(key, part):
    return projection_draw(jax.random.fold_in(key, 23), (D, KVH * HEAD))


def level_of(key, dims, pieces, smallest, top_value):
    level = 1.0
    for dim, parts in pieces:
        steps = jax.random.uniform(jax.random.fold_in(jax.random.fold_in(key, 6), dim), (parts,), jnp.float32, smallest / len(pieces), top_value / len(pieces))
        level = level * jnp.repeat(jnp.exp(steps), dims[dim] // parts).reshape((-1,) + (1,) * (len(dims) - 1 - dim))
    return level


def centred(rng, dims, scale, reach, pieces=(), kind=jnp.bfloat16):
    entries = scale * jax.random.normal(rng, dims, jnp.float32)
    if pieces:
        entries = entries * level_of(rng, dims, pieces, -0.22, 0.18)
    return jnp.clip(entries, -reach, reach).astype(kind)


def setup_inputs(seed: int = 0) -> dict:
    seeds = jax.random.split(jax.random.key(seed), 10)
    tokens = centred(seeds[0], (SEQ, D), 1.0, 6.0, ((0, 16),))
    norm_gain = jnp.clip(1.0 + 0.18 * jax.random.normal(seeds[1], (D,), jnp.float32), 0.1, 1.9)
    w_query = draw_w_query(jax.random.fold_in(seeds[9], 71), 0)
    w_key = draw_w_key(jax.random.fold_in(seeds[9], 71), 0)
    w_value = centred(seeds[4], (D, KVH * HEAD), D ** -0.5, 0.125, ((0, 16),))
    w_pool_in = centred(seeds[5], (D, POOL_W), D ** -0.5, 0.125, ((1, 2),))
    sink_logit = jnp.clip(3.0 + 4.0 * jax.random.uniform(seeds[6], (QH,), jnp.float32) ** level_of(seeds[6], (QH,), ((0, 2),), -0.2, 0.2), 3.0, 7.0)
    pool_scale = jnp.clip(jnp.exp(math.log(0.5) - 2.3025851 * jax.random.uniform(seeds[7], (POOL_W,), jnp.float32) ** level_of(seeds[7], (POOL_W,), ((0, 2),), -0.2, 0.2)), 0.05, 0.5)
    w_out = centred(seeds[8], (QH * HEAD + POOL_W, D), (4.0 * (QH * HEAD + POOL_W) ** -0.5), 0.75, ((0, 2), (1, 16)))
    return {"tokens": tokens, "norm_gain": norm_gain, "w_query": w_query, "w_key": w_key, "w_value": w_value, "w_pool_in": w_pool_in, "sink_logit": sink_logit, "pool_scale": pool_scale, "w_out": w_out}


NEG_BIG = -1e+30
POOL_SPANS = (2, 4, 8, 16)

def layer_normed(tokens, norm_gain):
    values = tokens.astype(jnp.float32)
    center = lax.optimization_barrier(jnp.mean(values, axis=-1, keepdims=True))
    spread = lax.optimization_barrier(jnp.mean(jnp.square(values - center), axis=-1, keepdims=True))
    return ((values - center) * lax.rsqrt(spread + 1e-06) * norm_gain).astype(jnp.bfloat16)

def rotate(values, positions):
    half = HEAD // 2
    inverse = 10000.0 ** (-jnp.arange(half, dtype=jnp.float32) / half)
    angles = positions[:, None] * inverse[None, :]
    cosine = jnp.cos(angles)[:, None, :]
    sine = jnp.sin(angles)[:, None, :]
    first = values[..., :half]
    second = values[..., half:]
    return jnp.concatenate([first * cosine - second * sine, first * sine + second * cosine], axis=-1)

def reference(tokens, norm_gain, w_query, w_key, w_value, w_pool_in, sink_logit, pool_scale, w_out):
    length = tokens.shape[0]
    group = QH // KVH
    normed = layer_normed(tokens, norm_gain)
    positions = jnp.arange(length).astype(jnp.float32)
    query = rotate(jnp.dot(normed, w_query, preferred_element_type=jnp.float32).reshape(length, QH, HEAD), positions).astype(jnp.bfloat16)
    key = rotate(jnp.dot(normed, w_key, preferred_element_type=jnp.float32).reshape(length, KVH, HEAD), positions).astype(jnp.bfloat16)
    value = jnp.dot(normed, w_value, preferred_element_type=jnp.float32).astype(jnp.bfloat16).reshape(length, KVH, HEAD)
    pool_in = jnp.dot(normed, w_pool_in, preferred_element_type=jnp.float32).astype(jnp.bfloat16)
    key_padded = jnp.pad(key, ((WINDOW, WINDOW), (0, 0), (0, 0)))
    value_padded = jnp.pad(value, ((WINDOW, WINDOW), (0, 0), (0, 0)))
    span = QB + 2 * WINDOW
    sink_grid = sink_logit.reshape(KVH, group)[:, :, None, None]

    def attend(start):
        queries = lax.dynamic_slice_in_dim(query, start, QB, 0).reshape(QB, KVH, group, HEAD)
        keys = lax.dynamic_slice_in_dim(key_padded, start, span, 0)
        values = lax.dynamic_slice_in_dim(value_padded, start, span, 0)
        scores = jnp.einsum('ikgd,jkd->kgij', queries.astype(jnp.float32), keys.astype(jnp.float32)) * HEAD ** (-0.5)
        query_pos = start + jnp.arange(QB).astype(jnp.int32)
        key_pos = start - WINDOW + jnp.arange(span).astype(jnp.int32)
        valid = (jnp.abs(query_pos[:, None] - key_pos[None, :]) <= WINDOW) & (key_pos[None, :] >= 0) & (key_pos[None, :] < length)
        scores = jnp.where(valid, scores, NEG_BIG)
        highest = jnp.maximum(lax.optimization_barrier(jnp.max(scores, axis=-1, keepdims=True)), sink_grid)
        expo = jnp.where(valid, jnp.exp(scores - highest), 0.0)
        total = lax.optimization_barrier(jnp.sum(expo, axis=-1, keepdims=True)) + jnp.exp(sink_grid - highest)
        weights = (expo / total).astype(jnp.bfloat16)
        result = jnp.einsum('kgij,jkd->ikgd', weights.astype(jnp.float32), values.astype(jnp.float32))
        return result.reshape(QB, QH * HEAD).astype(jnp.bfloat16)
    starts = (jnp.arange(length // QB) * QB).astype(jnp.int32)
    attended = lax.map(attend, starts).reshape(length, QH * HEAD)
    pool_vals = pool_in.astype(jnp.float32)
    running = jnp.pad(jnp.cumsum(pool_vals, axis=0), ((1, 0), (0, 0)))
    where_at = jnp.arange(length).astype(jnp.int32)
    means = []
    for index, width in enumerate(POOL_SPANS):
        lower = jnp.clip(where_at - width // 2, 0, length)
        upper = jnp.clip(where_at + width // 2, 0, length)
        block = running[:, index * POOL_CH:(index + 1) * POOL_CH]
        means.append((block[upper] - block[lower]) / (upper - lower).astype(jnp.float32)[:, None])
    pooled = ((jnp.concatenate(means, axis=1) - pool_vals) * pool_scale).astype(jnp.bfloat16)
    joined = jnp.concatenate([attended, pooled], axis=1)
    return jnp.dot(joined, w_out, preferred_element_type=jnp.float32).astype(jnp.bfloat16)
```

```python
import functools

import jax
import jax.numpy as jnp
import numpy as np
from jax import lax
from jax.experimental import pallas as pl
from jax.experimental.pallas import tpu as pltpu
from jax.sharding import PartitionSpec as P

HEAD = 64
QH = 8
KVH = 2
POOL_CH = 128
WINDOW = 128
QB = 128


NEG_BIG = -1e30
POOL_SPANS = (2, 4, 8, 16)


def extended(block, sides, width):
    for axis, dim in sides:
        count = lax.axis_size(axis)
        forward = [(i, i + 1) for i in range(count - 1)]
        backward = [(target, source) for source, target in forward]
        low = lax.ppermute(
            lax.slice_in_dim(block, block.shape[dim] - width, None, axis=dim), axis, forward
        )
        high = lax.ppermute(lax.slice_in_dim(block, 0, width, axis=dim), axis, backward)
        block = jnp.concatenate([low, block, high], axis=dim)
    return block


def layer_normed(tokens, norm_gain):
    values = tokens.astype(jnp.float32)
    center = jnp.mean(values, axis=-1, keepdims=True)
    spread = jnp.mean(jnp.square(values - center), axis=-1, keepdims=True)
    return ((values - center) * lax.rsqrt(spread + 1e-06) * norm_gain).astype(jnp.bfloat16)


def rotate(values, positions):
    half = HEAD // 2
    inverse = 10000.0 ** (-jnp.arange(half, dtype=jnp.float32) / half)
    angles = positions[:, None] * inverse[None, :]
    cosine = jnp.cos(angles)[:, None, :]
    sine = jnp.sin(angles)[:, None, :]
    first = values[..., :half]
    second = values[..., half:]
    return jnp.concatenate(
        [first * cosine - second * sine, first * sine + second * cosine], axis=-1
    )


def plain_body(tokens, norm_gain, w_query, w_key, w_value, w_pool_in, sink_logit, pool_scale, w_out):
    local_rows = tokens.shape[0]
    seq_total = local_rows * lax.axis_size("sp")
    offset = lax.axis_index("sp") * local_rows
    tp_place = lax.axis_index("tp")
    local_heads = w_query.shape[1] // HEAD
    local_pool = w_pool_in.shape[1]
    reach = POOL_SPANS[-1] // 2
    normed = layer_normed(tokens, norm_gain)
    positions = (offset + jnp.arange(local_rows)).astype(jnp.float32)
    query = rotate(
        jnp.dot(normed, w_query, preferred_element_type=jnp.float32).reshape(
            local_rows, local_heads, HEAD
        ),
        positions,
    ).astype(jnp.bfloat16)
    key_head = tp_place * local_heads // (QH // KVH)
    key_cols = lax.dynamic_slice_in_dim(w_key, key_head * HEAD, HEAD, 1)
    value_cols = lax.dynamic_slice_in_dim(w_value, key_head * HEAD, HEAD, 1)
    key_sum = jnp.dot(
        normed,
        lax.all_gather(key_cols, "sp", axis=0, tiled=True),
        preferred_element_type=jnp.float32,
    )
    value_sum = jnp.dot(
        normed,
        lax.all_gather(value_cols, "sp", axis=0, tiled=True),
        preferred_element_type=jnp.float32,
    )
    key = rotate(key_sum[:, None, :], positions)[:, 0, :].astype(jnp.bfloat16)
    value = value_sum.astype(jnp.bfloat16)
    key_value = jnp.concatenate([key, value], axis=1)
    pool_in = jnp.dot(normed, w_pool_in, preferred_element_type=jnp.float32).astype(jnp.bfloat16)
    widened = extended(jnp.concatenate([key_value, pool_in], axis=1), (("sp", 0),), WINDOW)
    kv_wide = widened[:, : 2 * HEAD]
    pool_wide = widened[WINDOW - reach : WINDOW + local_rows + reach, 2 * HEAD :]
    span = QB + 2 * WINDOW
    sink_here = sink_logit[:, None, None]
    results = []
    for block in range(local_rows // QB):
        queries = query[block * QB : (block + 1) * QB]
        keys = kv_wide[block * QB : block * QB + span, :HEAD]
        values = kv_wide[block * QB : block * QB + span, HEAD:]
        scores = jnp.einsum(
            "ihd,jd->hij", queries, keys, preferred_element_type=jnp.float32
        ) * HEAD ** (-0.5)
        query_pos = offset + block * QB + jnp.arange(QB)
        key_pos = offset + block * QB - WINDOW + jnp.arange(span)
        valid = (
            (jnp.abs(query_pos[:, None] - key_pos[None, :]) <= WINDOW)
            & (key_pos[None, :] >= 0)
            & (key_pos[None, :] < seq_total)
        )
        scores = jnp.where(valid, scores, NEG_BIG)
        highest = jnp.maximum(jnp.max(scores, axis=-1, keepdims=True), sink_here)
        expo = jnp.where(valid, jnp.exp(scores - highest), 0.0)
        total = jnp.sum(expo, axis=-1, keepdims=True) + jnp.exp(sink_here - highest)
        weights = (expo / total).astype(jnp.bfloat16)
        result = jnp.einsum("hij,jd->ihd", weights, values, preferred_element_type=jnp.float32)
        results.append(result.reshape(QB, local_heads * HEAD).astype(jnp.bfloat16))
    attended = jnp.concatenate(results, axis=0)
    pool_vals = pool_wide.astype(jnp.float32)
    window_sum = pool_vals
    global_pos = offset + jnp.arange(local_rows)
    channel = tp_place * local_pool + jnp.arange(local_pool)
    window_group = channel // POOL_CH
    measured = jnp.zeros((local_rows, local_pool), jnp.float32)
    stride = 1
    for index, width in enumerate(POOL_SPANS):
        window_sum = window_sum[:-stride] + window_sum[stride:]
        stride = width
        sums = window_sum[reach - width // 2 : reach - width // 2 + local_rows]
        counted = (
            jnp.minimum(global_pos + width // 2, seq_total)
            - jnp.maximum(global_pos - width // 2, 0)
        ).astype(jnp.float32)
        measured = measured + jnp.where(
            window_group[None, :] == index, sums / counted[:, None], 0.0
        )
    pooled = ((measured - pool_vals[reach : reach + local_rows]) * pool_scale).astype(jnp.bfloat16)
    attended_rows, pooled_rows = (
        lax.all_to_all(attended, "tp", split_axis=0, concat_axis=1, tiled=True),
        lax.all_to_all(pooled, "tp", split_axis=0, concat_axis=1, tiled=True),
    )
    joined = jnp.concatenate([attended_rows, pooled_rows], axis=1)
    out_rows_all = lax.all_gather(w_out, "tp", axis=0, tiled=True)
    projected = jnp.dot(
        joined,
        lax.all_gather(out_rows_all, "sp", axis=1, tiled=True),
        preferred_element_type=jnp.float32,
    )
    return projected.astype(jnp.bfloat16)


LANES = 128
CHUNK = 256
VMEM_LIMIT = 60 * 1024 * 1024
MESH = pl.DeviceIdType.MESH


def rope_tables(rows_total):
    half = HEAD // 2
    inverse = np.tile(10000.0 ** (-np.arange(half, dtype=np.float64) / half), LANES // half)[None, :]
    sign = np.where(np.arange(LANES) % HEAD < half, -1.0, 1.0)[None, :]
    inner = np.arange(QB, dtype=np.float64)[:, None] * inverse
    starts = (QB * np.arange(rows_total // QB, dtype=np.float64))[:, None] * inverse
    tables = (np.cos(inner), np.sin(inner) * sign, np.cos(starts), np.sin(starts) * sign)
    return [jnp.asarray(table.astype(np.float32)) for table in tables]


def mixer_kernel(
    places, tokens, gain, w_query, w_key, w_value, w_pool, sink, scale, w_out, cos_in, sin_in, cos_all, sin_all,
    out,
    tok, normed, wq, wp, kv_in, kvw, wfull, qs, kv, pool, pool_send, att_send, joined, acc, cos_at, sin_at,
    tok_sem, own_sem, kv_recv, kz_send, ko_send, kf_send, ky_send,
    wo_recv, wz_send, wo_send, wx_send, wd_send, w00_send, w10_send, w01_send, w11_send,
    halo_send, halo_recv, exp_send, exp_recv, exa_send, exa_recv,
):
    S, T = places
    Z = S // 4
    s = lax.axis_index("sp")
    t = lax.axis_index("tp")
    rows = tokens.shape[0]
    width = tokens.shape[1]
    blocks = rows // QB
    hb = blocks // 2
    chunks = rows // CHUNK
    local_heads = w_query.shape[1] // HEAD
    groups = w_query.shape[1] // LANES
    pgroups = w_pool.shape[1] // LANES
    reach = POOL_SPANS[-1] // 2
    offset = s * rows
    total_rows = S * rows
    c = s % 2
    y = (s // 2) % 2
    z = s // 4
    partner = s + 1 - 2 * c
    yflip = s + 2 - 4 * y
    after = (s + 1) % S
    before = (s + S - 1) % S
    cross = 1 - t
    far = [d for k in range(1, Z) for d in (k, -k)]

    def remote(a, b, send, recv, to_s, to_t):
        return pltpu.make_async_remote_copy(
            src_ref=a, dst_ref=b, send_sem=send, recv_sem=recv,
            device_id={"sp": to_s, "tp": to_t}, device_id_type=MESH,
        )

    tok_copies = [
        pltpu.make_async_copy(
            tokens.at[pl.ds(i * CHUNK, CHUNK)], tok.at[pl.ds(i * CHUNK, CHUNK)], tok_sem.at[i]
        )
        for i in range(chunks)
    ]
    own_copies = [
        pltpu.make_async_copy(w_key, kv_in.at[0], own_sem.at[0]),
        pltpu.make_async_copy(w_value, kv_in.at[1], own_sem.at[1]),
        pltpu.make_async_copy(w_out, wfull.at[s, t], own_sem.at[2]),
        pltpu.make_async_copy(w_query, wq, own_sem.at[3]),
        pltpu.make_async_copy(w_pool, wp, own_sem.at[4]),
        pltpu.make_async_copy(cos_all.at[pl.ds(pl.multiple_of(s * blocks, blocks), blocks)], cos_at, own_sem.at[5]),
        pltpu.make_async_copy(sin_all.at[pl.ds(pl.multiple_of(s * blocks, blocks), blocks)], sin_at, own_sem.at[6]),
    ]
    barrier = pltpu.get_barrier_semaphore()
    greet = [(((z + d) % Z) * 4 + s % 4, t) for d in range(1, Z)]
    greet += [(yflip, t), (after, t), (before, t), (s, cross)]
    for to_s, to_t in greet:
        pl.semaphore_signal(barrier, inc=1, device_id={"sp": to_s, "tp": to_t}, device_id_type=MESH)
    for copy in own_copies[:3]:
        copy.start()
    tok_copies[0].start()
    for copy in own_copies[3:]:
        copy.start()
    for copy in tok_copies[1:]:
        copy.start()

    lane = lax.broadcasted_iota(jnp.int32, (QB, LANES), 1)
    low_half = lane < HEAD
    first_half = lane % HEAD < HEAD // 2

    own_copies[0].wait()
    own_copies[1].wait()
    key_head = t * local_heads // (QH // KVH)
    key_in = kv_in[0].astype(jnp.float32)
    value_in = kv_in[1].astype(jnp.float32)
    key_cols = jnp.where(key_head == 0, key_in, pltpu.roll(key_in, HEAD, 1))
    value_cols = jnp.where(key_head == 0, pltpu.roll(value_in, HEAD, 1), value_in)
    kvw[s] = jnp.where(low_half, key_cols, value_cols).astype(jnp.bfloat16)
    own_copies[2].wait()
    pl.semaphore_wait(barrier, len(greet))

    pending = []

    def go(cond, make):
        pending.append((cond, make))
        if cond is None:
            make().start()
        else:
            @pl.when(cond)
            def _():
                make().start()

    def later(cond, make):
        pending.append((cond, make))

    def here(d):
        return (z + d >= 0) & (z + d < Z)

    def piece_kv(b):
        return kvw.at[b]

    def piece_wo(b, half):
        return wfull.at[b, half]

    def kv_copy(b, send, to):
        return lambda: remote(kvw.at[b], kvw.at[b], send, kv_recv.at[b], to, t)

    def wo_copy(b, half, send, to_s, to_t):
        return lambda: remote(wfull.at[b, half], wfull.at[b, half], send, wo_recv.at[b, half], to_s, to_t)

    hop = [1, -1, 2, -2]

    def at_z(d):
        return s + 4 * d

    def at_yz(d):
        return yflip + 4 * d

    def reach_index(d):
        return far.index(d)

    def start_all(items):
        for cond, make in items:
            if cond is None:
                make().start()
            else:
                @pl.when(cond)
                def _(make=make):
                    make().start()

    def event(cond, arrival, items):
        pending.extend([(cond if k is None else (k if cond is None else cond & k), m) for k, m in items])

        def act():
            def inner():
                if arrival is not None:
                    arrival().wait_recv()
                start_all(items)
            if cond is None:
                inner()
            else:
                pl.when(cond)(inner)
        return act

    def onward(d):
        step = -1 if d > 0 else 1
        return step, here(step)

    ev = {}
    ev["kv_own"] = event(None, None,
        [(here(h), kv_copy(s, kz_send.at[i], at_z(h))) for i, h in enumerate(hop) if abs(h) < Z]
        + [(None, kv_copy(s, ko_send.at[0], yflip)), (None, kv_copy(s, ko_send.at[1], partner))])
    for i, d in enumerate(far):
        step, fine = onward(d)
        items = [(None, kv_copy(at_z(d), kf_send.at[i, 0], yflip)), (None, kv_copy(at_z(d), kf_send.at[i, 1], partner))]
        if 2 <= abs(d) < Z - 1:
            items = [(fine, kv_copy(at_z(d), kf_send.at[i, 2], at_z(step)))] + items
        ev["kv", d] = event(here(d), kv_copy(at_z(d), kf_send.at[i, 0], yflip), items)
    for i, d in enumerate([0] + far):
        ev["kvy", d] = event(None if d == 0 else here(d), kv_copy(at_yz(d), ky_send.at[i], partner),
            [(None, kv_copy(at_yz(d), ky_send.at[i], partner))])

    ev["wo_own"] = event(None, None,
        [(None, wo_copy(s, t, wo_send.at[0], s, cross)), (None, wo_copy(s, t, wo_send.at[1], yflip, t))]
        + [(here(h), wo_copy(s, t, wz_send.at[i], at_z(h), t)) for i, h in enumerate(hop) if abs(h) < Z]
        + [(None, wo_copy(s, t, wo_send.at[2], partner, t))])
    ev["wo_x"] = event(None, wo_copy(s, cross, wx_send.at[0], yflip, t),
        [(None, wo_copy(s, cross, wx_send.at[0], yflip, t)), (None, wo_copy(s, cross, wx_send.at[1], partner, t))])
    ev["wo_d"] = event(None, wo_copy(yflip, cross, wd_send.at[4], partner, t),
        [(here(h), wo_copy(yflip, cross, wd_send.at[i], at_z(h), t)) for i, h in enumerate(hop) if abs(h) < Z]
        + [(None, wo_copy(yflip, cross, wd_send.at[4], partner, t))])
    for i, d in enumerate(far):
        step, fine = onward(d)
        b = at_z(d)
        items = [(None, wo_copy(b, t, w00_send.at[i, 0], s, cross)), (None, wo_copy(b, t, w00_send.at[i, 1], yflip, t)),
                 (None, wo_copy(b, t, w00_send.at[i, 2], partner, t))]
        if 2 <= abs(d) < Z - 1:
            items = [(fine, wo_copy(b, t, w00_send.at[i, 3], at_z(step), t))] + items
        ev["w00", d] = event(here(d), wo_copy(b, t, w00_send.at[i, 0], s, cross), items)
        ev["w10", d] = event(here(d), wo_copy(b, cross, w10_send.at[i], partner, t),
            [(None, wo_copy(b, cross, w10_send.at[i], partner, t))])
        b = at_yz(d)
        items = [(None, wo_copy(b, cross, w11_send.at[i, 0], partner, t))]
        if 2 <= abs(d) < Z - 1:
            items = [(fine, wo_copy(b, cross, w11_send.at[i, 1], at_z(step), t))] + items
        ev["w11", d] = event(here(d), wo_copy(b, cross, w11_send.at[i, 0], partner, t), items)
    for i, d in enumerate([0] + far):
        b = at_yz(d)
        ev["w01", d] = event(None if d == 0 else here(d), wo_copy(b, t, w01_send.at[i], partner, t),
            [(None, wo_copy(b, t, w01_send.at[i], partner, t))])

    def poll(kind, *distances):
        for k in distances:
            for d in ((k, -k) if k else (0,)):
                if abs(d) < Z:
                    ev[kind, d]()

    ev["kv_own"]()
    ev["wo_own"]()

    def rotated(values, b):
        ca = cos_at[pl.ds(b, 1), :]
        sa = sin_at[pl.ds(b, 1), :]
        ci = cos_in[...]
        si = sin_in[...]
        cosine = ca * ci - sa * si
        sine = sa * ci + ca * si
        swapped = jnp.where(
            first_half,
            pltpu.roll(values, LANES - HEAD // 2, 1),
            pltpu.roll(values, HEAD // 2, 1),
        )
        return values * cosine + swapped * sine

    for copy in own_copies[3:]:
        copy.wait()
    LN = 32

    def project(i, carry):
        base = pl.multiple_of(i * CHUNK, CHUNK)
        pltpu.make_async_copy(
            tokens.at[pl.ds(base, CHUNK)], tok.at[pl.ds(base, CHUNK)], tok_sem.at[i]
        ).wait()

        def norm(r, carry):
            at = pl.multiple_of(base + r * LN, LN)
            values = tok[pl.ds(at, LN), :].astype(jnp.float32)
            center = jnp.sum(values, axis=1, keepdims=True) * (1.0 / width)
            moved = values - center
            spread = jnp.sum(moved * moved, axis=1, keepdims=True) * (1.0 / width)
            normed[pl.ds(at, LN), :] = (moved * lax.rsqrt(spread + 1e-06) * gain[...]).astype(
                jnp.bfloat16
            )
            return carry

        lax.fori_loop(0, CHUNK // LN, norm, 0, unroll=2)
        part = normed[pl.ds(base, CHUNK), :]
        query = jnp.dot(part, wq[...], preferred_element_type=jnp.float32)
        for k in range(CHUNK // QB):
            b = i * (CHUNK // QB) + k
            for g in range(groups):
                turned = rotated(query[k * QB:(k + 1) * QB, g * LANES:(g + 1) * LANES], b) * HEAD ** (-0.5)
                qs[b, pl.ds(2 * g * QB, QB), :] = jnp.where(low_half, turned, 0.0).astype(jnp.bfloat16)
                qs[b, pl.ds((2 * g + 1) * QB, QB), :] = jnp.where(
                    low_half, pltpu.roll(turned, HEAD, 1), 0.0
                ).astype(jnp.bfloat16)
        mixed = jnp.dot(part, wp[...], preferred_element_type=jnp.float32)
        pool[pl.ds(pl.multiple_of(reach + base, 8), CHUNK), :] = mixed.astype(jnp.bfloat16).astype(jnp.float32)


        @pl.when(i == 1)
        def _():
            poll("kv", 1)

        @pl.when(i == 2)
        def _():
            poll("kv", 2)
            poll("kvy", 0)
            ev["wo_x"]()

        @pl.when(i == 3)
        def _():
            poll("kv", *range(3, Z))
            poll("kvy", 1)
            poll("w00", 1)
        return carry

    lax.fori_loop(0, chunks, project, 0)

    inner = s < S - 1
    outer = s > 0
    halo_pool = [
        (inner, lambda: remote(pool.at[pl.ds(rows, reach)], pool.at[pl.ds(0, reach)], halo_send.at[0], halo_recv.at[0], after, t)),
        (outer, lambda: remote(pool.at[pl.ds(reach, reach)], pool.at[pl.ds(rows + reach, reach)], halo_send.at[1], halo_recv.at[1], before, t)),
    ]
    halo_kv = [
        (inner, lambda: remote(kv.at[pl.ds(rows, WINDOW)], kv.at[pl.ds(0, WINDOW)], halo_send.at[2], halo_recv.at[2], after, t)),
        (outer, lambda: remote(kv.at[pl.ds(WINDOW, WINDOW)], kv.at[pl.ds(rows + WINDOW, WINDOW)], halo_send.at[3], halo_recv.at[3], before, t)),
    ]
    pending.extend(halo_pool + halo_kv)

    def halo_wait(pair):
        @pl.when(outer)
        def _():
            pair[0][1]().wait_recv()

        @pl.when(inner)
        def _():
            pair[1][1]().wait_recv()

    start_all(halo_pool)

    @pl.when(s == 0)
    def _():
        pool[0:reach, :] = jnp.zeros((reach, pool.shape[1]), jnp.float32)
        kv[0:WINDOW, :] = jnp.zeros((WINDOW, LANES), jnp.bfloat16)

    @pl.when(s == S - 1)
    def _():
        pool[rows + reach:rows + 2 * reach, :] = jnp.zeros((reach, pool.shape[1]), jnp.float32)
        kv[rows + WINDOW:rows + 2 * WINDOW, :] = jnp.zeros((WINDOW, LANES), jnp.bfloat16)

    poll("kvy", *range(2, Z))
    own_core = [s] + [at_z(d) for d in far] + [yflip] + [at_yz(d) for d in far]
    arrives = [(None, partner), (None, yflip + partner - s)]
    arrives += [(here(d), partner + 4 * d) for d in far] + [(here(d), yflip + partner - s + 4 * d) for d in far]
    for cond, b in arrives:
        make = kv_copy(b, ko_send.at[1], partner)
        if cond is None:
            make().wait_recv()
        else:
            @pl.when(cond)
            def _(make=make):
                make().wait_recv()

    def key_value(j, carry):
        i = jnp.where(j == 0, 0, jnp.where(j == 1, chunks - 1, j - 1))
        base = pl.multiple_of(i * CHUNK, CHUNK)
        both = jnp.dot(
            normed[pl.ds(base, CHUNK), :], kvw[...].reshape(width, LANES), preferred_element_type=jnp.float32
        )
        for k in range(CHUNK // QB):
            piece = both[k * QB:(k + 1) * QB, :]
            turned = rotated(piece, i * (CHUNK // QB) + k)
            kv[pl.ds(pl.multiple_of(WINDOW + base + k * QB, QB), QB), :] = jnp.where(
                low_half, turned, piece
            ).astype(jnp.bfloat16)

        @pl.when(j == 0)
        def _():
            ev["wo_d"]()

        @pl.when(j == 2)
        def _():
            start_all(halo_kv)
            poll("w00", 2)
        return carry

    lax.fori_loop(0, chunks, key_value, 0)
    halo_wait(halo_pool)

    def pooled(b, g):
        cols = slice(g * LANES, (g + 1) * LANES)
        length = QB + 2 * reach
        values = pool[pl.ds(pl.multiple_of(b * QB, QB), length), cols]
        index = (t * (pgroups * LANES) + g * LANES) // POOL_CH
        running = values
        stride = 1
        picked = jnp.zeros((QB, LANES), jnp.float32)
        wide = 0
        for k, span in enumerate(POOL_SPANS):
            running = running + pltpu.roll(running, length - stride, 0)
            stride = span
            shift = reach - span // 2
            sums = (pltpu.roll(running, length - shift, 0) if shift else running)[:QB]
            picked = jnp.where(index == k, sums, picked)
            wide = jnp.where(index == k, span // 2, wide)
        pos = offset + b * QB + lax.broadcasted_iota(jnp.int32, (QB, LANES), 0)
        counted = (jnp.minimum(pos + wide, total_rows) - jnp.maximum(pos - wide, 0)).astype(jnp.float32)
        return ((picked / counted - values[reach:reach + QB]) * scale[:, cols]).astype(jnp.bfloat16)

    def pool_other(i, carry):
        for g in range(pgroups):
            pool_send[pl.ds(pl.multiple_of(i * QB, QB), QB), g * LANES:(g + 1) * LANES] = pooled(cross * hb + i, g)
        return carry

    def pool_own(i, carry):
        for g in range(pgroups):
            joined[T + t, pl.ds(pl.multiple_of(i * QB, QB), QB), g * LANES:(g + 1) * LANES] = pooled(t * hb + i, g)
        return carry


    ex_pool = (None, lambda: remote(pool_send, joined.at[T + t], exp_send.at[0], exp_recv.at[0], s, cross))
    pending.append(ex_pool)

    def ex_att(n):
        at = pl.ds(pl.multiple_of(n * QB, QB), QB)
        return remote(att_send.at[at], joined.at[t, at], exa_send.at[n], exa_recv.at[n], s, cross)

    lax.fori_loop(0, hb, pool_other, 0)
    ex_pool[1]().start()
    poll("w00", *range(3, Z))
    lax.fori_loop(0, hb, pool_own, 0)
    poll("w10", 1)
    poll("w01", 0, 1)

    span = QB + 2 * WINDOW
    row_id = lax.broadcasted_iota(jnp.int32, (QB, span), 0)
    col_id = lax.broadcasted_iota(jnp.int32, (QB, span), 1)

    def attend(b):
        context = kv[pl.ds(pl.multiple_of(b * QB, QB), span), :]
        scores = lax.dot_general(
            qs[b], context, (((1,), (1,)), ((), ())), preferred_element_type=jnp.float32
        )
        start = offset + b * QB
        lowest = jnp.maximum(row_id, WINDOW - start)
        highest_col = jnp.minimum(row_id + 2 * WINDOW, total_rows - 1 - start + WINDOW)
        valid = (col_id >= lowest) & (col_id <= highest_col)
        expos = []
        norms = []
        for h in range(local_heads):
            part = jnp.where(valid, scores[h * QB:(h + 1) * QB], NEG_BIG)
            top = jnp.maximum(jnp.max(part, axis=1, keepdims=True), sink[h])
            expo = jnp.exp(part - top)
            norms.append(1.0 / (jnp.sum(expo, axis=1, keepdims=True) + jnp.exp(sink[h] - top)))
            expos.append(expo.astype(jnp.bfloat16))
        result = jnp.dot(jnp.concatenate(expos, axis=0), context, preferred_element_type=jnp.float32)
        heads = [result[h * QB:(h + 1) * QB] * norms[h] for h in range(local_heads)]
        return [
            jnp.where(low_half, pltpu.roll(heads[2 * g], HEAD, 1), heads[2 * g + 1]).astype(jnp.bfloat16)
            for g in range(groups)
        ]


    def attend_other(i, carry):
        @pl.when(i == hb - 1)
        def _():
            halo_wait(halo_kv)
        b = jnp.where(t == 0, hb + i, hb - 1 - i)
        n = b - cross * hb
        at = pl.multiple_of(n * QB, QB)
        for g, value in enumerate(attend(b)):
            att_send[pl.ds(at, QB), g * LANES:(g + 1) * LANES] = value
        ex_att(n).start()

        @pl.when(i == 1)
        def _():
            poll("w11", 1)
        return carry

    def attend_own(i, carry):
        b = jnp.where(t == 0, hb - 1 - i, hb + i)
        at = pl.multiple_of((b - t * hb) * QB, QB)
        for g, value in enumerate(attend(b)):
            joined[t, pl.ds(at, QB), g * LANES:(g + 1) * LANES] = value

        @pl.when(i == 0)
        def _():
            poll("w10", 2)
            poll("w01", 2)

        @pl.when(i == 2)
        def _():
            poll("w11", 2)
        return carry

    lax.fori_loop(0, hb, attend_other, 0)
    lax.fori_loop(0, hb, attend_own, 0)
    poll("w10", *range(3, Z))
    poll("w01", *range(3, Z))

    remote(pool_send, joined.at[T + cross], exp_send.at[0], exp_recv.at[0], s, cross).wait_recv()
    wide = joined.shape[2]

    def columns(n, half, start, count):
        at = pl.ds(pl.multiple_of(start, wide), count)
        return jnp.concatenate([wfull[2 * n, half, at, :], wfull[2 * n + 1, half, at, :]], axis=1)

    def most(j, carry):
        over = j // Z
        @pl.when(j == 2)
        def _():
            poll("w11", *range(3, Z))
        side = y + over - 2 * y * over
        k = j % Z
        zz = jnp.where(z < Z // 2, (z + k) % Z, (z + Z - k) % Z)
        n = zz * 2 + side
        for half in range(T):
            piece = wfull.at[2 * n + 1 - c, half]
            remote(piece, piece, wo_send.at[2], wo_recv.at[2 * n + 1 - c, half], partner, t).wait_recv()
        left = jnp.concatenate([joined[t]] + [joined[T + k] for k in range(T)], axis=1)
        right = jnp.concatenate([columns(n, 0, t * wide, wide), columns(n, 1, 0, T * wide)], axis=0)
        acc[n] = jnp.dot(left, right, preferred_element_type=jnp.float32)
        return carry

    lax.fori_loop(0, S // 2, most, 0)
    for n in range(hb):
        at = pl.ds(n * QB, QB)
        remote(att_send.at[at], joined.at[cross, at], exa_send.at[n], exa_recv.at[n], s, cross).wait_recv()

    def last(n, carry):
        total = acc[n] + jnp.dot(
            joined[cross], columns(n, 0, cross * wide, wide), preferred_element_type=jnp.float32
        )
        out[:, pl.ds(pl.multiple_of(n * 2 * LANES, 2 * LANES), 2 * LANES)] = total.astype(jnp.bfloat16)
        return carry

    lax.fori_loop(0, S // 2, last, 0)
    for cond, make in pending:
        if cond is None:
            make().wait_send()
        else:
            @pl.when(cond)
            def _(make=make):
                make().wait_send()
    for n in range(hb):
        ex_att(n).wait_send()


def body(mesh, tokens, norm_gain, w_query, w_key, w_value, w_pool_in, sink_logit, pool_scale, w_out):
    S = lax.axis_size("sp")
    T = lax.axis_size("tp")
    rows, width = tokens.shape
    local_heads = w_query.shape[1] // HEAD
    fits = (
        S % 4 == 0 and S > 4 and T == 2
        and w_out.shape[1] == LANES and w_key.shape == (LANES, LANES) and w_value.shape == w_key.shape
        and w_query.shape[1] % LANES == 0 and w_pool_in.shape[1] % LANES == 0
        and w_query.shape[1] == w_pool_in.shape[1]
        and local_heads == QH // KVH and rows % (2 * CHUNK) == 0
    )
    if not fits:
        return plain_body(
            tokens, norm_gain, w_query, w_key, w_value, w_pool_in, sink_logit, pool_scale, w_out
        )
    tables = rope_tables(S * rows)
    blocks = rows // QB
    half = rows // T
    Z = S // 4
    F = 2 * (Z - 1)
    reach = POOL_SPANS[-1] // 2
    wide = w_query.shape[1]
    vmem = pl.BlockSpec(memory_space=pltpu.VMEM)
    smem = pl.BlockSpec(memory_space=pltpu.SMEM)
    hbm = pl.BlockSpec(memory_space=pltpu.HBM)
    dma = pltpu.SemaphoreType.DMA
    bf = jnp.bfloat16
    return pl.pallas_call(
        functools.partial(mixer_kernel, (S, T)),
        out_shape=pltpu.VMEM((half, S * w_out.shape[1]), bf),
        in_specs=[hbm, vmem, hbm, hbm, hbm, hbm, smem, vmem, hbm, vmem, vmem, hbm, hbm],
        out_specs=vmem,
        scratch_shapes=[
            pltpu.VMEM((rows, width), bf),
            pltpu.VMEM((rows, width), bf),
            pltpu.VMEM(w_query.shape, bf),
            pltpu.VMEM(w_pool_in.shape, bf),
            pltpu.VMEM((2,) + w_key.shape, bf),
            pltpu.VMEM((S, LANES, LANES), bf),
            pltpu.VMEM((S, T) + w_out.shape, bf),
            pltpu.VMEM((blocks, local_heads * QB, LANES), bf),
            pltpu.VMEM((rows + 2 * WINDOW, LANES), bf),
            pltpu.VMEM((rows + 2 * reach, wide), jnp.float32),
            pltpu.VMEM((half, wide), bf),
            pltpu.VMEM((half, wide), bf),
            pltpu.VMEM((2 * T, half, wide), bf),
            pltpu.VMEM((S // 2, half, 2 * LANES), jnp.float32),
            pltpu.VMEM((blocks, LANES), jnp.float32),
            pltpu.VMEM((blocks, LANES), jnp.float32),
            dma((rows // CHUNK,)),
            dma((7,)),
            dma((S,)),
            dma((4,)),
            dma((2,)),
            dma((F, 3)),
            dma((F + 1,)),
            dma((S, T)),
            dma((4,)),
            dma((3,)),
            dma((2,)),
            dma((5,)),
            dma((F, 4)),
            dma((F,)),
            dma((F + 1,)),
            dma((F, 2)),
            dma((4,)),
            dma((4,)),
            dma((1,)),
            dma((1,)),
            dma((blocks // 2,)),
            dma((blocks // 2,)),
        ],
        compiler_params=pltpu.CompilerParams(
            collective_id=0, has_side_effects=True, vmem_limit_bytes=VMEM_LIMIT
        ),
    )(
        tokens, norm_gain[None, :], w_query, w_key, w_value, w_pool_in, sink_logit, pool_scale[None, :], w_out, *tables
    )


def solution(mesh):
    in_specs = (
        P("sp", None),
        P(),
        P(None, "tp"),
        P("sp", None),
        P("sp", None),
        P(None, "tp"),
        P("tp"),
        P("tp"),
        P("tp", "sp"),
    )
    out_specs = P(("sp", "tp"), None)
    return jax.shard_map(functools.partial(body, mesh), mesh=mesh, in_specs=in_specs, out_specs=out_specs, check_vma=False)
```

```python
import functools

import jax
import jax.numpy as jnp
import numpy as np
from jax import lax
from jax.experimental import pallas as pl
from jax.experimental.pallas import tpu as pltpu
from jax.sharding import PartitionSpec as P

HEAD = 64
QH = 8
KVH = 2
POOL_CH = 128
WINDOW = 128
QB = 128


NEG_BIG = -1e30
POOL_SPANS = (2, 4, 8, 16)


def extended(block, sides, width):
    for axis, dim in sides:
        count = lax.axis_size(axis)
        forward = [(i, i + 1) for i in range(count - 1)]
        backward = [(target, source) for source, target in forward]
        low = lax.ppermute(
            lax.slice_in_dim(block, block.shape[dim] - width, None, axis=dim), axis, forward
        )
        high = lax.ppermute(lax.slice_in_dim(block, 0, width, axis=dim), axis, backward)
        block = jnp.concatenate([low, block, high], axis=dim)
    return block


def layer_normed(tokens, norm_gain):
    values = tokens.astype(jnp.float32)
    center = jnp.mean(values, axis=-1, keepdims=True)
    spread = jnp.mean(jnp.square(values - center), axis=-1, keepdims=True)
    return ((values - center) * lax.rsqrt(spread + 1e-06) * norm_gain).astype(jnp.bfloat16)


def rotate(values, positions):
    half = HEAD // 2
    inverse = 10000.0 ** (-jnp.arange(half, dtype=jnp.float32) / half)
    angles = positions[:, None] * inverse[None, :]
    cosine = jnp.cos(angles)[:, None, :]
    sine = jnp.sin(angles)[:, None, :]
    first = values[..., :half]
    second = values[..., half:]
    return jnp.concatenate(
        [first * cosine - second * sine, first * sine + second * cosine], axis=-1
    )


def plain_body(tokens, norm_gain, w_query, w_key, w_value, w_pool_in, sink_logit, pool_scale, w_out):
    local_rows = tokens.shape[0]
    seq_total = local_rows * lax.axis_size("sp")
    offset = lax.axis_index("sp") * local_rows
    tp_place = lax.axis_index("tp")
    local_heads = w_query.shape[1] // HEAD
    local_pool = w_pool_in.shape[1]
    reach = POOL_SPANS[-1] // 2
    normed = layer_normed(tokens, norm_gain)
    positions = (offset + jnp.arange(local_rows)).astype(jnp.float32)
    query = rotate(
        jnp.dot(normed, w_query, preferred_element_type=jnp.float32).reshape(
            local_rows, local_heads, HEAD
        ),
        positions,
    ).astype(jnp.bfloat16)
    key_head = tp_place * local_heads // (QH // KVH)
    key_cols = lax.dynamic_slice_in_dim(w_key, key_head * HEAD, HEAD, 1)
    value_cols = lax.dynamic_slice_in_dim(w_value, key_head * HEAD, HEAD, 1)
    key_sum = jnp.dot(
        normed,
        lax.all_gather(key_cols, "sp", axis=0, tiled=True),
        preferred_element_type=jnp.float32,
    )
    value_sum = jnp.dot(
        normed,
        lax.all_gather(value_cols, "sp", axis=0, tiled=True),
        preferred_element_type=jnp.float32,
    )
    key = rotate(key_sum[:, None, :], positions)[:, 0, :].astype(jnp.bfloat16)
    value = value_sum.astype(jnp.bfloat16)
    key_value = jnp.concatenate([key, value], axis=1)
    pool_in = jnp.dot(normed, w_pool_in, preferred_element_type=jnp.float32).astype(jnp.bfloat16)
    widened = extended(jnp.concatenate([key_value, pool_in], axis=1), (("sp", 0),), WINDOW)
    kv_wide = widened[:, : 2 * HEAD]
    pool_wide = widened[WINDOW - reach : WINDOW + local_rows + reach, 2 * HEAD :]
    span = QB + 2 * WINDOW
    sink_here = sink_logit[:, None, None]
    results = []
    for block in range(local_rows // QB):
        queries = query[block * QB : (block + 1) * QB]
        keys = kv_wide[block * QB : block * QB + span, :HEAD]
        values = kv_wide[block * QB : block * QB + span, HEAD:]
        scores = jnp.einsum(
            "ihd,jd->hij", queries, keys, preferred_element_type=jnp.float32
        ) * HEAD ** (-0.5)
        query_pos = offset + block * QB + jnp.arange(QB)
        key_pos = offset + block * QB - WINDOW + jnp.arange(span)
        valid = (
            (jnp.abs(query_pos[:, None] - key_pos[None, :]) <= WINDOW)
            & (key_pos[None, :] >= 0)
            & (key_pos[None, :] < seq_total)
        )
        scores = jnp.where(valid, scores, NEG_BIG)
        highest = jnp.maximum(jnp.max(scores, axis=-1, keepdims=True), sink_here)
        expo = jnp.where(valid, jnp.exp(scores - highest), 0.0)
        total = jnp.sum(expo, axis=-1, keepdims=True) + jnp.exp(sink_here - highest)
        weights = (expo / total).astype(jnp.bfloat16)
        result = jnp.einsum("hij,jd->ihd", weights, values, preferred_element_type=jnp.float32)
        results.append(result.reshape(QB, local_heads * HEAD).astype(jnp.bfloat16))
    attended = jnp.concatenate(results, axis=0)
    pool_vals = pool_wide.astype(jnp.float32)
    window_sum = pool_vals
    global_pos = offset + jnp.arange(local_rows)
    channel = tp_place * local_pool + jnp.arange(local_pool)
    window_group = channel // POOL_CH
    measured = jnp.zeros((local_rows, local_pool), jnp.float32)
    stride = 1
    for index, width in enumerate(POOL_SPANS):
        window_sum = window_sum[:-stride] + window_sum[stride:]
        stride = width
        sums = window_sum[reach - width // 2 : reach - width // 2 + local_rows]
        counted = (
            jnp.minimum(global_pos + width // 2, seq_total)
            - jnp.maximum(global_pos - width // 2, 0)
        ).astype(jnp.float32)
        measured = measured + jnp.where(
            window_group[None, :] == index, sums / counted[:, None], 0.0
        )
    pooled = ((measured - pool_vals[reach : reach + local_rows]) * pool_scale).astype(jnp.bfloat16)
    attended_rows, pooled_rows = (
        lax.all_to_all(attended, "tp", split_axis=0, concat_axis=1, tiled=True),
        lax.all_to_all(pooled, "tp", split_axis=0, concat_axis=1, tiled=True),
    )
    joined = jnp.concatenate([attended_rows, pooled_rows], axis=1)
    out_rows_all = lax.all_gather(w_out, "tp", axis=0, tiled=True)
    projected = jnp.dot(
        joined,
        lax.all_gather(out_rows_all, "sp", axis=1, tiled=True),
        preferred_element_type=jnp.float32,
    )
    return projected.astype(jnp.bfloat16)


LANES = 128
CHUNK = 256
VMEM_LIMIT = 60 * 1024 * 1024
MESH = pl.DeviceIdType.MESH


def rope_tables(rows_total):
    half = HEAD // 2
    inverse = np.tile(10000.0 ** (-np.arange(half, dtype=np.float64) / half), LANES // half)[None, :]
    sign = np.where(np.arange(LANES) % HEAD < half, -1.0, 1.0)[None, :]
    inner = np.arange(QB, dtype=np.float64)[:, None] * inverse
    starts = (QB * np.arange(rows_total // QB, dtype=np.float64))[:, None] * inverse
    tables = (np.cos(inner), np.sin(inner) * sign, np.cos(starts), np.sin(starts) * sign)
    return [jnp.asarray(table.astype(np.float32)) for table in tables]


def mixer_kernel(
    places, tokens, gain, w_query, w_key, w_value, w_pool, sink, scale, w_out, cos_in, sin_in, cos_all, sin_all,
    out,
    gain_v, scale_v, sink_v, cos_v, sin_v, tok, wq, wp, wqp, scale_at, shift_at, kv_in, kvw, wfull, qs, kv, pool, pool_send, att_send, joined, acc, cos_at, sin_at,
    tok_sem, own_sem, kv_recv, kz_send, ko_send, kf_send, ky_send,
    wo_recv, wz_send, wo_send, wx_send, wd_send, w00_send, w10_send, w01_send, w11_send,
    halo_send, halo_recv, exp_send, exp_recv, exa_send, exa_recv,
):
    S, T = places
    Z = S // 4
    s = lax.axis_index("sp")
    t = lax.axis_index("tp")
    rows = tokens.shape[0]
    width = tokens.shape[1]
    blocks = rows // QB
    hb = blocks // 2
    chunks = rows // CHUNK
    local_heads = w_query.shape[1] // HEAD
    groups = w_query.shape[1] // LANES
    pgroups = w_pool.shape[1] // LANES
    reach = POOL_SPANS[-1] // 2
    offset = s * rows
    total_rows = S * rows
    c = s % 2
    y = (s // 2) % 2
    z = s // 4
    partner = s + 1 - 2 * c
    yflip = s + 2 - 4 * y
    after = (s + 1) % S
    before = (s + S - 1) % S
    cross = 1 - t
    far = [d for k in range(1, Z) for d in (k, -k)]

    def remote(a, b, send, recv, to_s, to_t):
        return pltpu.make_async_remote_copy(
            src_ref=a, dst_ref=b, send_sem=send, recv_sem=recv,
            device_id={"sp": to_s, "tp": to_t}, device_id_type=MESH,
        )

    def chunk_at(i):
        return pl.multiple_of(jnp.where(t == 0, chunks - 1 - i, i) * CHUNK, CHUNK)

    def tok_copy(i):
        at = pl.ds(chunk_at(i), CHUNK)
        return pltpu.make_async_copy(tokens.at[at], tok.at[at], tok_sem.at[i])

    own_copies = [
        pltpu.make_async_copy(gain, gain_v, own_sem.at[7]),
        pltpu.make_async_copy(w_key, kv_in.at[0], own_sem.at[0]),
        pltpu.make_async_copy(w_value, kv_in.at[1], own_sem.at[1]),
        pltpu.make_async_copy(w_out, wfull.at[s, t], own_sem.at[2]),
        pltpu.make_async_copy(w_query, wq, own_sem.at[3]),
        pltpu.make_async_copy(w_pool, wp, own_sem.at[4]),
        pltpu.make_async_copy(cos_all.at[pl.ds(pl.multiple_of(s * blocks, blocks), blocks)], cos_at, own_sem.at[5]),
        pltpu.make_async_copy(sin_all.at[pl.ds(pl.multiple_of(s * blocks, blocks), blocks)], sin_at, own_sem.at[6]),
        pltpu.make_async_copy(cos_in, cos_v, own_sem.at[8]),
        pltpu.make_async_copy(sin_in, sin_v, own_sem.at[9]),
        pltpu.make_async_copy(scale, scale_v, own_sem.at[10]),
        pltpu.make_async_copy(sink, sink_v, own_sem.at[11]),
    ]
    barrier = pltpu.get_barrier_semaphore()
    greet = [(((z + d) % Z) * 4 + s % 4, t) for d in range(1, Z)]
    greet += [(yflip, t), (after, t), (before, t), (s, cross), (yflip, cross)]
    for to_s, to_t in greet:
        pl.semaphore_signal(barrier, inc=1, device_id={"sp": to_s, "tp": to_t}, device_id_type=MESH)
    for copy in own_copies[:6]:
        copy.start()
    tok_copy(0).start()
    for copy in own_copies[6:]:
        copy.start()
    for i in range(1, chunks):
        tok_copy(i).start()

    lane = lax.broadcasted_iota(jnp.int32, (QB, LANES), 1)
    low_half = lane < HEAD
    first_half = lane % HEAD < HEAD // 2

    own_copies[0].wait()
    gains = jnp.transpose(jnp.concatenate([gain_v[...]] * (LANES // gain.shape[0]), axis=0))

    def gain_column(b):
        return pltpu.roll(gains, (LANES - b) % LANES, 1)[:, :1]

    own_copies[1].wait()
    own_copies[2].wait()
    key_head = t * local_heads // (QH // KVH)
    key_in = kv_in[0].astype(jnp.float32)
    value_in = kv_in[1].astype(jnp.float32)
    key_cols = jnp.where(key_head == 0, key_in, pltpu.roll(key_in, HEAD, 1))
    value_cols = jnp.where(key_head == 0, pltpu.roll(value_in, HEAD, 1), value_in)
    kvw[s] = (jnp.where(low_half, key_cols, value_cols) * gain_column(s)).astype(jnp.bfloat16)
    own_copies[3].wait()

    pending = []

    def go(cond, make):
        pending.append((cond, make))
        if cond is None:
            make().start()
        else:
            @pl.when(cond)
            def _():
                make().start()

    def later(cond, make):
        pending.append((cond, make))

    def here(d):
        return (z + d >= 0) & (z + d < Z)

    def piece_kv(b):
        return kvw.at[b]

    def piece_wo(b, half):
        return wfull.at[b, half]

    def kv_copy(b, send, to):
        return lambda: remote(kvw.at[b], kvw.at[b], send, kv_recv.at[b], to, t)

    def wo_copy(b, half, send, to_s, to_t):
        return lambda: remote(wfull.at[b, half], wfull.at[b, half], send, wo_recv.at[b, half], to_s, to_t)

    hop = [2, -2, 1, -1]

    def at_z(d):
        return s + 4 * d

    def at_yz(d):
        return yflip + 4 * d

    def reach_index(d):
        return far.index(d)

    def start_all(items):
        for cond, make in items:
            if cond is None:
                make().start()
            else:
                @pl.when(cond)
                def _(make=make):
                    make().start()

    def event(cond, arrival, items):
        pending.extend([(cond if k is None else (k if cond is None else cond & k), m) for k, m in items])

        def act():
            def inner():
                if arrival is not None:
                    arrival().wait_recv()
                start_all(items)
            if cond is None:
                inner()
            else:
                pl.when(cond)(inner)
        return act

    def onward(d):
        step = -1 if d > 0 else 1
        return step, here(step)

    ev = {}
    ev["kv_own"] = event(None, None,
        [(here(h), kv_copy(s, kz_send.at[i], at_z(h))) for i, h in enumerate(far)]
        + [(None, kv_copy(s, ko_send.at[0], yflip)), (None, kv_copy(s, ko_send.at[1], partner))])
    for i, d in enumerate(far):
        step, fine = onward(d)
        items = [(None, kv_copy(at_z(d), kf_send.at[i, 0], yflip)), (None, kv_copy(at_z(d), kf_send.at[i, 1], partner))]
        ev["kv", d] = event(here(d), kv_copy(at_z(d), kf_send.at[i, 0], yflip), items)
    for i, d in enumerate([0] + far):
        ev["kvy", d] = event(None if d == 0 else here(d), kv_copy(at_yz(d), ky_send.at[i], partner),
            [(None, kv_copy(at_yz(d), ky_send.at[i], partner))])

    ev["wo_own"] = event(None, None,
        [(None, wo_copy(s, t, wo_send.at[0], s, cross)), (None, wo_copy(s, t, wo_send.at[1], yflip, t))]
        + [(here(h), wo_copy(s, t, wz_send.at[i], at_z(h), t)) for i, h in enumerate(hop) if abs(h) < Z]
        + [(None, wo_copy(s, t, wo_send.at[3], yflip, cross)), (None, wo_copy(s, t, wo_send.at[2], partner, t))])
    ev["wo_x"] = event(None, wo_copy(s, cross, wx_send.at[1], partner, t),
        [(None, wo_copy(s, cross, wx_send.at[1], partner, t))])
    ev["wo_d"] = event(None, wo_copy(yflip, cross, wd_send.at[4], partner, t),
        [(here(h), wo_copy(yflip, cross, wd_send.at[i], at_z(h), t)) for i, h in enumerate(hop) if abs(h) < Z]
        + [(None, wo_copy(yflip, cross, wd_send.at[4], partner, t))])
    for i, d in enumerate(far):
        step, fine = onward(d)
        b = at_z(d)
        items = [(None, wo_copy(b, t, w00_send.at[i, 1], yflip, t)), (None, wo_copy(b, t, w00_send.at[i, 2], partner, t))]
        if abs(d) != 2:
            items = [(None, wo_copy(b, t, w00_send.at[i, 0], s, cross))] + items
        if 2 <= abs(d) < Z - 1:
            items = [(fine, wo_copy(b, t, w00_send.at[i, 3], at_z(step), t))] + items
        ev["w00", d] = event(here(d), wo_copy(b, t, w00_send.at[i, 0], s, cross), items)
        ev["w10", d] = event(here(d), wo_copy(b, cross, w10_send.at[i], partner, t),
            [(None, wo_copy(b, cross, w10_send.at[i], partner, t))])
        b = at_yz(d)
        items = [(None, wo_copy(b, cross, w11_send.at[i, 0], partner, t))]
        if 2 <= abs(d) < Z - 1:
            items = [(fine, wo_copy(b, cross, w11_send.at[i, 1], at_z(step), t))] + items
        if abs(d) == 2:
            items = items + [(None, wo_copy(b, cross, w11_send.at[i, 2], yflip, t))]
        ev["w11", d] = event(here(d), wo_copy(b, cross, w11_send.at[i, 0], partner, t), items)
    for i, d in enumerate([0] + far):
        b = at_yz(d)
        ev["w01", d] = event(None if d == 0 else here(d), wo_copy(b, t, w01_send.at[i], partner, t),
            [(None, wo_copy(b, t, w01_send.at[i], partner, t))])

    def poll(kind, *distances):
        for k in distances:
            for d in ((k, -k) if k else (0,)):
                if abs(d) < Z:
                    ev[kind, d]()

    def begin():
        pl.semaphore_wait(barrier, len(greet))
        ev["kv_own"]()
        ev["wo_own"]()

    late = z > 0

    @pl.when(late)
    def _():
        begin()

    def rotated(values, b):
        ca = cos_at[pl.ds(b, 1), :]
        sa = sin_at[pl.ds(b, 1), :]
        ci = cos_v[...]
        si = sin_v[...]
        cosine = ca * ci - sa * si
        sine = sa * ci + ca * si
        swapped = jnp.where(
            first_half,
            pltpu.roll(values, LANES - HEAD // 2, 1),
            pltpu.roll(values, HEAD // 2, 1),
        )
        return values * cosine + swapped * sine

    for copy in own_copies[4:6]:
        copy.wait()
    wide = w_query.shape[1]

    def fold(b, carry):
        at = pl.ds(pl.multiple_of(b * LANES, LANES), LANES)
        column = gain_column(b)
        sums = []
        for k, part in enumerate((wq, wp)):
            scaled = (part[at, :].astype(jnp.float32) * column).astype(jnp.bfloat16)
            wqp[at, k * wide:(k + 1) * wide] = scaled
            sums.append(jnp.sum(scaled.astype(jnp.float32).reshape(LANES // 8, 8, wide), axis=0))
        return carry + jnp.concatenate(sums, axis=1)

    folded = lax.fori_loop(0, width // LANES, fold, jnp.zeros((8, 2 * wide), jnp.float32), unroll=2)
    total_qp = jnp.sum(folded, axis=0, keepdims=True)
    for copy in own_copies[6:]:
        copy.wait()
    LN = 16
    hc = chunks // 2

    def pooled(b, g):
        cols = slice(g * LANES, (g + 1) * LANES)
        length = QB + 2 * reach
        values = pool[pl.ds(pl.multiple_of(b * QB, QB), length), cols]
        index = (t * (pgroups * LANES) + g * LANES) // POOL_CH
        running = values
        stride = 1
        picked = jnp.zeros((QB, LANES), jnp.float32)
        wide = 0
        for k, span in enumerate(POOL_SPANS):
            running = running + pltpu.roll(running, length - stride, 0)
            stride = span
            shift = reach - span // 2
            sums = (pltpu.roll(running, length - shift, 0) if shift else running)[:QB]
            picked = jnp.where(index == k, sums, picked)
            wide = jnp.where(index == k, span // 2, wide)
        pos = offset + b * QB + lax.broadcasted_iota(jnp.int32, (QB, LANES), 0)
        counted = (jnp.minimum(pos + wide, total_rows) - jnp.maximum(pos - wide, 0)).astype(jnp.float32)
        return ((picked / counted - values[reach:reach + QB]) * scale_v[:, cols]).astype(jnp.bfloat16)


    def ex_pool(n):
        at = pl.ds(pl.multiple_of(n * QB, QB), QB)
        return remote(pool_send.at[at], joined.at[T + t, at], exp_send.at[n], exp_recv.at[n], s, cross)

    def ex_att(n):
        at = pl.ds(pl.multiple_of(n * QB, QB), QB)
        return remote(att_send.at[at], joined.at[t, at], exa_send.at[n], exa_recv.at[n], s, cross)

    def send_pooled(n):
        for g in range(pgroups):
            pool_send[pl.ds(pl.multiple_of(n * QB, QB), QB), g * LANES:(g + 1) * LANES] = pooled(cross * hb + n, g)
        ex_pool(n).start()

    def project(i, carry):
        base = chunk_at(i)
        tok_copy(i).wait()
        raw = jnp.dot(tok[pl.ds(base, CHUNK), :], wqp[...], preferred_element_type=jnp.float32)
        scales = []
        shifts = []
        for r in range(CHUNK // LN):
            at = pl.ds(pl.multiple_of(base + r * LN, LN), LN)
            values = tok[at, :].astype(jnp.float32)
            center = jnp.sum(values, axis=1, keepdims=True) * (1.0 / width)
            moved = values - center
            spread = jnp.sum(moved * moved, axis=1, keepdims=True) * (1.0 / width)
            inverse = lax.rsqrt(spread + 1e-06)
            scales.append(inverse)
            shifts.append(center * inverse)
        rstd = jnp.broadcast_to(jnp.concatenate(scales, axis=0), (CHUNK, LANES))
        drop = jnp.broadcast_to(jnp.concatenate(shifts, axis=0), (CHUNK, LANES))
        scale_at[pl.ds(base, CHUNK), :] = rstd
        shift_at[pl.ds(base, CHUNK), :] = drop

        def normal(k, g):
            at = slice(k * QB, (k + 1) * QB)
            cols = slice(g * LANES, (g + 1) * LANES)
            return raw[at, cols] * rstd[at] - drop[at] * total_qp[:, cols]

        for k in range(CHUNK // QB):
            b = base // QB + k
            for g in range(groups):
                turned = rotated(normal(k, g), b) * HEAD ** (-0.5)
                qs[b, pl.ds(2 * g * QB, QB), :] = jnp.where(low_half, turned, 0.0).astype(jnp.bfloat16)
                qs[b, pl.ds((2 * g + 1) * QB, QB), :] = jnp.where(
                    low_half, pltpu.roll(turned, HEAD, 1), 0.0
                ).astype(jnp.bfloat16)
            for g in range(pgroups):
                pool[pl.ds(pl.multiple_of(reach + base + k * QB, 8), QB), g * LANES:(g + 1) * LANES] = (
                    normal(k, groups + g).astype(jnp.bfloat16).astype(jnp.float32)
                )

        @pl.when((i == 0) & (z == 0))
        def _():
            begin()

        @pl.when(i == hc - 1)
        def _():
            for n in range(1, hb - 1):
                send_pooled(n)

        @pl.when(i == hc)
        def _():
            send_pooled(jnp.where(t == 0, 0, hb - 1))
            poll("kv", *range(1, Z))

        @pl.when(i == chunks - 1)
        def _():
            ev["wo_x"]()
            poll("w01", 0)
        return carry

    lax.fori_loop(0, chunks, project, 0)

    inner = s < S - 1
    outer = s > 0
    halo_pool = [
        (inner, lambda: remote(pool.at[pl.ds(rows, reach)], pool.at[pl.ds(0, reach)], halo_send.at[0], halo_recv.at[0], after, t)),
        (outer, lambda: remote(pool.at[pl.ds(reach, reach)], pool.at[pl.ds(rows + reach, reach)], halo_send.at[1], halo_recv.at[1], before, t)),
    ]
    halo_kv = [
        (inner, lambda: remote(kv.at[pl.ds(rows, WINDOW)], kv.at[pl.ds(0, WINDOW)], halo_send.at[2], halo_recv.at[2], after, t)),
        (outer, lambda: remote(kv.at[pl.ds(WINDOW, WINDOW)], kv.at[pl.ds(rows + WINDOW, WINDOW)], halo_send.at[3], halo_recv.at[3], before, t)),
    ]
    pending.extend(halo_pool + halo_kv)

    def halo_wait(pair):
        @pl.when(outer)
        def _():
            pair[0][1]().wait_recv()

        @pl.when(inner)
        def _():
            pair[1][1]().wait_recv()

    start_all(halo_pool)

    @pl.when(s == 0)
    def _():
        pool[0:reach, :] = jnp.zeros((reach, pool.shape[1]), jnp.float32)
        kv[0:WINDOW, :] = jnp.zeros((WINDOW, LANES), jnp.bfloat16)

    @pl.when(s == S - 1)
    def _():
        pool[rows + reach:rows + 2 * reach, :] = jnp.zeros((reach, pool.shape[1]), jnp.float32)
        kv[rows + WINDOW:rows + 2 * WINDOW, :] = jnp.zeros((WINDOW, LANES), jnp.bfloat16)

    def pool_own(i, carry):
        for g in range(pgroups):
            joined[T + t, pl.ds(pl.multiple_of(i * QB, QB), QB), g * LANES:(g + 1) * LANES] = pooled(t * hb + i, g)
        return carry

    halo_wait(halo_pool)
    send_pooled(jnp.where(t == 0, hb - 1, 0))
    poll("kvy", *range(Z))
    poll("w00", 2)
    lax.fori_loop(0, hb, pool_own, 0)
    arrives = [(None, partner), (None, yflip + partner - s)]
    arrives += [(here(d), partner + 4 * d) for d in far] + [(here(d), yflip + partner - s + 4 * d) for d in far]
    for cond, b in arrives:
        make = kv_copy(b, ko_send.at[1], partner)
        if cond is None:
            make().wait_recv()
        else:
            @pl.when(cond)
            def _(make=make):
                make().wait_recv()

    def gather_sum(b, carry):
        return carry + jnp.sum(kvw[b].astype(jnp.float32).reshape(LANES // 8, 8, LANES), axis=0)

    total_kv = jnp.sum(
        lax.fori_loop(0, S, gather_sum, jnp.zeros((8, LANES), jnp.float32), unroll=4), axis=0, keepdims=True
    )

    def key_value(j, carry):
        i = jnp.where(j == 0, 0, jnp.where(j == 1, chunks - 1, j - 1))
        base = pl.multiple_of(i * CHUNK, CHUNK)
        both = jnp.dot(
            tok[pl.ds(base, CHUNK), :], kvw[...].reshape(width, LANES), preferred_element_type=jnp.float32
        )
        both = both * scale_at[pl.ds(base, CHUNK), :] - shift_at[pl.ds(base, CHUNK), :] * total_kv
        for k in range(CHUNK // QB):
            piece = both[k * QB:(k + 1) * QB, :]
            turned = rotated(piece, i * (CHUNK // QB) + k)
            kv[pl.ds(pl.multiple_of(WINDOW + base + k * QB, QB), QB), :] = jnp.where(
                low_half, turned, piece
            ).astype(jnp.bfloat16)

        @pl.when(j == 1)
        def _():
            start_all(halo_kv)
            ev["wo_d"]()
            poll("w00", 1)
        return carry

    lax.fori_loop(0, chunks, key_value, 0)

    span = QB + 2 * WINDOW
    row_id = lax.broadcasted_iota(jnp.int32, (QB, span), 0)
    col_id = lax.broadcasted_iota(jnp.int32, (QB, span), 1)

    def attend(b):
        context = kv[pl.ds(pl.multiple_of(b * QB, QB), span), :]
        scores = lax.dot_general(
            qs[b], context, (((1,), (1,)), ((), ())), preferred_element_type=jnp.float32
        )
        start = offset + b * QB
        lowest = jnp.maximum(row_id, WINDOW - start)
        highest_col = jnp.minimum(row_id + 2 * WINDOW, total_rows - 1 - start + WINDOW)
        valid = (col_id >= lowest) & (col_id <= highest_col)
        expos = []
        norms = []
        for h in range(local_heads):
            part = jnp.where(valid, scores[h * QB:(h + 1) * QB], NEG_BIG)
            top = jnp.maximum(jnp.max(part, axis=1, keepdims=True), sink_v[h])
            expo = jnp.exp(part - top)
            norms.append(1.0 / (jnp.sum(expo, axis=1, keepdims=True) + jnp.exp(sink_v[h] - top)))
            expos.append(expo.astype(jnp.bfloat16))
        result = jnp.dot(jnp.concatenate(expos, axis=0), context, preferred_element_type=jnp.float32)
        heads = [result[h * QB:(h + 1) * QB] * norms[h] for h in range(local_heads)]
        return [
            jnp.where(low_half, pltpu.roll(heads[2 * g], HEAD, 1), heads[2 * g + 1]).astype(jnp.bfloat16)
            for g in range(groups)
        ]


    def attend_other(i, carry):
        @pl.when(i == hb - 1)
        def _():
            halo_wait(halo_kv)
        b = jnp.where(t == 0, hb + i, hb - 1 - i)
        n = b - cross * hb
        at = pl.multiple_of(n * QB, QB)
        for g, value in enumerate(attend(b)):
            att_send[pl.ds(at, QB), g * LANES:(g + 1) * LANES] = value
        ex_att(n).start()

        @pl.when(i == hb - 1)
        def _():
            poll("w01", 2)
            poll("w00", *range(3, Z))
        return carry

    def attend_own(i, carry):
        b = jnp.where(t == 0, hb - 1 - i, hb + i)
        at = pl.multiple_of((b - t * hb) * QB, QB)
        for g, value in enumerate(attend(b)):
            joined[t, pl.ds(at, QB), g * LANES:(g + 1) * LANES] = value

        @pl.when(i == 1)
        def _():
            poll("w01", 1)
            poll("w10", 1)

        @pl.when(i == hb - 1)
        def _():
            poll("w11", 2)
        return carry

    lax.fori_loop(0, hb, attend_other, 0)
    lax.fori_loop(0, hb, attend_own, 0)
    for n in range(hb):
        at = pl.ds(n * QB, QB)
        remote(pool_send.at[at], joined.at[T + cross, at], exp_send.at[n], exp_recv.at[n], s, cross).wait_recv()

    def columns(n, half, start, count):
        at = pl.ds(pl.multiple_of(start, wide), count)
        return jnp.concatenate([wfull[2 * n, half, at, :], wfull[2 * n + 1, half, at, :]], axis=1)

    def most(j, carry):
        @pl.when(j == 0)
        def _():
            poll("w11", 1)

        @pl.when(j == 2)
        def _():
            poll("w01", *range(3, Z))
            poll("w10", *range(2, Z))
            poll("w11", *range(3, Z))
        over = j % 2
        side = y + over - 2 * y * over
        k = j // 2
        zz = jnp.where(z < Z // 2, (z + k) % Z, (z + Z - k) % Z)
        n = zz * 2 + side
        for half in range(T):
            piece = wfull.at[2 * n + 1 - c, half]
            remote(piece, piece, wo_send.at[2], wo_recv.at[2 * n + 1 - c, half], partner, t).wait_recv()
        left = jnp.concatenate([joined[t]] + [joined[T + k] for k in range(T)], axis=1)
        right = jnp.concatenate([columns(n, 0, t * wide, wide), columns(n, 1, 0, T * wide)], axis=0)
        acc[n] = jnp.dot(left, right, preferred_element_type=jnp.float32)
        return carry

    lax.fori_loop(0, S // 2, most, 0)
    for n in range(hb):
        at = pl.ds(n * QB, QB)
        remote(att_send.at[at], joined.at[cross, at], exa_send.at[n], exa_recv.at[n], s, cross).wait_recv()

    def last(n, carry):
        total = acc[n] + jnp.dot(
            joined[cross], columns(n, 0, cross * wide, wide), preferred_element_type=jnp.float32
        )
        out[:, pl.ds(pl.multiple_of(n * 2 * LANES, 2 * LANES), 2 * LANES)] = total.astype(jnp.bfloat16)
        return carry

    lax.fori_loop(0, S // 2, last, 0)
    for cond, make in pending:
        if cond is None:
            make().wait_send()
        else:
            @pl.when(cond)
            def _(make=make):
                make().wait_send()
    for n in range(hb):
        ex_pool(n).wait_send()
        ex_att(n).wait_send()


def body(mesh, tokens, norm_gain, w_query, w_key, w_value, w_pool_in, sink_logit, pool_scale, w_out):
    S = lax.axis_size("sp")
    T = lax.axis_size("tp")
    rows, width = tokens.shape
    local_heads = w_query.shape[1] // HEAD
    fits = (
        S % 4 == 0 and S > 4 and T == 2
        and w_out.shape[1] == LANES and w_key.shape == (LANES, LANES) and w_value.shape == w_key.shape
        and w_query.shape[1] % LANES == 0 and w_pool_in.shape[1] % LANES == 0
        and w_query.shape[1] == w_pool_in.shape[1]
        and local_heads == QH // KVH and rows % (2 * CHUNK) == 0
        and width == S * LANES and LANES % S == 0
    )
    if not fits:
        return plain_body(
            tokens, norm_gain, w_query, w_key, w_value, w_pool_in, sink_logit, pool_scale, w_out
        )
    tables = rope_tables(S * rows)
    blocks = rows // QB
    half = rows // T
    Z = S // 4
    F = 2 * (Z - 1)
    reach = POOL_SPANS[-1] // 2
    wide = w_query.shape[1]
    vmem = pl.BlockSpec(memory_space=pltpu.VMEM)
    hbm = pl.BlockSpec(memory_space=pltpu.HBM)
    dma = pltpu.SemaphoreType.DMA
    bf = jnp.bfloat16
    return pl.pallas_call(
        functools.partial(mixer_kernel, (S, T)),
        out_shape=pltpu.VMEM((half, S * w_out.shape[1]), bf),
        in_specs=[hbm] * 13,
        out_specs=vmem,
        scratch_shapes=[
            pltpu.VMEM((width // LANES, LANES), jnp.float32),
            pltpu.VMEM((1, wide), jnp.float32),
            pltpu.SMEM(sink_logit.shape, jnp.float32),
            pltpu.VMEM((QB, LANES), jnp.float32),
            pltpu.VMEM((QB, LANES), jnp.float32),
            pltpu.VMEM((rows, width), bf),
            pltpu.VMEM(w_query.shape, bf),
            pltpu.VMEM(w_pool_in.shape, bf),
            pltpu.VMEM((width, 2 * wide), bf),
            pltpu.VMEM((rows, LANES), jnp.float32),
            pltpu.VMEM((rows, LANES), jnp.float32),
            pltpu.VMEM((2,) + w_key.shape, bf),
            pltpu.VMEM((S, LANES, LANES), bf),
            pltpu.VMEM((S, T) + w_out.shape, bf),
            pltpu.VMEM((blocks, local_heads * QB, LANES), bf),
            pltpu.VMEM((rows + 2 * WINDOW, LANES), bf),
            pltpu.VMEM((rows + 2 * reach, wide), jnp.float32),
            pltpu.VMEM((half, wide), bf),
            pltpu.VMEM((half, wide), bf),
            pltpu.VMEM((2 * T, half, wide), bf),
            pltpu.VMEM((S // 2, half, 2 * LANES), jnp.float32),
            pltpu.VMEM((blocks, LANES), jnp.float32),
            pltpu.VMEM((blocks, LANES), jnp.float32),
            dma((rows // CHUNK,)),
            dma((12,)),
            dma((S,)),
            dma((F,)),
            dma((2,)),
            dma((F, 2)),
            dma((F + 1,)),
            dma((S, T)),
            dma((4,)),
            dma((4,)),
            dma((2,)),
            dma((5,)),
            dma((F, 4)),
            dma((F,)),
            dma((F + 1,)),
            dma((F, 3)),
            dma((4,)),
            dma((4,)),
            dma((blocks // 2,)),
            dma((blocks // 2,)),
            dma((blocks // 2,)),
            dma((blocks // 2,)),
        ],
        compiler_params=pltpu.CompilerParams(
            collective_id=0, has_side_effects=True, vmem_limit_bytes=VMEM_LIMIT
        ),
    )(
        tokens, norm_gain.reshape(width // LANES, LANES), w_query, w_key, w_value, w_pool_in, sink_logit, pool_scale[None, :], w_out, *tables
    )


def solution(mesh):
    in_specs = (
        P("sp", None),
        P(),
        P(None, "tp"),
        P("sp", None),
        P("sp", None),
        P(None, "tp"),
        P("tp"),
        P("tp"),
        P("tp", "sp"),
    )
    out_specs = P(("sp", "tp"), None)
    return jax.shard_map(functools.partial(body, mesh), mesh=mesh, in_specs=in_specs, out_specs=out_specs, check_vma=False)
```

```python
import functools

import jax
import jax.numpy as jnp
import numpy as np
from jax import lax
from jax.experimental import pallas as pl
from jax.experimental.pallas import tpu as pltpu
from jax.sharding import PartitionSpec as P

HEAD = 64
QH = 8
KVH = 2
POOL_CH = 128
WINDOW = 128
QB = 128


NEG_BIG = -1e30
POOL_SPANS = (2, 4, 8, 16)


def extended(block, sides, width):
    for axis, dim in sides:
        count = lax.axis_size(axis)
        forward = [(i, i + 1) for i in range(count - 1)]
        backward = [(target, source) for source, target in forward]
        low = lax.ppermute(
            lax.slice_in_dim(block, block.shape[dim] - width, None, axis=dim), axis, forward
        )
        high = lax.ppermute(lax.slice_in_dim(block, 0, width, axis=dim), axis, backward)
        block = jnp.concatenate([low, block, high], axis=dim)
    return block


def layer_normed(tokens, norm_gain):
    values = tokens.astype(jnp.float32)
    center = jnp.mean(values, axis=-1, keepdims=True)
    spread = jnp.mean(jnp.square(values - center), axis=-1, keepdims=True)
    return ((values - center) * lax.rsqrt(spread + 1e-06) * norm_gain).astype(jnp.bfloat16)


def rotate(values, positions):
    half = HEAD // 2
    inverse = 10000.0 ** (-jnp.arange(half, dtype=jnp.float32) / half)
    angles = positions[:, None] * inverse[None, :]
    cosine = jnp.cos(angles)[:, None, :]
    sine = jnp.sin(angles)[:, None, :]
    first = values[..., :half]
    second = values[..., half:]
    return jnp.concatenate(
        [first * cosine - second * sine, first * sine + second * cosine], axis=-1
    )


def plain_body(tokens, norm_gain, w_query, w_key, w_value, w_pool_in, sink_logit, pool_scale, w_out):
    local_rows = tokens.shape[0]
    seq_total = local_rows * lax.axis_size("sp")
    offset = lax.axis_index("sp") * local_rows
    tp_place = lax.axis_index("tp")
    local_heads = w_query.shape[1] // HEAD
    local_pool = w_pool_in.shape[1]
    reach = POOL_SPANS[-1] // 2
    normed = layer_normed(tokens, norm_gain)
    positions = (offset + jnp.arange(local_rows)).astype(jnp.float32)
    query = rotate(
        jnp.dot(normed, w_query, preferred_element_type=jnp.float32).reshape(
            local_rows, local_heads, HEAD
        ),
        positions,
    ).astype(jnp.bfloat16)
    key_head = tp_place * local_heads // (QH // KVH)
    key_cols = lax.dynamic_slice_in_dim(w_key, key_head * HEAD, HEAD, 1)
    value_cols = lax.dynamic_slice_in_dim(w_value, key_head * HEAD, HEAD, 1)
    key_sum = jnp.dot(
        normed,
        lax.all_gather(key_cols, "sp", axis=0, tiled=True),
        preferred_element_type=jnp.float32,
    )
    value_sum = jnp.dot(
        normed,
        lax.all_gather(value_cols, "sp", axis=0, tiled=True),
        preferred_element_type=jnp.float32,
    )
    key = rotate(key_sum[:, None, :], positions)[:, 0, :].astype(jnp.bfloat16)
    value = value_sum.astype(jnp.bfloat16)
    key_value = jnp.concatenate([key, value], axis=1)
    pool_in = jnp.dot(normed, w_pool_in, preferred_element_type=jnp.float32).astype(jnp.bfloat16)
    widened = extended(jnp.concatenate([key_value, pool_in], axis=1), (("sp", 0),), WINDOW)
    kv_wide = widened[:, : 2 * HEAD]
    pool_wide = widened[WINDOW - reach : WINDOW + local_rows + reach, 2 * HEAD :]
    span = QB + 2 * WINDOW
    sink_here = sink_logit[:, None, None]
    results = []
    for block in range(local_rows // QB):
        queries = query[block * QB : (block + 1) * QB]
        keys = kv_wide[block * QB : block * QB + span, :HEAD]
        values = kv_wide[block * QB : block * QB + span, HEAD:]
        scores = jnp.einsum(
            "ihd,jd->hij", queries, keys, preferred_element_type=jnp.float32
        ) * HEAD ** (-0.5)
        query_pos = offset + block * QB + jnp.arange(QB)
        key_pos = offset + block * QB - WINDOW + jnp.arange(span)
        valid = (
            (jnp.abs(query_pos[:, None] - key_pos[None, :]) <= WINDOW)
            & (key_pos[None, :] >= 0)
            & (key_pos[None, :] < seq_total)
        )
        scores = jnp.where(valid, scores, NEG_BIG)
        highest = jnp.maximum(jnp.max(scores, axis=-1, keepdims=True), sink_here)
        expo = jnp.where(valid, jnp.exp(scores - highest), 0.0)
        total = jnp.sum(expo, axis=-1, keepdims=True) + jnp.exp(sink_here - highest)
        weights = (expo / total).astype(jnp.bfloat16)
        result = jnp.einsum("hij,jd->ihd", weights, values, preferred_element_type=jnp.float32)
        results.append(result.reshape(QB, local_heads * HEAD).astype(jnp.bfloat16))
    attended = jnp.concatenate(results, axis=0)
    pool_vals = pool_wide.astype(jnp.float32)
    window_sum = pool_vals
    global_pos = offset + jnp.arange(local_rows)
    channel = tp_place * local_pool + jnp.arange(local_pool)
    window_group = channel // POOL_CH
    measured = jnp.zeros((local_rows, local_pool), jnp.float32)
    stride = 1
    for index, width in enumerate(POOL_SPANS):
        window_sum = window_sum[:-stride] + window_sum[stride:]
        stride = width
        sums = window_sum[reach - width // 2 : reach - width // 2 + local_rows]
        counted = (
            jnp.minimum(global_pos + width // 2, seq_total)
            - jnp.maximum(global_pos - width // 2, 0)
        ).astype(jnp.float32)
        measured = measured + jnp.where(
            window_group[None, :] == index, sums / counted[:, None], 0.0
        )
    pooled = ((measured - pool_vals[reach : reach + local_rows]) * pool_scale).astype(jnp.bfloat16)
    attended_rows, pooled_rows = (
        lax.all_to_all(attended, "tp", split_axis=0, concat_axis=1, tiled=True),
        lax.all_to_all(pooled, "tp", split_axis=0, concat_axis=1, tiled=True),
    )
    joined = jnp.concatenate([attended_rows, pooled_rows], axis=1)
    out_rows_all = lax.all_gather(w_out, "tp", axis=0, tiled=True)
    projected = jnp.dot(
        joined,
        lax.all_gather(out_rows_all, "sp", axis=1, tiled=True),
        preferred_element_type=jnp.float32,
    )
    return projected.astype(jnp.bfloat16)


LANES = 128
CHUNK = 256
VMEM_LIMIT = 60 * 1024 * 1024
MESH = pl.DeviceIdType.MESH


def rope_tables(rows_total):
    half = HEAD // 2
    inverse = np.tile(10000.0 ** (-np.arange(half, dtype=np.float64) / half), LANES // half)[None, :]
    sign = np.where(np.arange(LANES) % HEAD < half, -1.0, 1.0)[None, :]
    inner = np.arange(QB, dtype=np.float64)[:, None] * inverse
    starts = (QB * np.arange(rows_total // QB, dtype=np.float64))[:, None] * inverse
    tables = (np.cos(inner), np.sin(inner) * sign, np.cos(starts), np.sin(starts) * sign)
    return [jnp.asarray(table.astype(np.float32)) for table in tables]


def mixer_kernel(
    places, tokens, gain, w_query, w_key, w_value, w_pool, sink, scale, w_out, cos_in, sin_in, cos_all, sin_all,
    out,
    tok_halo, gain_v, scale_v, sink_v, cos_v, sin_v, tok, wq, wp, wqp, scale_at, shift_at, kv_in, kvw, wfull, qs, kv, pool, pool_send, att_send, joined, acc, cos_at, sin_at,
    tok_sem, own_sem, kv_recv, kz_send, ko_send, kf_send, ky_send,
    wo_recv, wz_send, wo_send, wx_send, wd_send, w00_send, w10_send, w01_send, w11_send,
    halo_send, halo_recv, exp_send, exp_recv, exa_send, exa_recv,
):
    S, T = places
    Z = S // 4
    s = lax.axis_index("sp")
    t = lax.axis_index("tp")
    rows = tokens.shape[0]
    width = tokens.shape[1]
    blocks = rows // QB
    hb = blocks // 2
    chunks = rows // CHUNK
    local_heads = w_query.shape[1] // HEAD
    groups = w_query.shape[1] // LANES
    pgroups = w_pool.shape[1] // LANES
    reach = POOL_SPANS[-1] // 2
    offset = s * rows
    total_rows = S * rows
    c = s % 2
    y = (s // 2) % 2
    z = s // 4
    partner = s + 1 - 2 * c
    yflip = s + 2 - 4 * y
    after = (s + 1) % S
    before = (s + S - 1) % S
    cross = 1 - t
    far = [d for k in range(1, Z) for d in (k, -k)]

    def remote(a, b, send, recv, to_s, to_t):
        return pltpu.make_async_remote_copy(
            src_ref=a, dst_ref=b, send_sem=send, recv_sem=recv,
            device_id={"sp": to_s, "tp": to_t}, device_id_type=MESH,
        )

    def chunk_at(i):
        return pl.multiple_of(jnp.where(t == 0, chunks - 1 - i, i) * CHUNK, CHUNK)

    def tok_copy(i):
        at = pl.ds(chunk_at(i), CHUNK)
        return pltpu.make_async_copy(tokens.at[at], tok.at[at], tok_sem.at[i])

    own_copies = [
        pltpu.make_async_copy(gain, gain_v, own_sem.at[7]),
        pltpu.make_async_copy(w_key, kv_in.at[0], own_sem.at[0]),
        pltpu.make_async_copy(w_value, kv_in.at[1], own_sem.at[1]),
        pltpu.make_async_copy(w_out, wfull.at[s, t], own_sem.at[2]),
        pltpu.make_async_copy(w_query, wq, own_sem.at[3]),
        pltpu.make_async_copy(w_pool, wp, own_sem.at[4]),
        pltpu.make_async_copy(cos_all.at[pl.ds(pl.multiple_of(s * blocks, blocks), blocks)], cos_at, own_sem.at[5]),
        pltpu.make_async_copy(sin_all.at[pl.ds(pl.multiple_of(s * blocks, blocks), blocks)], sin_at, own_sem.at[6]),
        pltpu.make_async_copy(cos_in, cos_v, own_sem.at[8]),
        pltpu.make_async_copy(sin_in, sin_v, own_sem.at[9]),
        pltpu.make_async_copy(scale, scale_v, own_sem.at[10]),
        pltpu.make_async_copy(sink, sink_v, own_sem.at[11]),
    ]
    barrier = pltpu.get_barrier_semaphore()
    greet = [(((z + d) % Z) * 4 + s % 4, t) for d in range(1, Z)]
    greet += [(yflip, t), (after, t), (before, t), (s, cross), (yflip, cross)]
    for to_s, to_t in greet:
        pl.semaphore_signal(barrier, inc=1, device_id={"sp": to_s, "tp": to_t}, device_id_type=MESH)
    for copy in own_copies[:6]:
        copy.start()
    tok_copy(0).start()
    for copy in own_copies[6:]:
        copy.start()
    for i in range(1, chunks):
        tok_copy(i).start()

    lane = lax.broadcasted_iota(jnp.int32, (QB, LANES), 1)
    low_half = lane < HEAD
    first_half = lane % HEAD < HEAD // 2

    own_copies[0].wait()
    gains = jnp.transpose(jnp.concatenate([gain_v[...]] * (LANES // gain.shape[0]), axis=0))

    def gain_column(b):
        return pltpu.roll(gains, (LANES - b) % LANES, 1)[:, :1]

    own_copies[1].wait()
    own_copies[2].wait()
    key_head = t * local_heads // (QH // KVH)
    key_in = kv_in[0].astype(jnp.float32)
    value_in = kv_in[1].astype(jnp.float32)
    key_cols = jnp.where(key_head == 0, key_in, pltpu.roll(key_in, HEAD, 1))
    value_cols = jnp.where(key_head == 0, pltpu.roll(value_in, HEAD, 1), value_in)
    kvw[s] = (jnp.where(low_half, key_cols, value_cols) * gain_column(s)).astype(jnp.bfloat16)
    own_copies[3].wait()

    pending = []

    def go(cond, make):
        pending.append((cond, make))
        if cond is None:
            make().start()
        else:
            @pl.when(cond)
            def _():
                make().start()

    def later(cond, make):
        pending.append((cond, make))

    def here(d):
        return (z + d >= 0) & (z + d < Z)

    def piece_kv(b):
        return kvw.at[b]

    def piece_wo(b, half):
        return wfull.at[b, half]

    def kv_copy(b, send, to):
        return lambda: remote(kvw.at[b], kvw.at[b], send, kv_recv.at[b], to, t)

    def wo_copy(b, half, send, to_s, to_t):
        return lambda: remote(wfull.at[b, half], wfull.at[b, half], send, wo_recv.at[b, half], to_s, to_t)

    hop = [2, -2, 1, -1]

    def at_z(d):
        return s + 4 * d

    def at_yz(d):
        return yflip + 4 * d

    def reach_index(d):
        return far.index(d)

    def start_all(items):
        for cond, make in items:
            if cond is None:
                make().start()
            else:
                @pl.when(cond)
                def _(make=make):
                    make().start()

    def event(cond, arrival, items):
        pending.extend([(cond if k is None else (k if cond is None else cond & k), m) for k, m in items])

        def act():
            def inner():
                if arrival is not None:
                    arrival().wait_recv()
                start_all(items)
            if cond is None:
                inner()
            else:
                pl.when(cond)(inner)
        return act

    def onward(d):
        step = -1 if d > 0 else 1
        return step, here(step)

    ev = {}
    ev["kv_own"] = event(None, None,
        [(here(h), kv_copy(s, kz_send.at[i], at_z(h))) for i, h in enumerate(far)]
        + [(None, kv_copy(s, ko_send.at[0], yflip)), (None, kv_copy(s, ko_send.at[1], partner))])
    for i, d in enumerate(far):
        step, fine = onward(d)
        items = [(None, kv_copy(at_z(d), kf_send.at[i, 0], yflip)), (None, kv_copy(at_z(d), kf_send.at[i, 1], partner))]
        ev["kv", d] = event(here(d), kv_copy(at_z(d), kf_send.at[i, 0], yflip), items)
    for i, d in enumerate([0] + far):
        ev["kvy", d] = event(None if d == 0 else here(d), kv_copy(at_yz(d), ky_send.at[i], partner),
            [(None, kv_copy(at_yz(d), ky_send.at[i], partner))])

    ev["wo_own"] = event(None, None,
        [(None, wo_copy(s, t, wo_send.at[0], s, cross)), (None, wo_copy(s, t, wo_send.at[1], yflip, t)),
         (None, wo_copy(s, t, wo_send.at[2], partner, t))])
    ev["wo_own_z"] = event(None, None,
        [(here(h), wo_copy(s, t, wz_send.at[i], at_z(h), t)) for i, h in enumerate(hop) if abs(h) < Z])
    ev["wo_x"] = event(None, wo_copy(s, cross, wx_send.at[0], yflip, t),
        [(None, wo_copy(s, cross, wx_send.at[0], yflip, t)), (None, wo_copy(s, cross, wx_send.at[1], partner, t))])
    ev["wo_d"] = event(None, wo_copy(yflip, cross, wd_send.at[4], partner, t),
        [(here(h), wo_copy(yflip, cross, wd_send.at[i], at_z(h), t)) for i, h in enumerate(hop) if abs(h) < Z]
        + [(None, wo_copy(yflip, cross, wd_send.at[4], partner, t))])
    for i, d in enumerate(far):
        step, fine = onward(d)
        b = at_z(d)
        items = [(None, wo_copy(b, t, w00_send.at[i, 2], partner, t))]
        ev["w00y", d] = event(here(d), None, [(None, wo_copy(b, t, w00_send.at[i, 1], yflip, t))])
        items = [(None, wo_copy(b, t, w00_send.at[i, 0], s, cross))] + items
        if 2 <= abs(d) < Z - 1:
            items = [(fine, wo_copy(b, t, w00_send.at[i, 3], at_z(step), t))] + items
        ev["w00", d] = event(here(d), wo_copy(b, t, w00_send.at[i, 0], s, cross), items)
        ev["w10", d] = event(here(d), wo_copy(b, cross, w10_send.at[i], partner, t),
            [(None, wo_copy(b, cross, w10_send.at[i], partner, t))])
        b = at_yz(d)
        items = [(None, wo_copy(b, cross, w11_send.at[i, 0], partner, t))]
        if 2 <= abs(d) < Z - 1:
            items = [(fine, wo_copy(b, cross, w11_send.at[i, 1], at_z(step), t))] + items
        ev["w11", d] = event(here(d), wo_copy(b, cross, w11_send.at[i, 0], partner, t), items)
    for i, d in enumerate([0] + far):
        b = at_yz(d)
        ev["w01", d] = event(None if d == 0 else here(d), wo_copy(b, t, w01_send.at[i], partner, t),
            [(None, wo_copy(b, t, w01_send.at[i], partner, t))])

    def poll(kind, *distances):
        for k in distances:
            for d in ((k, -k) if k else (0,)):
                if abs(d) < Z:
                    ev[kind, d]()

    inner = s < S - 1
    outer = s > 0
    halo_tok = [
        (inner, lambda: remote(tokens.at[pl.ds(rows - reach, reach)], tok_halo.at[0], halo_send.at[0], halo_recv.at[0], after, t)),
        (outer, lambda: remote(tokens.at[pl.ds(0, reach)], tok_halo.at[1], halo_send.at[1], halo_recv.at[1], before, t)),
    ]
    halo_kv = [
        (inner, lambda: remote(kv.at[pl.ds(rows, WINDOW)], kv.at[pl.ds(0, WINDOW)], halo_send.at[2], halo_recv.at[2], after, t)),
        (outer, lambda: remote(kv.at[pl.ds(WINDOW, WINDOW)], kv.at[pl.ds(rows + WINDOW, WINDOW)], halo_send.at[3], halo_recv.at[3], before, t)),
    ]
    pending.extend(halo_tok + halo_kv)

    def halo_wait(pair):
        @pl.when(outer)
        def _():
            pair[0][1]().wait_recv()

        @pl.when(inner)
        def _():
            pair[1][1]().wait_recv()

    @pl.when(s == 0)
    def _():
        tok_halo[0] = jnp.zeros((reach, width), jnp.bfloat16)
        kv[0:WINDOW, :] = jnp.zeros((WINDOW, LANES), jnp.bfloat16)

    @pl.when(s == S - 1)
    def _():
        tok_halo[1] = jnp.zeros((reach, width), jnp.bfloat16)
        kv[rows + WINDOW:rows + 2 * WINDOW, :] = jnp.zeros((WINDOW, LANES), jnp.bfloat16)

    def begin():
        pl.semaphore_wait(barrier, len(greet))
        start_all(halo_tok)
        ev["kv_own"]()
        ev["wo_own"]()

    late = z > 0

    @pl.when(late)
    def _():
        begin()

    def rotated(values, b):
        ca = cos_at[pl.ds(b, 1), :]
        sa = sin_at[pl.ds(b, 1), :]
        ci = cos_v[...]
        si = sin_v[...]
        cosine = ca * ci - sa * si
        sine = sa * ci + ca * si
        swapped = jnp.where(
            first_half,
            pltpu.roll(values, LANES - HEAD // 2, 1),
            pltpu.roll(values, HEAD // 2, 1),
        )
        return values * cosine + swapped * sine

    for copy in own_copies[4:6]:
        copy.wait()
    wide = w_query.shape[1]

    def fold(b, carry):
        at = pl.ds(pl.multiple_of(b * LANES, LANES), LANES)
        column = gain_column(b)
        sums = []
        for k, part in enumerate((wq, wp)):
            scaled = (part[at, :].astype(jnp.float32) * column).astype(jnp.bfloat16)
            wqp[at, k * wide:(k + 1) * wide] = scaled
            sums.append(jnp.sum(scaled.astype(jnp.float32).reshape(LANES // 8, 8, wide), axis=0))
        return carry + jnp.concatenate(sums, axis=1)

    folded = lax.fori_loop(0, width // LANES, fold, jnp.zeros((8, 2 * wide), jnp.float32), unroll=2)
    total_qp = jnp.sum(folded, axis=0, keepdims=True)

    for copy in own_copies[6:]:
        copy.wait()
    LN = 16
    hc = chunks // 2

    def pooled(b, g):
        cols = slice(g * LANES, (g + 1) * LANES)
        length = QB + 2 * reach
        values = pool[pl.ds(pl.multiple_of(b * QB, QB), length), cols]
        index = (t * (pgroups * LANES) + g * LANES) // POOL_CH
        running = values
        stride = 1
        picked = jnp.zeros((QB, LANES), jnp.float32)
        wide = 0
        for k, span in enumerate(POOL_SPANS):
            running = running + pltpu.roll(running, length - stride, 0)
            stride = span
            shift = reach - span // 2
            sums = (pltpu.roll(running, length - shift, 0) if shift else running)[:QB]
            picked = jnp.where(index == k, sums, picked)
            wide = jnp.where(index == k, span // 2, wide)
        pos = offset + b * QB + lax.broadcasted_iota(jnp.int32, (QB, LANES), 0)
        counted = (jnp.minimum(pos + wide, total_rows) - jnp.maximum(pos - wide, 0)).astype(jnp.float32)
        return ((picked / counted - values[reach:reach + QB]) * scale_v[:, cols]).astype(jnp.bfloat16)


    def ex_pool(n):
        at = pl.ds(pl.multiple_of(n * QB, QB), QB)
        return remote(pool_send.at[at], joined.at[T + t, at], exp_send.at[n], exp_recv.at[n], s, cross)

    def ex_att(n):
        at = pl.ds(pl.multiple_of(n * QB, QB), QB)
        return remote(att_send.at[at], joined.at[t, at], exa_send.at[n], exa_recv.at[n], s, cross)

    def send_pooled(n):
        for g in range(pgroups):
            pool_send[pl.ds(pl.multiple_of(n * QB, QB), QB), g * LANES:(g + 1) * LANES] = pooled(cross * hb + n, g)
        ex_pool(n).start()

    def moments(rows_in):
        values = rows_in.astype(jnp.float32)
        center = jnp.sum(values, axis=1, keepdims=True) * (1.0 / width)
        moved = values - center
        spread = jnp.sum(moved * moved, axis=1, keepdims=True) * (1.0 / width)
        inverse = lax.rsqrt(spread + 1e-06)
        return inverse, center * inverse

    def project(i, carry):
        base = chunk_at(i)
        tok_copy(i).wait()
        raw = jnp.dot(tok[pl.ds(base, CHUNK), :], wqp[...], preferred_element_type=jnp.float32)
        scales = []
        shifts = []
        for r in range(CHUNK // LN):
            at = pl.ds(pl.multiple_of(base + r * LN, LN), LN)
            inverse, shifted = moments(tok[at, :])
            scales.append(inverse)
            shifts.append(shifted)
        rstd = jnp.broadcast_to(jnp.concatenate(scales, axis=0), (CHUNK, LANES))
        drop = jnp.broadcast_to(jnp.concatenate(shifts, axis=0), (CHUNK, LANES))
        scale_at[pl.ds(base, CHUNK), :] = rstd
        shift_at[pl.ds(base, CHUNK), :] = drop

        def normal(k, g):
            at = slice(k * QB, (k + 1) * QB)
            cols = slice(g * LANES, (g + 1) * LANES)
            return raw[at, cols] * rstd[at] - drop[at] * total_qp[:, cols]

        for k in range(CHUNK // QB):
            b = base // QB + k
            for g in range(groups):
                turned = rotated(normal(k, g), b) * HEAD ** (-0.5)
                qs[b, pl.ds(2 * g * QB, QB), :] = jnp.where(low_half, turned, 0.0).astype(jnp.bfloat16)
                qs[b, pl.ds((2 * g + 1) * QB, QB), :] = jnp.where(
                    low_half, pltpu.roll(turned, HEAD, 1), 0.0
                ).astype(jnp.bfloat16)
            for g in range(pgroups):
                pool[pl.ds(pl.multiple_of(reach + base + k * QB, 8), QB), g * LANES:(g + 1) * LANES] = (
                    normal(k, groups + g).astype(jnp.bfloat16).astype(jnp.float32)
                )

        @pl.when((i == 0) & (z == 0))
        def _():
            begin()

        @pl.when(i == jnp.where(z == 0, 1, 0))
        def _():
            ev["wo_own_z"]()

        @pl.when(i == hc - 1)
        def _():
            for n in range(1, hb - 1):
                send_pooled(n)

        @pl.when(i == hc)
        def _():
            send_pooled(jnp.where(t == 0, 0, hb - 1))
            poll("kv", *range(1, Z))
            ev["wo_x"]()

        return carry

    lax.fori_loop(0, chunks, project, 0)

    halo_wait(halo_tok)
    edge = jnp.concatenate([tok_halo[0], tok_halo[1]], axis=0)
    edge_scale, edge_shift = moments(edge)
    edge_pool = (
        jnp.dot(edge, wqp[:, wide:], preferred_element_type=jnp.float32) * edge_scale - edge_shift * total_qp[:, wide:]
    ).astype(jnp.bfloat16).astype(jnp.float32)
    pool[0:reach, :] = edge_pool[:reach]
    pool[rows + reach:rows + 2 * reach, :] = edge_pool[reach:]

    def pool_own(i, carry):
        n = jnp.where(t == 0, i, hb - 1 - i)
        for g in range(pgroups):
            joined[T + t, pl.ds(pl.multiple_of(n * QB, QB), QB), g * LANES:(g + 1) * LANES] = pooled(t * hb + n, g)
        return carry

    send_pooled(jnp.where(t == 0, hb - 1, 0))
    lax.fori_loop(0, hb, pool_own, 0)
    poll("kvy", *range(Z))
    poll("w00", 2)
    arrives = [(None, partner), (None, yflip + partner - s)]
    arrives += [(here(d), partner + 4 * d) for d in far] + [(here(d), yflip + partner - s + 4 * d) for d in far]
    for cond, b in arrives:
        make = kv_copy(b, ko_send.at[1], partner)
        if cond is None:
            make().wait_recv()
        else:
            @pl.when(cond)
            def _(make=make):
                make().wait_recv()

    def gather_sum(b, carry):
        return carry + jnp.sum(kvw[b].astype(jnp.float32).reshape(LANES // 8, 8, LANES), axis=0)

    total_kv = jnp.sum(
        lax.fori_loop(0, S, gather_sum, jnp.zeros((8, LANES), jnp.float32), unroll=4), axis=0, keepdims=True
    )

    def key_value(i):
        base = i * CHUNK
        both = jnp.dot(
            tok[pl.ds(base, CHUNK), :], kvw[...].reshape(width, LANES), preferred_element_type=jnp.float32
        )
        both = both * scale_at[pl.ds(base, CHUNK), :] - shift_at[pl.ds(base, CHUNK), :] * total_kv
        for k in range(CHUNK // QB):
            piece = both[k * QB:(k + 1) * QB, :]
            turned = rotated(piece, i * (CHUNK // QB) + k)
            kv[pl.ds(WINDOW + base + k * QB, QB), :] = jnp.where(low_half, turned, piece).astype(jnp.bfloat16)

    key_value(0)
    key_value(chunks - 1)
    start_all(halo_kv)
    poll("w00y", 2)
    poll("w00", 1)
    for i in range(1, chunks - 1):
        key_value(i)
    ev["wo_d"]()
    poll("w01", 0)
    poll("w00y", 1)

    span = QB + 2 * WINDOW
    row_id = lax.broadcasted_iota(jnp.int32, (QB, span), 0)
    col_id = lax.broadcasted_iota(jnp.int32, (QB, span), 1)

    def attend(b):
        context = kv[pl.ds(pl.multiple_of(b * QB, QB), span), :]
        scores = lax.dot_general(
            qs[b], context, (((1,), (1,)), ((), ())), preferred_element_type=jnp.float32
        )
        start = offset + b * QB
        lowest = jnp.maximum(row_id, WINDOW - start)
        highest_col = jnp.minimum(row_id + 2 * WINDOW, total_rows - 1 - start + WINDOW)
        valid = (col_id >= lowest) & (col_id <= highest_col)
        expos = []
        norms = []
        for h in range(local_heads):
            part = jnp.where(valid, scores[h * QB:(h + 1) * QB], NEG_BIG)
            top = jnp.maximum(jnp.max(part, axis=1, keepdims=True), sink_v[h])
            expo = jnp.exp(part - top)
            norms.append(1.0 / (jnp.sum(expo, axis=1, keepdims=True) + jnp.exp(sink_v[h] - top)))
            expos.append(expo.astype(jnp.bfloat16))
        result = jnp.dot(jnp.concatenate(expos, axis=0), context, preferred_element_type=jnp.float32)
        heads = [result[h * QB:(h + 1) * QB] * norms[h] for h in range(local_heads)]
        return [
            jnp.where(low_half, pltpu.roll(heads[2 * g], HEAD, 1), heads[2 * g + 1]).astype(jnp.bfloat16)
            for g in range(groups)
        ]


    def attend_other(i, carry):
        @pl.when(i == hb - 1)
        def _():
            halo_wait(halo_kv)
        b = jnp.where(t == 0, hb + i, hb - 1 - i)
        n = b - cross * hb
        at = pl.multiple_of(n * QB, QB)
        for g, value in enumerate(attend(b)):
            att_send[pl.ds(at, QB), g * LANES:(g + 1) * LANES] = value
        ex_att(n).start()

        return carry

    def attend_own(i, carry):
        b = jnp.where(t == 0, hb - 1 - i, hb + i)
        at = pl.multiple_of((b - t * hb) * QB, QB)
        for g, value in enumerate(attend(b)):
            joined[t, pl.ds(at, QB), g * LANES:(g + 1) * LANES] = value

        @pl.when(i == 0)
        def _():
            poll("w00", *range(3, Z))
            poll("w00y", *range(3, Z))

        @pl.when(i == 2)
        def _():
            poll("w11", 2)

        @pl.when(i == hb - 1)
        def _():
            poll("w01", 2)
            poll("w10", 2)
            poll("w01", 1)
            poll("w10", 1)
        return carry

    lax.fori_loop(0, hb, attend_other, 0)
    lax.fori_loop(0, hb, attend_own, 0)
    for n in range(hb):
        at = pl.ds(n * QB, QB)
        remote(pool_send.at[at], joined.at[T + cross, at], exp_send.at[n], exp_recv.at[n], s, cross).wait_recv()

    def columns(n, half, start, count):
        at = pl.ds(pl.multiple_of(start, wide), count)
        return jnp.concatenate([wfull[2 * n, half, at, :], wfull[2 * n + 1, half, at, :]], axis=1)

    def chunk_of(j):
        over = j % 2
        side = y + over - 2 * y * over
        k = j // 2
        zz = jnp.where(z < Z // 2, (z + k) % Z, (z + Z - k) % Z)
        return zz * 2 + side

    def chunk_wait(n):
        for half in range(T):
            piece = wfull.at[2 * n + 1 - c, half]
            remote(piece, piece, wo_send.at[2], wo_recv.at[2 * n + 1 - c, half], partner, t).wait_recv()

    def store(n, total):
        out[:, pl.ds(pl.multiple_of(n * 2 * LANES, 2 * LANES), 2 * LANES)] = total.astype(jnp.bfloat16)

    def most(j, carry):
        @pl.when(j == 1)
        def _():
            poll("w11", 1)
        n = chunk_of(j)
        chunk_wait(n)
        left = jnp.concatenate([joined[t]] + [joined[T + k] for k in range(T)], axis=1)
        right = jnp.concatenate([columns(n, 0, t * wide, wide), columns(n, 1, 0, T * wide)], axis=0)
        acc[n] = jnp.dot(left, right, preferred_element_type=jnp.float32)
        return carry

    def last(j, carry):
        n = chunk_of(j)
        store(n, acc[n] + jnp.dot(
            joined[cross], columns(n, 0, cross * wide, wide), preferred_element_type=jnp.float32
        ))
        return carry

    def whole(j, carry):
        @pl.when(j == split)
        def _():
            poll("w01", *range(3, Z))
            poll("w11", *range(3, Z))

        @pl.when(j == split + 1)
        def _():
            poll("w10", *range(3, Z))
        n = chunk_of(j)
        chunk_wait(n)
        left = jnp.concatenate([joined[k] for k in range(2 * T)], axis=1)
        right = jnp.concatenate([columns(n, half, 0, T * wide) for half in range(T)], axis=0)
        store(n, jnp.dot(left, right, preferred_element_type=jnp.float32))
        return carry

    split = S // 4
    lax.fori_loop(0, split, most, 0)
    for n in range(hb):
        at = pl.ds(n * QB, QB)
        remote(att_send.at[at], joined.at[cross, at], exa_send.at[n], exa_recv.at[n], s, cross).wait_recv()
    lax.fori_loop(0, split, last, 0)
    lax.fori_loop(split, S // 2, whole, 0)
    for cond, make in pending:
        if cond is None:
            make().wait_send()
        else:
            @pl.when(cond)
            def _(make=make):
                make().wait_send()
    for n in range(hb):
        ex_pool(n).wait_send()
        ex_att(n).wait_send()


def body(mesh, tokens, norm_gain, w_query, w_key, w_value, w_pool_in, sink_logit, pool_scale, w_out):
    S = lax.axis_size("sp")
    T = lax.axis_size("tp")
    rows, width = tokens.shape
    local_heads = w_query.shape[1] // HEAD
    fits = (
        S % 4 == 0 and S > 4 and T == 2
        and w_out.shape[1] == LANES and w_key.shape == (LANES, LANES) and w_value.shape == w_key.shape
        and w_query.shape[1] % LANES == 0 and w_pool_in.shape[1] % LANES == 0
        and w_query.shape[1] == w_pool_in.shape[1]
        and local_heads == QH // KVH and rows % (2 * CHUNK) == 0
        and width == S * LANES and LANES % S == 0
    )
    if not fits:
        return plain_body(
            tokens, norm_gain, w_query, w_key, w_value, w_pool_in, sink_logit, pool_scale, w_out
        )
    tables = rope_tables(S * rows)
    blocks = rows // QB
    half = rows // T
    Z = S // 4
    F = 2 * (Z - 1)
    reach = POOL_SPANS[-1] // 2
    wide = w_query.shape[1]
    vmem = pl.BlockSpec(memory_space=pltpu.VMEM)
    hbm = pl.BlockSpec(memory_space=pltpu.HBM)
    dma = pltpu.SemaphoreType.DMA
    bf = jnp.bfloat16
    return pl.pallas_call(
        functools.partial(mixer_kernel, (S, T)),
        out_shape=pltpu.VMEM((half, S * w_out.shape[1]), bf),
        in_specs=[hbm] * 13,
        out_specs=vmem,
        scratch_shapes=[
            pltpu.VMEM((2, reach, width), bf),
            pltpu.VMEM((width // LANES, LANES), jnp.float32),
            pltpu.VMEM((1, wide), jnp.float32),
            pltpu.SMEM(sink_logit.shape, jnp.float32),
            pltpu.VMEM((QB, LANES), jnp.float32),
            pltpu.VMEM((QB, LANES), jnp.float32),
            pltpu.VMEM((rows, width), bf),
            pltpu.VMEM(w_query.shape, bf),
            pltpu.VMEM(w_pool_in.shape, bf),
            pltpu.VMEM((width, 2 * wide), bf),
            pltpu.VMEM((rows, LANES), jnp.float32),
            pltpu.VMEM((rows, LANES), jnp.float32),
            pltpu.VMEM((2,) + w_key.shape, bf),
            pltpu.VMEM((S, LANES, LANES), bf),
            pltpu.VMEM((S, T) + w_out.shape, bf),
            pltpu.VMEM((blocks, local_heads * QB, LANES), bf),
            pltpu.VMEM((rows + 2 * WINDOW, LANES), bf),
            pltpu.VMEM((rows + 2 * reach, wide), jnp.float32),
            pltpu.VMEM((half, wide), bf),
            pltpu.VMEM((half, wide), bf),
            pltpu.VMEM((2 * T, half, wide), bf),
            pltpu.VMEM((S // 2, half, 2 * LANES), jnp.float32),
            pltpu.VMEM((blocks, LANES), jnp.float32),
            pltpu.VMEM((blocks, LANES), jnp.float32),
            dma((rows // CHUNK,)),
            dma((12,)),
            dma((S,)),
            dma((F,)),
            dma((2,)),
            dma((F, 2)),
            dma((F + 1,)),
            dma((S, T)),
            dma((4,)),
            dma((4,)),
            dma((2,)),
            dma((5,)),
            dma((F, 4)),
            dma((F,)),
            dma((F + 1,)),
            dma((F, 3)),
            dma((4,)),
            dma((4,)),
            dma((blocks // 2,)),
            dma((blocks // 2,)),
            dma((blocks // 2,)),
            dma((blocks // 2,)),
        ],
        compiler_params=pltpu.CompilerParams(
            collective_id=0, has_side_effects=True, vmem_limit_bytes=VMEM_LIMIT
        ),
    )(
        tokens, norm_gain.reshape(width // LANES, LANES), w_query, w_key, w_value, w_pool_in, sink_logit, pool_scale[None, :], w_out, *tables
    )


def solution(mesh):
    in_specs = (
        P("sp", None),
        P(),
        P(None, "tp"),
        P("sp", None),
        P("sp", None),
        P(None, "tp"),
        P("tp"),
        P("tp"),
        P("tp", "sp"),
    )
    out_specs = P(("sp", "tp"), None)
    return jax.shard_map(functools.partial(body, mesh), mesh=mesh, in_specs=in_specs, out_specs=out_specs, check_vma=False)
```

```python
import functools

import jax
import jax.numpy as jnp
import numpy as np
from jax import lax
from jax.experimental import pallas as pl
from jax.experimental.pallas import tpu as pltpu
from jax.sharding import PartitionSpec as P

HEAD = 64
QH = 8
KVH = 2
POOL_CH = 128
WINDOW = 128
QB = 128


NEG_BIG = -1e30
POOL_SPANS = (2, 4, 8, 16)


def extended(block, sides, width):
    for axis, dim in sides:
        count = lax.axis_size(axis)
        forward = [(i, i + 1) for i in range(count - 1)]
        backward = [(target, source) for source, target in forward]
        low = lax.ppermute(
            lax.slice_in_dim(block, block.shape[dim] - width, None, axis=dim), axis, forward
        )
        high = lax.ppermute(lax.slice_in_dim(block, 0, width, axis=dim), axis, backward)
        block = jnp.concatenate([low, block, high], axis=dim)
    return block


def layer_normed(tokens, norm_gain):
    values = tokens.astype(jnp.float32)
    center = jnp.mean(values, axis=-1, keepdims=True)
    spread = jnp.mean(jnp.square(values - center), axis=-1, keepdims=True)
    return ((values - center) * lax.rsqrt(spread + 1e-06) * norm_gain).astype(jnp.bfloat16)


def rotate(values, positions):
    half = HEAD // 2
    inverse = 10000.0 ** (-jnp.arange(half, dtype=jnp.float32) / half)
    angles = positions[:, None] * inverse[None, :]
    cosine = jnp.cos(angles)[:, None, :]
    sine = jnp.sin(angles)[:, None, :]
    first = values[..., :half]
    second = values[..., half:]
    return jnp.concatenate(
        [first * cosine - second * sine, first * sine + second * cosine], axis=-1
    )


def plain_body(tokens, norm_gain, w_query, w_key, w_value, w_pool_in, sink_logit, pool_scale, w_out):
    local_rows = tokens.shape[0]
    seq_total = local_rows * lax.axis_size("sp")
    offset = lax.axis_index("sp") * local_rows
    tp_place = lax.axis_index("tp")
    local_heads = w_query.shape[1] // HEAD
    local_pool = w_pool_in.shape[1]
    reach = POOL_SPANS[-1] // 2
    normed = layer_normed(tokens, norm_gain)
    positions = (offset + jnp.arange(local_rows)).astype(jnp.float32)
    query = rotate(
        jnp.dot(normed, w_query, preferred_element_type=jnp.float32).reshape(
            local_rows, local_heads, HEAD
        ),
        positions,
    ).astype(jnp.bfloat16)
    key_head = tp_place * local_heads // (QH // KVH)
    key_cols = lax.dynamic_slice_in_dim(w_key, key_head * HEAD, HEAD, 1)
    value_cols = lax.dynamic_slice_in_dim(w_value, key_head * HEAD, HEAD, 1)
    key_sum = jnp.dot(
        normed,
        lax.all_gather(key_cols, "sp", axis=0, tiled=True),
        preferred_element_type=jnp.float32,
    )
    value_sum = jnp.dot(
        normed,
        lax.all_gather(value_cols, "sp", axis=0, tiled=True),
        preferred_element_type=jnp.float32,
    )
    key = rotate(key_sum[:, None, :], positions)[:, 0, :].astype(jnp.bfloat16)
    value = value_sum.astype(jnp.bfloat16)
    key_value = jnp.concatenate([key, value], axis=1)
    pool_in = jnp.dot(normed, w_pool_in, preferred_element_type=jnp.float32).astype(jnp.bfloat16)
    widened = extended(jnp.concatenate([key_value, pool_in], axis=1), (("sp", 0),), WINDOW)
    kv_wide = widened[:, : 2 * HEAD]
    pool_wide = widened[WINDOW - reach : WINDOW + local_rows + reach, 2 * HEAD :]
    span = QB + 2 * WINDOW
    sink_here = sink_logit[:, None, None]
    results = []
    for block in range(local_rows // QB):
        queries = query[block * QB : (block + 1) * QB]
        keys = kv_wide[block * QB : block * QB + span, :HEAD]
        values = kv_wide[block * QB : block * QB + span, HEAD:]
        scores = jnp.einsum(
            "ihd,jd->hij", queries, keys, preferred_element_type=jnp.float32
        ) * HEAD ** (-0.5)
        query_pos = offset + block * QB + jnp.arange(QB)
        key_pos = offset + block * QB - WINDOW + jnp.arange(span)
        valid = (
            (jnp.abs(query_pos[:, None] - key_pos[None, :]) <= WINDOW)
            & (key_pos[None, :] >= 0)
            & (key_pos[None, :] < seq_total)
        )
        scores = jnp.where(valid, scores, NEG_BIG)
        highest = jnp.maximum(jnp.max(scores, axis=-1, keepdims=True), sink_here)
        expo = jnp.where(valid, jnp.exp(scores - highest), 0.0)
        total = jnp.sum(expo, axis=-1, keepdims=True) + jnp.exp(sink_here - highest)
        weights = (expo / total).astype(jnp.bfloat16)
        result = jnp.einsum("hij,jd->ihd", weights, values, preferred_element_type=jnp.float32)
        results.append(result.reshape(QB, local_heads * HEAD).astype(jnp.bfloat16))
    attended = jnp.concatenate(results, axis=0)
    pool_vals = pool_wide.astype(jnp.float32)
    window_sum = pool_vals
    global_pos = offset + jnp.arange(local_rows)
    channel = tp_place * local_pool + jnp.arange(local_pool)
    window_group = channel // POOL_CH
    measured = jnp.zeros((local_rows, local_pool), jnp.float32)
    stride = 1
    for index, width in enumerate(POOL_SPANS):
        window_sum = window_sum[:-stride] + window_sum[stride:]
        stride = width
        sums = window_sum[reach - width // 2 : reach - width // 2 + local_rows]
        counted = (
            jnp.minimum(global_pos + width // 2, seq_total)
            - jnp.maximum(global_pos - width // 2, 0)
        ).astype(jnp.float32)
        measured = measured + jnp.where(
            window_group[None, :] == index, sums / counted[:, None], 0.0
        )
    pooled = ((measured - pool_vals[reach : reach + local_rows]) * pool_scale).astype(jnp.bfloat16)
    attended_rows, pooled_rows = (
        lax.all_to_all(attended, "tp", split_axis=0, concat_axis=1, tiled=True),
        lax.all_to_all(pooled, "tp", split_axis=0, concat_axis=1, tiled=True),
    )
    joined = jnp.concatenate([attended_rows, pooled_rows], axis=1)
    out_rows_all = lax.all_gather(w_out, "tp", axis=0, tiled=True)
    projected = jnp.dot(
        joined,
        lax.all_gather(out_rows_all, "sp", axis=1, tiled=True),
        preferred_element_type=jnp.float32,
    )
    return projected.astype(jnp.bfloat16)


LANES = 128
CHUNK = 256
VMEM_LIMIT = 60 * 1024 * 1024
MESH = pl.DeviceIdType.MESH


def rope_tables(rows_total):
    half = HEAD // 2
    inverse = np.tile(10000.0 ** (-np.arange(half, dtype=np.float64) / half), LANES // half)[None, :]
    sign = np.where(np.arange(LANES) % HEAD < half, -1.0, 1.0)[None, :]
    inner = np.arange(QB, dtype=np.float64)[:, None] * inverse
    starts = (QB * np.arange(rows_total // QB, dtype=np.float64))[:, None] * inverse
    tables = (np.cos(inner), np.sin(inner) * sign, np.cos(starts), np.sin(starts) * sign)
    return [jnp.asarray(table.astype(np.float32)) for table in tables]


def mixer_kernel(
    places, tokens, gain, w_query, w_key, w_value, w_pool, sink, scale, w_out, cos_in, sin_in, cos_all, sin_all,
    out,
    tok_halo, gain_v, scale_v, sink_v, cos_v, sin_v, tok, wq, wp, wqp, scale_at, shift_at, kv_in, kvw, wfull, qs, kv, pool, pool_send, att_send, joined, acc, cos_at, sin_at,
    tok_sem, own_sem, kv_send, kv_recv, wo_send, wo_recv, wp_recv, halo_send, halo_recv, ex_send, ex_recv,
):
    S, T = places
    Z = S // 4
    s = lax.axis_index("sp")
    t = lax.axis_index("tp")
    rows = tokens.shape[0]
    width = tokens.shape[1]
    blocks = rows // QB
    hb = blocks // 2
    chunks = rows // CHUNK
    local_heads = w_query.shape[1] // HEAD
    groups = w_query.shape[1] // LANES
    pgroups = w_pool.shape[1] // LANES
    reach = POOL_SPANS[-1] // 2
    offset = s * rows
    total_rows = S * rows
    c = s % 2
    y = (s // 2) % 2
    z = s // 4
    partner = s + 1 - 2 * c
    yflip = s + 2 - 4 * y
    after = (s + 1) % S
    before = (s + S - 1) % S
    cross = 1 - t
    far = [d for k in range(1, Z) for d in (k, -k)]

    def remote(a, b, send, recv, to_s, to_t):
        return pltpu.make_async_remote_copy(
            src_ref=a, dst_ref=b, send_sem=send, recv_sem=recv,
            device_id={"sp": to_s, "tp": to_t}, device_id_type=MESH,
        )

    def chunk_at(i):
        return pl.multiple_of(jnp.where(t == 0, chunks - 1 - i, i) * CHUNK, CHUNK)

    def tok_copy(i):
        at = pl.ds(chunk_at(i), CHUNK)
        return pltpu.make_async_copy(tokens.at[at], tok.at[at], tok_sem.at[i])

    own_copies = [
        pltpu.make_async_copy(gain, gain_v, own_sem.at[7]),
        pltpu.make_async_copy(w_key, kv_in.at[0], own_sem.at[0]),
        pltpu.make_async_copy(w_value, kv_in.at[1], own_sem.at[1]),
        pltpu.make_async_copy(w_out, wfull.at[s, t], own_sem.at[2]),
        pltpu.make_async_copy(w_query, wq, own_sem.at[3]),
        pltpu.make_async_copy(w_pool, wp, own_sem.at[4]),
        pltpu.make_async_copy(cos_all.at[pl.ds(pl.multiple_of(s * blocks, blocks), blocks)], cos_at, own_sem.at[5]),
        pltpu.make_async_copy(sin_all.at[pl.ds(pl.multiple_of(s * blocks, blocks), blocks)], sin_at, own_sem.at[6]),
        pltpu.make_async_copy(cos_in, cos_v, own_sem.at[8]),
        pltpu.make_async_copy(sin_in, sin_v, own_sem.at[9]),
        pltpu.make_async_copy(scale, scale_v, own_sem.at[10]),
        pltpu.make_async_copy(sink, sink_v, own_sem.at[11]),
    ]
    barrier = pltpu.get_barrier_semaphore()
    greet = [(((z + d) % Z) * 4 + s % 4, t) for d in range(1, Z)]
    greet += [(yflip, t), (after, t), (before, t), (s, cross), (yflip, cross)]
    for to_s, to_t in greet:
        pl.semaphore_signal(barrier, inc=1, device_id={"sp": to_s, "tp": to_t}, device_id_type=MESH)
    for copy in own_copies[:6]:
        copy.start()
    tok_copy(0).start()
    for copy in own_copies[6:]:
        copy.start()
    for i in range(1, chunks):
        tok_copy(i).start()

    lane = lax.broadcasted_iota(jnp.int32, (QB, LANES), 1)
    low_half = lane < HEAD
    first_half = lane % HEAD < HEAD // 2

    own_copies[0].wait()
    gains = jnp.transpose(jnp.concatenate([gain_v[...]] * (LANES // gain.shape[0]), axis=0))

    def gain_column(b):
        return pltpu.roll(gains, (LANES - b) % LANES, 1)[:, :1]

    own_copies[1].wait()
    own_copies[2].wait()
    key_head = t * local_heads // (QH // KVH)
    key_in = kv_in[0].astype(jnp.float32)
    value_in = kv_in[1].astype(jnp.float32)
    key_cols = jnp.where(key_head == 0, key_in, pltpu.roll(key_in, HEAD, 1))
    value_cols = jnp.where(key_head == 0, pltpu.roll(value_in, HEAD, 1), value_in)
    kvw[s] = (jnp.where(low_half, key_cols, value_cols) * gain_column(s)).astype(jnp.bfloat16)
    own_copies[3].wait()

    def here(d):
        return (z + d >= 0) & (z + d < Z)

    def kv_copy(b, link, to):
        return lambda: remote(kvw.at[b], kvw.at[b], kv_send.at[0], kv_recv.at[link], to, t)

    def kv_wait(link, count):
        some = kvw.at[pl.ds(0, count)]
        remote(some, some, kv_send.at[0], kv_recv.at[link], partner, t).wait_recv()

    def wo_copy(b, half, group, to_s, to_t):
        return lambda: remote(wfull.at[b, half], wfull.at[b, half], wo_send.at[group], wo_recv.at[b // 2, half], to_s, to_t)

    def hand(b, half, group=0):
        return (None, lambda: remote(
            wfull.at[b, half], wfull.at[b, half], wo_send.at[group], wp_recv.at[b // 4], partner, t))

    hop = [2, -2, 1, -1]

    def at_z(d):
        return s + 4 * d

    def at_yz(d):
        return yflip + 4 * d

    def start_all(items):
        for cond, make in items:
            if cond is None:
                make().start()
            else:
                @pl.when(cond)
                def _(make=make):
                    make().start()

    def event(cond, arrival, items):
        def act():
            def inner():
                if arrival is not None:
                    arrival().wait_recv()
                start_all(items)
            if cond is None:
                inner()
            else:
                pl.when(cond)(inner)
        return act

    def onward(d):
        step = -1 if d > 0 else 1
        return step, here(step)

    ev = {}
    ev["kv_own"] = event(None, None,
        [(here(h), kv_copy(s, 0, at_z(h))) for h in far]
        + [(None, kv_copy(s, 1, yflip)), (None, kv_copy(s, 2, partner))])
    kv_to_y = [(here(d), kv_copy(at_z(d), 1, yflip)) for d in far]
    kv_to_p = [(here(d), kv_copy(at_z(d), 2, partner)) for d in far]
    kv_y_to_p = [(None, kv_copy(yflip, 2, partner))] + [(here(d), kv_copy(at_yz(d), 2, partner)) for d in far]

    ev["wo_own"] = event(None, None,
        [(None, wo_copy(s, t, 0, s, cross)), (z > 0, wo_copy(s, t, 0, yflip, t)), hand(s, t, 2)])
    ev["wo_own_y"] = event(None, None, [(z == 0, wo_copy(s, t, 0, yflip, t))])
    ahead = [(h, here(h) & here(2 * h) if abs(h) == 1 else here(h)) for h in hop if abs(h) < Z]
    ends = [(h, here(h) & jnp.logical_not(here(2 * h))) for h in hop if abs(h) == 1]
    ev["wo_own_z"] = event(None, None, [(ok, wo_copy(s, t, 1, at_z(h), t)) for h, ok in ahead])
    ev["wo_own_end"] = event(None, None, [(ok, wo_copy(s, t, 1, at_z(h), t)) for h, ok in ends])
    ev["wo_x"] = event(None, wo_copy(s, cross, 0, yflip, t),
        [(None, wo_copy(s, cross, 0, yflip, t)), hand(s, cross)])
    ev["wo_d"] = event(None, wo_copy(yflip, cross, 0, partner, t),
        [(ok, wo_copy(yflip, cross, 1, at_z(h), t)) for h, ok in ahead] + [hand(yflip, cross)])
    ev["wo_d_end"] = event(None, None, [(ok, wo_copy(yflip, cross, 1, at_z(h), t)) for h, ok in ends])
    for d in far:
        step, fine = onward(d)
        relay = 2 <= abs(d) < Z - 1
        b = at_z(d)
        items = [(None, wo_copy(b, t, 0, s, cross)), (None, wo_copy(b, t, 0, yflip, t)), hand(b, t)]
        if relay:
            items = [(fine, wo_copy(b, t, 1, at_z(step), t))] + items
        ev["w00", d] = event(here(d), wo_copy(b, t, 0, s, cross), items)
        ev["w10", d] = event(here(d), wo_copy(b, cross, 0, partner, t), [hand(b, cross)])
        b = at_yz(d)
        items = [hand(b, cross)]
        if relay:
            items = [(fine, wo_copy(b, cross, 1, at_z(step), t))] + items
        ev["w11", d] = event(here(d), wo_copy(b, cross, 0, partner, t), items)
    for d in [0] + far:
        b = at_yz(d)
        ev["w01", d] = event(None if d == 0 else here(d), wo_copy(b, t, 0, partner, t), [hand(b, t)])

    def poll(kind, *distances):
        for k in distances:
            for d in ((k, -k) if k else (0,)):
                if abs(d) < Z:
                    ev[kind, d]()

    inner = s < S - 1
    outer = s > 0
    halo_tok = [
        (inner, lambda: remote(tokens.at[pl.ds(rows - reach, reach)], tok_halo.at[0], halo_send.at[0], halo_recv.at[0], after, t)),
        (outer, lambda: remote(tokens.at[pl.ds(0, reach)], tok_halo.at[1], halo_send.at[1], halo_recv.at[1], before, t)),
    ]
    halo_kv = [
        (inner, lambda: remote(kv.at[pl.ds(rows, WINDOW)], kv.at[pl.ds(0, WINDOW)], halo_send.at[2], halo_recv.at[2], after, t)),
        (outer, lambda: remote(kv.at[pl.ds(WINDOW, WINDOW)], kv.at[pl.ds(rows + WINDOW, WINDOW)], halo_send.at[3], halo_recv.at[3], before, t)),
    ]

    def halo_wait(pair):
        @pl.when(outer)
        def _():
            pair[0][1]().wait_recv()

        @pl.when(inner)
        def _():
            pair[1][1]().wait_recv()

    @pl.when(s == 0)
    def _():
        tok_halo[0] = jnp.zeros((reach, width), jnp.bfloat16)
        kv[0:WINDOW, :] = jnp.zeros((WINDOW, LANES), jnp.bfloat16)

    @pl.when(s == S - 1)
    def _():
        tok_halo[1] = jnp.zeros((reach, width), jnp.bfloat16)
        kv[rows + WINDOW:rows + 2 * WINDOW, :] = jnp.zeros((WINDOW, LANES), jnp.bfloat16)

    def begin():
        pl.semaphore_wait(barrier, len(greet))
        ev["kv_own"]()
        start_all(halo_tok)
        ev["wo_own"]()

    late = z > 0

    @pl.when(late)
    def _():
        begin()

    def rotated(values, b):
        ca = cos_at[pl.ds(b, 1), :]
        sa = sin_at[pl.ds(b, 1), :]
        ci = cos_v[...]
        si = sin_v[...]
        cosine = ca * ci - sa * si
        sine = sa * ci + ca * si
        swapped = jnp.where(
            first_half,
            pltpu.roll(values, LANES - HEAD // 2, 1),
            pltpu.roll(values, HEAD // 2, 1),
        )
        return values * cosine + swapped * sine

    for copy in own_copies[4:6]:
        copy.wait()
    wide = w_query.shape[1]

    def fold(b, carry):
        at = pl.ds(pl.multiple_of(b * LANES, LANES), LANES)
        column = gain_column(b)
        sums = []
        for k, part in enumerate((wq, wp)):
            scaled = (part[at, :].astype(jnp.float32) * column).astype(jnp.bfloat16)
            wqp[at, k * wide:(k + 1) * wide] = scaled
            sums.append(jnp.sum(scaled.astype(jnp.float32).reshape(LANES // 8, 8, wide), axis=0))
        return carry + jnp.concatenate(sums, axis=1)

    folded = lax.fori_loop(0, width // LANES, fold, jnp.zeros((8, 2 * wide), jnp.float32), unroll=2)
    total_qp = jnp.sum(folded, axis=0, keepdims=True)

    for copy in own_copies[6:]:
        copy.wait()
    LN = 16
    hc = chunks // 2

    def pooled(b, g):
        cols = slice(g * LANES, (g + 1) * LANES)
        length = QB + 2 * reach
        values = pool[pl.ds(pl.multiple_of(b * QB, QB), length), cols]
        index = (t * (pgroups * LANES) + g * LANES) // POOL_CH
        running = values
        stride = 1
        picked = jnp.zeros((QB, LANES), jnp.float32)
        wide = 0
        for k, span in enumerate(POOL_SPANS):
            running = running + pltpu.roll(running, length - stride, 0)
            stride = span
            shift = reach - span // 2
            sums = (pltpu.roll(running, length - shift, 0) if shift else running)[:QB]
            picked = jnp.where(index == k, sums, picked)
            wide = jnp.where(index == k, span // 2, wide)
        pos = offset + b * QB + lax.broadcasted_iota(jnp.int32, (QB, LANES), 0)
        counted = (jnp.minimum(pos + wide, total_rows) - jnp.maximum(pos - wide, 0)).astype(jnp.float32)
        return ((picked / counted - values[reach:reach + QB]) * scale_v[:, cols]).astype(jnp.bfloat16)


    def ex_pool(n):
        at = pl.ds(pl.multiple_of(n * QB, QB), QB)
        return remote(pool_send.at[at], joined.at[T + t, at], ex_send.at[0], ex_recv.at[0], s, cross)

    def ex_att(n):
        at = pl.ds(pl.multiple_of(n * QB, QB), QB)
        return remote(att_send.at[at], joined.at[t, at], ex_send.at[1], ex_recv.at[1], s, cross)

    def send_pooled(n):
        for g in range(pgroups):
            pool_send[pl.ds(pl.multiple_of(n * QB, QB), QB), g * LANES:(g + 1) * LANES] = pooled(cross * hb + n, g)
        ex_pool(n).start()

    def moments(rows_in):
        values = rows_in.astype(jnp.float32)
        center = jnp.sum(values, axis=1, keepdims=True) * (1.0 / width)
        moved = values - center
        spread = jnp.sum(moved * moved, axis=1, keepdims=True) * (1.0 / width)
        inverse = lax.rsqrt(spread + 1e-06)
        return inverse, center * inverse

    def project(i, carry):
        base = chunk_at(i)
        tok_copy(i).wait()
        raw = jnp.dot(tok[pl.ds(base, CHUNK), :], wqp[...], preferred_element_type=jnp.float32)
        scales = []
        shifts = []
        for r in range(CHUNK // LN):
            at = pl.ds(pl.multiple_of(base + r * LN, LN), LN)
            inverse, shifted = moments(tok[at, :])
            scales.append(inverse)
            shifts.append(shifted)
        rstd = jnp.broadcast_to(jnp.concatenate(scales, axis=0), (CHUNK, LANES))
        drop = jnp.broadcast_to(jnp.concatenate(shifts, axis=0), (CHUNK, LANES))
        scale_at[pl.ds(base, CHUNK), :] = rstd
        shift_at[pl.ds(base, CHUNK), :] = drop

        def normal(k, g):
            at = slice(k * QB, (k + 1) * QB)
            cols = slice(g * LANES, (g + 1) * LANES)
            return raw[at, cols] * rstd[at] - drop[at] * total_qp[:, cols]

        for k in range(CHUNK // QB):
            b = base // QB + k
            for g in range(groups):
                turned = rotated(normal(k, g), b) * HEAD ** (-0.5)
                qs[b, pl.ds(2 * g * QB, QB), :] = jnp.where(low_half, turned, 0.0).astype(jnp.bfloat16)
                qs[b, pl.ds((2 * g + 1) * QB, QB), :] = jnp.where(
                    low_half, pltpu.roll(turned, HEAD, 1), 0.0
                ).astype(jnp.bfloat16)
            for g in range(pgroups):
                pool[pl.ds(pl.multiple_of(reach + base + k * QB, 8), QB), g * LANES:(g + 1) * LANES] = (
                    normal(k, groups + g).astype(jnp.bfloat16).astype(jnp.float32)
                )

        @pl.when((i == 0) & (z == 0))
        def _():
            begin()

        @pl.when(i == jnp.where(z == 0, 1, 0))
        def _():
            ev["wo_own_z"]()

        @pl.when(i == hc - 1)
        def _():
            for n in range(1, hb - 1):
                send_pooled(n)

        @pl.when(i == hc)
        def _():
            send_pooled(jnp.where(t == 0, 0, hb - 1))
            kv_wait(0, Z - 1)
            start_all(kv_to_y)
            start_all(kv_to_p)
            ev["wo_own_end"]()

        @pl.when(i == jnp.where(z == 0, chunks - 1, hc))
        def _():
            ev["wo_x"]()
            ev["wo_own_y"]()

        return carry

    lax.fori_loop(0, chunks, project, 0)

    halo_wait(halo_tok)
    edge = jnp.concatenate([tok_halo[0], tok_halo[1]], axis=0)
    edge_scale, edge_shift = moments(edge)
    edge_pool = (
        jnp.dot(edge, wqp[:, wide:], preferred_element_type=jnp.float32) * edge_scale - edge_shift * total_qp[:, wide:]
    ).astype(jnp.bfloat16).astype(jnp.float32)
    pool[0:reach, :] = edge_pool[:reach]
    pool[rows + reach:rows + 2 * reach, :] = edge_pool[reach:]

    def pool_own(i, carry):
        n = jnp.where(t == 0, i, hb - 1 - i)
        for g in range(pgroups):
            joined[T + t, pl.ds(pl.multiple_of(n * QB, QB), QB), g * LANES:(g + 1) * LANES] = pooled(t * hb + n, g)
        return carry

    send_pooled(jnp.where(t == 0, hb - 1, 0))
    lax.fori_loop(0, hb, pool_own, 0)
    kv_wait(1, Z)
    start_all(kv_y_to_p)
    kv_wait(2, 2 * Z)

    def gather_sum(b, carry):
        return carry + jnp.sum(kvw[b].astype(jnp.float32).reshape(LANES // 8, 8, LANES), axis=0)

    total_kv = jnp.sum(
        lax.fori_loop(0, S, gather_sum, jnp.zeros((8, LANES), jnp.float32), unroll=4), axis=0, keepdims=True
    )

    def key_value(i):
        base = i * CHUNK
        both = jnp.dot(
            tok[pl.ds(base, CHUNK), :], kvw[...].reshape(width, LANES), preferred_element_type=jnp.float32
        )
        both = both * scale_at[pl.ds(base, CHUNK), :] - shift_at[pl.ds(base, CHUNK), :] * total_kv
        for k in range(CHUNK // QB):
            piece = both[k * QB:(k + 1) * QB, :]
            turned = rotated(piece, i * (CHUNK // QB) + k)
            kv[pl.ds(WINDOW + base + k * QB, QB), :] = jnp.where(low_half, turned, piece).astype(jnp.bfloat16)

    key_value(0)
    key_value(chunks - 1)
    start_all(halo_kv)
    poll("w00", 2)
    ev["wo_d"]()
    poll("w00", 1)
    for i in range(1, chunks - 1):
        key_value(i)
    ev["wo_d_end"]()

    span = QB + 2 * WINDOW
    row_id = lax.broadcasted_iota(jnp.int32, (QB, span), 0)
    col_id = lax.broadcasted_iota(jnp.int32, (QB, span), 1)

    def attend(b):
        context = kv[pl.ds(pl.multiple_of(b * QB, QB), span), :]
        scores = lax.dot_general(
            qs[b], context, (((1,), (1,)), ((), ())), preferred_element_type=jnp.float32
        )
        start = offset + b * QB
        lowest = jnp.maximum(row_id, WINDOW - start)
        highest_col = jnp.minimum(row_id + 2 * WINDOW, total_rows - 1 - start + WINDOW)
        valid = (col_id >= lowest) & (col_id <= highest_col)
        expos = []
        norms = []
        for h in range(local_heads):
            part = jnp.where(valid, scores[h * QB:(h + 1) * QB], NEG_BIG)
            top = jnp.maximum(jnp.max(part, axis=1, keepdims=True), sink_v[h])
            expo = jnp.exp(part - top)
            norms.append(1.0 / (jnp.sum(expo, axis=1, keepdims=True) + jnp.exp(sink_v[h] - top)))
            expos.append(expo.astype(jnp.bfloat16))
        result = jnp.dot(jnp.concatenate(expos, axis=0), context, preferred_element_type=jnp.float32)
        heads = [result[h * QB:(h + 1) * QB] * norms[h] for h in range(local_heads)]
        return [
            jnp.where(low_half, pltpu.roll(heads[2 * g], HEAD, 1), heads[2 * g + 1]).astype(jnp.bfloat16)
            for g in range(groups)
        ]


    def attend_other(i, carry):
        @pl.when(i == hb - 1)
        def _():
            halo_wait(halo_kv)
        b = jnp.where(t == 0, hb + i, hb - 1 - i)
        n = b - cross * hb
        at = pl.multiple_of(n * QB, QB)
        for g, value in enumerate(attend(b)):
            att_send[pl.ds(at, QB), g * LANES:(g + 1) * LANES] = value
        ex_att(n).start()

        return carry

    def attend_own(i, carry):
        b = jnp.where(t == 0, hb - 1 - i, hb + i)
        at = pl.multiple_of((b - t * hb) * QB, QB)
        for g, value in enumerate(attend(b)):
            joined[t, pl.ds(at, QB), g * LANES:(g + 1) * LANES] = value

        @pl.when(i == 0)
        def _():
            poll("w00", *range(3, Z))

        @pl.when(i == 2)
        def _():
            poll("w01", 0)
            poll("w11", 2)

        return carry

    lax.fori_loop(0, hb, attend_other, 0)
    lax.fori_loop(0, hb, attend_own, 0)
    whole_pool = remote(pool_send, joined.at[T + cross], ex_send.at[0], ex_recv.at[0], s, cross)
    whole_att = remote(att_send, joined.at[cross], ex_send.at[1], ex_recv.at[1], s, cross)
    whole_pool.wait_recv()

    def columns(n, half, start, count):
        at = pl.ds(pl.multiple_of(start, wide), count)
        return jnp.concatenate([wfull[2 * n, half, at, :], wfull[2 * n + 1, half, at, :]], axis=1)

    def pair_of(p):
        zz = jnp.where(z < Z // 2, (z + p) % Z, (z + Z - p) % Z)
        return [zz * 2 + y, zz * 2 + 1 - y]

    def pair_wait(pair):
        some = wfull.at[pl.ds(0, 2)]
        remote(some, some, wo_send.at[2], wp_recv.at[pair[0] // 2], partner, t).wait_recv()

    def pair_columns(pair, half, start, count):
        return jnp.concatenate([columns(n, half, start, count) for n in pair], axis=1)

    def store(n, total):
        out[:, pl.ds(pl.multiple_of(n * 2 * LANES, 2 * LANES), 2 * LANES)] = total.astype(jnp.bfloat16)

    def most(p, carry):
        @pl.when(p == 1)
        def _():
            poll("w10", 1)
            poll("w11", 1)
            poll("w01", 1)
        pair = pair_of(p)
        pair_wait(pair)
        left = jnp.concatenate([joined[t]] + [joined[T + k] for k in range(T)], axis=1)
        right = jnp.concatenate([pair_columns(pair, 0, t * wide, wide), pair_columns(pair, 1, 0, T * wide)], axis=0)
        total = jnp.dot(left, right, preferred_element_type=jnp.float32)
        acc[pair[0]] = total[:, :2 * LANES]
        acc[pair[1]] = total[:, 2 * LANES:]
        return carry

    def last(p, carry):
        pair = pair_of(p)
        total = jnp.dot(
            joined[cross], pair_columns(pair, 0, cross * wide, wide), preferred_element_type=jnp.float32
        )
        store(pair[0], acc[pair[0]] + total[:, :2 * LANES])
        store(pair[1], acc[pair[1]] + total[:, 2 * LANES:])
        return carry

    def whole(p, carry):
        @pl.when(p == split)
        def _():
            poll("w10", *range(3, Z))
            poll("w11", *range(3, Z))
        pair = pair_of(p)
        pair_wait(pair)
        left = jnp.concatenate([joined[k] for k in range(2 * T)], axis=1)
        right = jnp.concatenate([pair_columns(pair, half, 0, T * wide) for half in range(T)], axis=0)
        total = jnp.dot(left, right, preferred_element_type=jnp.float32)
        store(pair[0], total[:, :2 * LANES])
        store(pair[1], total[:, 2 * LANES:])
        return carry

    split = Z // 2
    lax.fori_loop(0, split, most, 0)
    poll("w01", *range(2, Z))
    poll("w10", 2)
    whole_att.wait_recv()
    lax.fori_loop(0, split, last, 0)
    lax.fori_loop(split, Z, whole, 0)

    def sent(ref, sem):
        remote(ref, ref, sem, halo_recv.at[0], partner, t).wait_send()

    for cond, make in halo_tok + halo_kv:
        @pl.when(cond)
        def _(make=make):
            make().wait_send()
    whole_pool.wait_send()
    whole_att.wait_send()
    sent(kvw.at[pl.ds(0, 4 * Z - 1)], kv_send.at[0])
    sent(wfull.at[s, t], wo_send.at[2])
    sent(wfull.at[pl.ds(0, 3 * Z)], wo_send.at[0])
    for at in range(Z):
        inside = lambda k: 0 <= k < Z
        count = sum(inside(at + h) for h in hop)
        count += sum(inside(at + d) and inside(at - d // abs(d)) for d in far if 2 <= abs(d) < Z - 1)

        @pl.when(z == at)
        def _(count=count):
            sent(wfull.at[pl.ds(0, count)], wo_send.at[1])


def body(mesh, tokens, norm_gain, w_query, w_key, w_value, w_pool_in, sink_logit, pool_scale, w_out):
    S = lax.axis_size("sp")
    T = lax.axis_size("tp")
    rows, width = tokens.shape
    local_heads = w_query.shape[1] // HEAD
    fits = (
        S % 4 == 0 and S > 4 and T == 2
        and w_out.shape[1] == LANES and w_key.shape == (LANES, LANES) and w_value.shape == w_key.shape
        and w_query.shape[1] % LANES == 0 and w_pool_in.shape[1] % LANES == 0
        and w_query.shape[1] == w_pool_in.shape[1]
        and local_heads == QH // KVH and rows % (2 * CHUNK) == 0
        and width == S * LANES and LANES % S == 0
    )
    if not fits:
        return plain_body(
            tokens, norm_gain, w_query, w_key, w_value, w_pool_in, sink_logit, pool_scale, w_out
        )
    tables = rope_tables(S * rows)
    blocks = rows // QB
    half = rows // T
    Z = S // 4
    reach = POOL_SPANS[-1] // 2
    wide = w_query.shape[1]
    vmem = pl.BlockSpec(memory_space=pltpu.VMEM)
    hbm = pl.BlockSpec(memory_space=pltpu.HBM)
    dma = pltpu.SemaphoreType.DMA
    bf = jnp.bfloat16
    return pl.pallas_call(
        functools.partial(mixer_kernel, (S, T)),
        out_shape=pltpu.VMEM((half, S * w_out.shape[1]), bf),
        in_specs=[hbm] * 13,
        out_specs=vmem,
        scratch_shapes=[
            pltpu.VMEM((2, reach, width), bf),
            pltpu.VMEM((width // LANES, LANES), jnp.float32),
            pltpu.VMEM((1, wide), jnp.float32),
            pltpu.SMEM(sink_logit.shape, jnp.float32),
            pltpu.VMEM((QB, LANES), jnp.float32),
            pltpu.VMEM((QB, LANES), jnp.float32),
            pltpu.VMEM((rows, width), bf),
            pltpu.VMEM(w_query.shape, bf),
            pltpu.VMEM(w_pool_in.shape, bf),
            pltpu.VMEM((width, 2 * wide), bf),
            pltpu.VMEM((rows, LANES), jnp.float32),
            pltpu.VMEM((rows, LANES), jnp.float32),
            pltpu.VMEM((2,) + w_key.shape, bf),
            pltpu.VMEM((S, LANES, LANES), bf),
            pltpu.VMEM((S, T) + w_out.shape, bf),
            pltpu.VMEM((blocks, local_heads * QB, LANES), bf),
            pltpu.VMEM((rows + 2 * WINDOW, LANES), bf),
            pltpu.VMEM((rows + 2 * reach, wide), jnp.float32),
            pltpu.VMEM((half, wide), bf),
            pltpu.VMEM((half, wide), bf),
            pltpu.VMEM((2 * T, half, wide), bf),
            pltpu.VMEM((S // 2, half, 2 * LANES), jnp.float32),
            pltpu.VMEM((blocks, LANES), jnp.float32),
            pltpu.VMEM((blocks, LANES), jnp.float32),
            dma((rows // CHUNK,)),
            dma((12,)),
            dma((1,)),
            dma((3,)),
            dma((3,)),
            dma((S // 2, T)),
            dma((Z,)),
            dma((4,)),
            dma((4,)),
            dma((2,)),
            dma((2,)),
        ],
        compiler_params=pltpu.CompilerParams(
            collective_id=0, has_side_effects=True, vmem_limit_bytes=VMEM_LIMIT
        ),
    )(
        tokens, norm_gain.reshape(width // LANES, LANES), w_query, w_key, w_value, w_pool_in, sink_logit, pool_scale[None, :], w_out, *tables
    )


def solution(mesh):
    in_specs = (
        P("sp", None),
        P(),
        P(None, "tp"),
        P("sp", None),
        P("sp", None),
        P(None, "tp"),
        P("tp"),
        P("tp"),
        P("tp", "sp"),
    )
    out_specs = P(("sp", "tp"), None)
    return jax.shard_map(functools.partial(body, mesh), mesh=mesh, in_specs=in_specs, out_specs=out_specs, check_vma=False)
```

```python
import functools

import jax
import jax.numpy as jnp
import numpy as np
from jax import lax
from jax.experimental import pallas as pl
from jax.experimental.pallas import tpu as pltpu
from jax.sharding import PartitionSpec as P

HEAD = 64
QH = 8
KVH = 2
POOL_CH = 128
WINDOW = 128
QB = 128


NEG_BIG = -1e30
POOL_SPANS = (2, 4, 8, 16)


def extended(block, sides, width):
    for axis, dim in sides:
        count = lax.axis_size(axis)
        forward = [(i, i + 1) for i in range(count - 1)]
        backward = [(target, source) for source, target in forward]
        low = lax.ppermute(
            lax.slice_in_dim(block, block.shape[dim] - width, None, axis=dim), axis, forward
        )
        high = lax.ppermute(lax.slice_in_dim(block, 0, width, axis=dim), axis, backward)
        block = jnp.concatenate([low, block, high], axis=dim)
    return block


def layer_normed(tokens, norm_gain):
    values = tokens.astype(jnp.float32)
    center = jnp.mean(values, axis=-1, keepdims=True)
    spread = jnp.mean(jnp.square(values - center), axis=-1, keepdims=True)
    return ((values - center) * lax.rsqrt(spread + 1e-06) * norm_gain).astype(jnp.bfloat16)


def rotate(values, positions):
    half = HEAD // 2
    inverse = 10000.0 ** (-jnp.arange(half, dtype=jnp.float32) / half)
    angles = positions[:, None] * inverse[None, :]
    cosine = jnp.cos(angles)[:, None, :]
    sine = jnp.sin(angles)[:, None, :]
    first = values[..., :half]
    second = values[..., half:]
    return jnp.concatenate(
        [first * cosine - second * sine, first * sine + second * cosine], axis=-1
    )


def plain_body(tokens, norm_gain, w_query, w_key, w_value, w_pool_in, sink_logit, pool_scale, w_out):
    local_rows = tokens.shape[0]
    seq_total = local_rows * lax.axis_size("sp")
    offset = lax.axis_index("sp") * local_rows
    tp_place = lax.axis_index("tp")
    local_heads = w_query.shape[1] // HEAD
    local_pool = w_pool_in.shape[1]
    reach = POOL_SPANS[-1] // 2
    normed = layer_normed(tokens, norm_gain)
    positions = (offset + jnp.arange(local_rows)).astype(jnp.float32)
    query = rotate(
        jnp.dot(normed, w_query, preferred_element_type=jnp.float32).reshape(
            local_rows, local_heads, HEAD
        ),
        positions,
    ).astype(jnp.bfloat16)
    key_head = tp_place * local_heads // (QH // KVH)
    key_cols = lax.dynamic_slice_in_dim(w_key, key_head * HEAD, HEAD, 1)
    value_cols = lax.dynamic_slice_in_dim(w_value, key_head * HEAD, HEAD, 1)
    key_sum = jnp.dot(
        normed,
        lax.all_gather(key_cols, "sp", axis=0, tiled=True),
        preferred_element_type=jnp.float32,
    )
    value_sum = jnp.dot(
        normed,
        lax.all_gather(value_cols, "sp", axis=0, tiled=True),
        preferred_element_type=jnp.float32,
    )
    key = rotate(key_sum[:, None, :], positions)[:, 0, :].astype(jnp.bfloat16)
    value = value_sum.astype(jnp.bfloat16)
    key_value = jnp.concatenate([key, value], axis=1)
    pool_in = jnp.dot(normed, w_pool_in, preferred_element_type=jnp.float32).astype(jnp.bfloat16)
    widened = extended(jnp.concatenate([key_value, pool_in], axis=1), (("sp", 0),), WINDOW)
    kv_wide = widened[:, : 2 * HEAD]
    pool_wide = widened[WINDOW - reach : WINDOW + local_rows + reach, 2 * HEAD :]
    span = QB + 2 * WINDOW
    sink_here = sink_logit[:, None, None]
    results = []
    for block in range(local_rows // QB):
        queries = query[block * QB : (block + 1) * QB]
        keys = kv_wide[block * QB : block * QB + span, :HEAD]
        values = kv_wide[block * QB : block * QB + span, HEAD:]
        scores = jnp.einsum(
            "ihd,jd->hij", queries, keys, preferred_element_type=jnp.float32
        ) * HEAD ** (-0.5)
        query_pos = offset + block * QB + jnp.arange(QB)
        key_pos = offset + block * QB - WINDOW + jnp.arange(span)
        valid = (
            (jnp.abs(query_pos[:, None] - key_pos[None, :]) <= WINDOW)
            & (key_pos[None, :] >= 0)
            & (key_pos[None, :] < seq_total)
        )
        scores = jnp.where(valid, scores, NEG_BIG)
        highest = jnp.maximum(jnp.max(scores, axis=-1, keepdims=True), sink_here)
        expo = jnp.where(valid, jnp.exp(scores - highest), 0.0)
        total = jnp.sum(expo, axis=-1, keepdims=True) + jnp.exp(sink_here - highest)
        weights = (expo / total).astype(jnp.bfloat16)
        result = jnp.einsum("hij,jd->ihd", weights, values, preferred_element_type=jnp.float32)
        results.append(result.reshape(QB, local_heads * HEAD).astype(jnp.bfloat16))
    attended = jnp.concatenate(results, axis=0)
    pool_vals = pool_wide.astype(jnp.float32)
    window_sum = pool_vals
    global_pos = offset + jnp.arange(local_rows)
    channel = tp_place * local_pool + jnp.arange(local_pool)
    window_group = channel // POOL_CH
    measured = jnp.zeros((local_rows, local_pool), jnp.float32)
    stride = 1
    for index, width in enumerate(POOL_SPANS):
        window_sum = window_sum[:-stride] + window_sum[stride:]
        stride = width
        sums = window_sum[reach - width // 2 : reach - width // 2 + local_rows]
        counted = (
            jnp.minimum(global_pos + width // 2, seq_total)
            - jnp.maximum(global_pos - width // 2, 0)
        ).astype(jnp.float32)
        measured = measured + jnp.where(
            window_group[None, :] == index, sums / counted[:, None], 0.0
        )
    pooled = ((measured - pool_vals[reach : reach + local_rows]) * pool_scale).astype(jnp.bfloat16)
    attended_rows, pooled_rows = (
        lax.all_to_all(attended, "tp", split_axis=0, concat_axis=1, tiled=True),
        lax.all_to_all(pooled, "tp", split_axis=0, concat_axis=1, tiled=True),
    )
    joined = jnp.concatenate([attended_rows, pooled_rows], axis=1)
    out_rows_all = lax.all_gather(w_out, "tp", axis=0, tiled=True)
    projected = jnp.dot(
        joined,
        lax.all_gather(out_rows_all, "sp", axis=1, tiled=True),
        preferred_element_type=jnp.float32,
    )
    return projected.astype(jnp.bfloat16)


LANES = 128
CHUNK = 256
VMEM_LIMIT = 60 * 1024 * 1024
MESH = pl.DeviceIdType.MESH


def rope_tables(rows_total):
    half = HEAD // 2
    inverse = np.tile(10000.0 ** (-np.arange(half, dtype=np.float64) / half), LANES // half)[None, :]
    sign = np.where(np.arange(LANES) % HEAD < half, -1.0, 1.0)[None, :]
    inner = np.arange(QB, dtype=np.float64)[:, None] * inverse
    starts = (QB * np.arange(rows_total // QB, dtype=np.float64))[:, None] * inverse
    tables = (np.cos(inner), np.sin(inner) * sign, np.cos(starts), np.sin(starts) * sign)
    return [jnp.asarray(table.astype(np.float32)) for table in tables]


def mixer_kernel(
    places, tokens, gain, w_query, w_key, w_value, w_pool, sink, scale, w_out, cos_in, sin_in, cos_all, sin_all,
    out,
    tok_halo, gain_v, scale_v, sink_v, cos_v, sin_v, tok, wq, wp, wqp, scale_at, shift_at, kv_in, kvw, wfull, qs, kv, pool, pool_send, att_send, joined, acc, cos_at, sin_at,
    tok_sem, own_sem, kv_send, kv_recv, wo_send, wo_recv, wp_recv, halo_send, halo_recv, ex_send, ex_recv,
):
    S, T = places
    Z = S // 4
    s = lax.axis_index("sp")
    t = lax.axis_index("tp")
    rows = tokens.shape[0]
    width = tokens.shape[1]
    blocks = rows // QB
    hb = blocks // 2
    chunks = rows // CHUNK
    local_heads = w_query.shape[1] // HEAD
    groups = w_query.shape[1] // LANES
    pgroups = w_pool.shape[1] // LANES
    reach = POOL_SPANS[-1] // 2
    offset = s * rows
    total_rows = S * rows
    c = s % 2
    y = (s // 2) % 2
    z = s // 4
    partner = s + 1 - 2 * c
    yflip = s + 2 - 4 * y
    after = (s + 1) % S
    before = (s + S - 1) % S
    cross = 1 - t
    far = [d for k in range(1, Z) for d in (k, -k)]

    def remote(a, b, send, recv, to_s, to_t):
        return pltpu.make_async_remote_copy(
            src_ref=a, dst_ref=b, send_sem=send, recv_sem=recv,
            device_id={"sp": to_s, "tp": to_t}, device_id_type=MESH,
        )

    def chunk_at(i):
        return pl.multiple_of(jnp.where(t == 0, chunks - 1 - i, i) * CHUNK, CHUNK)

    def tok_copy(i):
        at = pl.ds(chunk_at(i), CHUNK)
        return pltpu.make_async_copy(tokens.at[at], tok.at[at], tok_sem.at[i])

    own_copies = [
        pltpu.make_async_copy(gain, gain_v, own_sem.at[7]),
        pltpu.make_async_copy(w_key, kv_in.at[0], own_sem.at[0]),
        pltpu.make_async_copy(w_value, kv_in.at[1], own_sem.at[1]),
        pltpu.make_async_copy(w_out, wfull.at[s, t], own_sem.at[2]),
        pltpu.make_async_copy(w_query, wq, own_sem.at[3]),
        pltpu.make_async_copy(w_pool, wp, own_sem.at[4]),
        pltpu.make_async_copy(cos_all.at[pl.ds(pl.multiple_of(s * blocks, blocks), blocks)], cos_at, own_sem.at[5]),
        pltpu.make_async_copy(sin_all.at[pl.ds(pl.multiple_of(s * blocks, blocks), blocks)], sin_at, own_sem.at[6]),
        pltpu.make_async_copy(cos_in, cos_v, own_sem.at[8]),
        pltpu.make_async_copy(sin_in, sin_v, own_sem.at[9]),
        pltpu.make_async_copy(scale, scale_v, own_sem.at[10]),
        pltpu.make_async_copy(sink, sink_v, own_sem.at[11]),
    ]
    barrier = pltpu.get_barrier_semaphore()
    greet = [(((z + d) % Z) * 4 + s % 4, t) for d in range(1, Z)]
    greet += [(yflip, t), (after, t), (before, t), (s, cross), (yflip, cross)]
    for to_s, to_t in greet:
        pl.semaphore_signal(barrier, inc=1, device_id={"sp": to_s, "tp": to_t}, device_id_type=MESH)
    for copy in own_copies[:6]:
        copy.start()
    tok_copy(0).start()
    for copy in own_copies[6:]:
        copy.start()
    for i in range(1, chunks):
        tok_copy(i).start()

    lane = lax.broadcasted_iota(jnp.int32, (QB, LANES), 1)
    low_half = lane < HEAD
    first_half = lane % HEAD < HEAD // 2

    own_copies[0].wait()
    gains = jnp.transpose(jnp.concatenate([gain_v[...]] * (LANES // gain.shape[0]), axis=0))

    def gain_column(b):
        return pltpu.roll(gains, (LANES - b) % LANES, 1)[:, :1]

    own_copies[1].wait()
    own_copies[2].wait()
    key_head = t * local_heads // (QH // KVH)
    key_in = kv_in[0].astype(jnp.float32)
    value_in = kv_in[1].astype(jnp.float32)
    key_cols = jnp.where(key_head == 0, key_in, pltpu.roll(key_in, HEAD, 1))
    value_cols = jnp.where(key_head == 0, pltpu.roll(value_in, HEAD, 1), value_in)
    kvw[s] = (jnp.where(low_half, key_cols, value_cols) * gain_column(s)).astype(jnp.bfloat16)
    own_copies[3].wait()

    def here(d):
        return (z + d >= 0) & (z + d < Z)

    def kv_copy(b, link, to):
        return lambda: remote(kvw.at[b], kvw.at[b], kv_send.at[0], kv_recv.at[link], to, t)

    def kv_wait(link, count):
        some = kvw.at[pl.ds(0, count)]
        remote(some, some, kv_send.at[0], kv_recv.at[link], partner, t).wait_recv()

    def wo_copy(b, half, group, to_s, to_t):
        return lambda: remote(wfull.at[b, half], wfull.at[b, half], wo_send.at[group], wo_recv.at[b // 2, half], to_s, to_t)

    def hand(b, half, group=0):
        return (None, lambda: remote(
            wfull.at[b, half], wfull.at[b, half], wo_send.at[group], wp_recv.at[b // 4], partner, t))

    hop = [2, -2, 1, -1]

    def at_z(d):
        return s + 4 * d

    def at_yz(d):
        return yflip + 4 * d

    def start_all(items):
        for cond, make in items:
            if cond is None:
                make().start()
            else:
                @pl.when(cond)
                def _(make=make):
                    make().start()

    def event(cond, arrival, items):
        def act():
            def inner():
                if arrival is not None:
                    arrival().wait_recv()
                start_all(items)
            if cond is None:
                inner()
            else:
                pl.when(cond)(inner)
        return act

    def onward(d):
        step = -1 if d > 0 else 1
        return step, here(step)

    ev = {}
    ev["kv_own"] = event(None, None,
        [(here(h), kv_copy(s, 0, at_z(h))) for h in far]
        + [(None, kv_copy(s, 1, yflip)), (None, kv_copy(s, 2, partner))])
    kv_to_y = [(here(d), kv_copy(at_z(d), 1, yflip)) for d in far]
    kv_to_p = [(here(d), kv_copy(at_z(d), 2, partner)) for d in far]
    kv_y_to_p = [(None, kv_copy(yflip, 2, partner))] + [(here(d), kv_copy(at_yz(d), 2, partner)) for d in far]

    ev["wo_own"] = event(None, None,
        [(None, wo_copy(s, t, 2, s, cross)), (z > 0, wo_copy(s, t, 0, yflip, t)), hand(s, t, 2)])
    ev["wo_own_y"] = event(None, None, [(z == 0, wo_copy(s, t, 0, yflip, t))])
    ahead = [(h, here(h) & here(2 * h) if abs(h) == 1 else here(h)) for h in hop if abs(h) < Z]
    ends = [(h, here(h) & jnp.logical_not(here(2 * h))) for h in hop if abs(h) == 1]
    ev["wo_own_z"] = event(None, None, [(ok, wo_copy(s, t, 1, at_z(h), t)) for h, ok in ahead])
    ev["wo_own_end"] = event(None, None, [(ok, wo_copy(s, t, 1, at_z(h), t)) for h, ok in ends])
    def rim(d):
        return here(d) & ((z == 0) | (z == Z - 1) | (z + d == 0) | (z + d == Z - 1))

    ev["wo_x"] = event(None, wo_copy(s, cross, 0, yflip, t),
        [(None, wo_copy(s, cross, 0, yflip, t)), hand(s, cross)]
        + [(rim(h), wo_copy(s, cross, 1, at_z(h), t)) for h in (1, -1)])
    ev["wo_d"] = event(None, wo_copy(yflip, cross, 0, partner, t),
        [(ok, wo_copy(yflip, cross, 1, at_z(h), t)) for h, ok in ahead] + [hand(yflip, cross)])
    def split_event(kind, d, arrival, items, at_rim=(), inner_only=()):
        if abs(d) == 1:
            ev[kind + "r", d] = event(rim(d), arrival, list(at_rim) + items)
            ev[kind, d] = event(here(d) & jnp.logical_not(rim(d)), arrival, list(inner_only) + items)
        else:
            ev[kind, d] = event(None if d == 0 else here(d), arrival, list(inner_only) + items)

    for d in far:
        step, fine = onward(d)
        relay = 2 <= abs(d) < Z - 1
        b = at_z(d)
        to_x = [(None, wo_copy(b, t, 0, s, cross))]
        items = [(None, wo_copy(b, t, 0, yflip, t)), hand(b, t)]
        if relay:
            to_x = [(fine, wo_copy(b, t, 1, at_z(step), t))] + to_x
        split_event("w00", d, wo_copy(b, t, 0, s, cross), items, inner_only=to_x)
        split_event("w10", d, wo_copy(b, cross, 0, partner, t), [hand(b, cross)],
            [((z == 0) | (z == Z - 1), wo_copy(b, cross, 1, yflip, t))])
        b = at_yz(d)
        items = [hand(b, cross)]
        if relay:
            items = [(fine, wo_copy(b, cross, 1, at_z(step), t))] + items
        split_event("w11", d, wo_copy(b, cross, 0, partner, t), items)
    for d in [0] + far:
        b = at_yz(d)
        split_event("w01", d, wo_copy(b, t, 0, partner, t), [hand(b, t)])

    def poll(kind, *distances):
        for k in distances:
            for d in ((k, -k) if k else (0,)):
                if abs(d) < Z:
                    ev[kind, d]()

    inner = s < S - 1
    outer = s > 0
    halo_tok = [
        (inner, lambda: remote(tokens.at[pl.ds(rows - reach, reach)], tok_halo.at[0], halo_send.at[0], halo_recv.at[0], after, t)),
        (outer, lambda: remote(tokens.at[pl.ds(0, reach)], tok_halo.at[1], halo_send.at[1], halo_recv.at[1], before, t)),
    ]
    halo_kv = [
        (inner, lambda: remote(kv.at[pl.ds(rows, WINDOW)], kv.at[pl.ds(0, WINDOW)], halo_send.at[2], halo_recv.at[2], after, t)),
        (outer, lambda: remote(kv.at[pl.ds(WINDOW, WINDOW)], kv.at[pl.ds(rows + WINDOW, WINDOW)], halo_send.at[3], halo_recv.at[3], before, t)),
    ]

    def halo_wait(pair):
        @pl.when(outer)
        def _():
            pair[0][1]().wait_recv()

        @pl.when(inner)
        def _():
            pair[1][1]().wait_recv()

    @pl.when(s == 0)
    def _():
        tok_halo[0] = jnp.zeros((reach, width), jnp.bfloat16)
        kv[0:WINDOW, :] = jnp.zeros((WINDOW, LANES), jnp.bfloat16)

    @pl.when(s == S - 1)
    def _():
        tok_halo[1] = jnp.zeros((reach, width), jnp.bfloat16)
        kv[rows + WINDOW:rows + 2 * WINDOW, :] = jnp.zeros((WINDOW, LANES), jnp.bfloat16)

    def begin():
        pl.semaphore_wait(barrier, len(greet))
        ev["kv_own"]()
        start_all(halo_tok)
        ev["wo_own"]()

    late = z > 0

    @pl.when(late)
    def _():
        begin()

    def rotated(values, b):
        ca = cos_at[pl.ds(b, 1), :]
        sa = sin_at[pl.ds(b, 1), :]
        ci = cos_v[...]
        si = sin_v[...]
        cosine = ca * ci - sa * si
        sine = sa * ci + ca * si
        swapped = jnp.where(
            first_half,
            pltpu.roll(values, LANES - HEAD // 2, 1),
            pltpu.roll(values, HEAD // 2, 1),
        )
        return values * cosine + swapped * sine

    for copy in own_copies[4:6]:
        copy.wait()
    wide = w_query.shape[1]

    def fold(b, carry):
        at = pl.ds(pl.multiple_of(b * LANES, LANES), LANES)
        column = gain_column(b)
        sums = []
        for k, part in enumerate((wq, wp)):
            scaled = (part[at, :].astype(jnp.float32) * column).astype(jnp.bfloat16)
            wqp[at, k * wide:(k + 1) * wide] = scaled
            sums.append(jnp.sum(scaled.astype(jnp.float32).reshape(LANES // 8, 8, wide), axis=0))
        return carry + jnp.concatenate(sums, axis=1)

    folded = lax.fori_loop(0, width // LANES, fold, jnp.zeros((8, 2 * wide), jnp.float32), unroll=2)
    total_qp = jnp.sum(folded, axis=0, keepdims=True)

    for copy in own_copies[6:]:
        copy.wait()
    LN = 16
    hc = chunks // 2

    def pooled(b, g):
        cols = slice(g * LANES, (g + 1) * LANES)
        length = QB + 2 * reach
        values = pool[pl.ds(pl.multiple_of(b * QB, QB), length), cols]
        index = (t * (pgroups * LANES) + g * LANES) // POOL_CH
        running = values
        stride = 1
        picked = jnp.zeros((QB, LANES), jnp.float32)
        wide = 0
        for k, span in enumerate(POOL_SPANS):
            running = running + pltpu.roll(running, length - stride, 0)
            stride = span
            shift = reach - span // 2
            sums = (pltpu.roll(running, length - shift, 0) if shift else running)[:QB]
            picked = jnp.where(index == k, sums, picked)
            wide = jnp.where(index == k, span // 2, wide)
        pos = offset + b * QB + lax.broadcasted_iota(jnp.int32, (QB, LANES), 0)
        counted = (jnp.minimum(pos + wide, total_rows) - jnp.maximum(pos - wide, 0)).astype(jnp.float32)
        return ((picked / counted - values[reach:reach + QB]) * scale_v[:, cols]).astype(jnp.bfloat16)


    def ex_pool(n):
        at = pl.ds(pl.multiple_of(n * QB, QB), QB)
        return remote(pool_send.at[at], joined.at[T + t, at], ex_send.at[0], ex_recv.at[0], s, cross)

    def ex_att(n):
        at = pl.ds(pl.multiple_of(n * QB, QB), QB)
        return remote(att_send.at[at], joined.at[t, at], ex_send.at[1], ex_recv.at[1], s, cross)

    def send_pooled(n):
        for g in range(pgroups):
            pool_send[pl.ds(pl.multiple_of(n * QB, QB), QB), g * LANES:(g + 1) * LANES] = pooled(cross * hb + n, g)
        ex_pool(n).start()

    def moments(rows_in):
        values = rows_in.astype(jnp.float32)
        center = jnp.sum(values, axis=1, keepdims=True) * (1.0 / width)
        moved = values - center
        spread = jnp.sum(moved * moved, axis=1, keepdims=True) * (1.0 / width)
        inverse = lax.rsqrt(spread + 1e-06)
        return inverse, center * inverse

    def project(i, carry):
        base = chunk_at(i)
        tok_copy(i).wait()
        raw = jnp.dot(tok[pl.ds(base, CHUNK), :], wqp[...], preferred_element_type=jnp.float32)
        scales = []
        shifts = []
        for r in range(CHUNK // LN):
            at = pl.ds(pl.multiple_of(base + r * LN, LN), LN)
            inverse, shifted = moments(tok[at, :])
            scales.append(inverse)
            shifts.append(shifted)
        rstd = jnp.broadcast_to(jnp.concatenate(scales, axis=0), (CHUNK, LANES))
        drop = jnp.broadcast_to(jnp.concatenate(shifts, axis=0), (CHUNK, LANES))
        scale_at[pl.ds(base, CHUNK), :] = rstd
        shift_at[pl.ds(base, CHUNK), :] = drop

        def normal(k, g):
            at = slice(k * QB, (k + 1) * QB)
            cols = slice(g * LANES, (g + 1) * LANES)
            return raw[at, cols] * rstd[at] - drop[at] * total_qp[:, cols]

        for k in range(CHUNK // QB):
            b = base // QB + k
            for g in range(groups):
                turned = rotated(normal(k, g), b) * HEAD ** (-0.5)
                qs[b, pl.ds(2 * g * QB, QB), :] = jnp.where(low_half, turned, 0.0).astype(jnp.bfloat16)
                qs[b, pl.ds((2 * g + 1) * QB, QB), :] = jnp.where(
                    low_half, pltpu.roll(turned, HEAD, 1), 0.0
                ).astype(jnp.bfloat16)
            for g in range(pgroups):
                pool[pl.ds(pl.multiple_of(reach + base + k * QB, 8), QB), g * LANES:(g + 1) * LANES] = (
                    normal(k, groups + g).astype(jnp.bfloat16).astype(jnp.float32)
                )

        @pl.when((i == 0) & (z == 0))
        def _():
            begin()

        @pl.when(i == jnp.where(z == 0, 1, 0))
        def _():
            ev["wo_own_z"]()

        @pl.when(i == hc - 1)
        def _():
            for n in range(1, hb - 1):
                send_pooled(n)

        @pl.when(i == hc)
        def _():
            send_pooled(jnp.where(t == 0, 0, hb - 1))
            kv_wait(0, Z - 1)
            start_all(kv_to_y)
            start_all(kv_to_p)
            ev["wo_own_end"]()

        @pl.when(i == jnp.where(z == 0, chunks - 1, hc))
        def _():
            ev["wo_x"]()
            ev["wo_own_y"]()

        return carry

    lax.fori_loop(0, chunks, project, 0)

    halo_wait(halo_tok)
    edge = jnp.concatenate([tok_halo[0], tok_halo[1]], axis=0)
    edge_scale, edge_shift = moments(edge)
    edge_pool = (
        jnp.dot(edge, wqp[:, wide:], preferred_element_type=jnp.float32) * edge_scale - edge_shift * total_qp[:, wide:]
    ).astype(jnp.bfloat16).astype(jnp.float32)
    pool[0:reach, :] = edge_pool[:reach]
    pool[rows + reach:rows + 2 * reach, :] = edge_pool[reach:]

    def pool_own(i, carry):
        n = jnp.where(t == 0, i, hb - 1 - i)
        for g in range(pgroups):
            joined[T + t, pl.ds(pl.multiple_of(n * QB, QB), QB), g * LANES:(g + 1) * LANES] = pooled(t * hb + n, g)
        return carry

    send_pooled(jnp.where(t == 0, hb - 1, 0))
    lax.fori_loop(0, hb, pool_own, 0)
    kv_wait(1, Z)
    start_all(kv_y_to_p)
    kv_wait(2, 2 * Z)

    def gather_sum(b, carry):
        return carry + jnp.sum(kvw[b].astype(jnp.float32).reshape(LANES // 8, 8, LANES), axis=0)

    total_kv = jnp.sum(
        lax.fori_loop(0, S, gather_sum, jnp.zeros((8, LANES), jnp.float32), unroll=4), axis=0, keepdims=True
    )

    def key_value(i):
        base = i * CHUNK
        both = jnp.dot(
            tok[pl.ds(base, CHUNK), :], kvw[...].reshape(width, LANES), preferred_element_type=jnp.float32
        )
        both = both * scale_at[pl.ds(base, CHUNK), :] - shift_at[pl.ds(base, CHUNK), :] * total_kv
        for k in range(CHUNK // QB):
            piece = both[k * QB:(k + 1) * QB, :]
            turned = rotated(piece, i * (CHUNK // QB) + k)
            kv[pl.ds(WINDOW + base + k * QB, QB), :] = jnp.where(low_half, turned, piece).astype(jnp.bfloat16)

    key_value(0)
    key_value(chunks - 1)
    start_all(halo_kv)
    def early_relays():
        poll("w00", 2)
        ev["wo_d"]()
        poll("w00r", 1)
        poll("w00", 1)

    early_relays()
    for i in range(1, chunks - 1):
        key_value(i)
    span = QB + 2 * WINDOW
    row_id = lax.broadcasted_iota(jnp.int32, (QB, span), 0)
    col_id = lax.broadcasted_iota(jnp.int32, (QB, span), 1)

    def attend(b):
        context = kv[pl.ds(pl.multiple_of(b * QB, QB), span), :]
        scores = lax.dot_general(
            qs[b], context, (((1,), (1,)), ((), ())), preferred_element_type=jnp.float32
        )
        start = offset + b * QB
        lowest = jnp.maximum(row_id, WINDOW - start)
        highest_col = jnp.minimum(row_id + 2 * WINDOW, total_rows - 1 - start + WINDOW)
        valid = (col_id >= lowest) & (col_id <= highest_col)
        expos = []
        norms = []
        for h in range(local_heads):
            part = jnp.where(valid, scores[h * QB:(h + 1) * QB], NEG_BIG)
            top = jnp.maximum(jnp.max(part, axis=1, keepdims=True), sink_v[h])
            expo = jnp.exp(part - top)
            norms.append(1.0 / (jnp.sum(expo, axis=1, keepdims=True) + jnp.exp(sink_v[h] - top)))
            expos.append(expo.astype(jnp.bfloat16))
        result = jnp.dot(jnp.concatenate(expos, axis=0), context, preferred_element_type=jnp.float32)
        heads = [result[h * QB:(h + 1) * QB] * norms[h] for h in range(local_heads)]
        return [
            jnp.where(low_half, pltpu.roll(heads[2 * g], HEAD, 1), heads[2 * g + 1]).astype(jnp.bfloat16)
            for g in range(groups)
        ]


    def attend_other(i, carry):
        @pl.when(i == hb - 1)
        def _():
            halo_wait(halo_kv)
        b = jnp.where(t == 0, hb + i, hb - 1 - i)
        n = b - cross * hb
        at = pl.multiple_of(n * QB, QB)
        for g, value in enumerate(attend(b)):
            att_send[pl.ds(at, QB), g * LANES:(g + 1) * LANES] = value
        ex_att(n).start()

        @pl.when(i == 0)
        def _():
            poll("w10r", 1)

        @pl.when(i == 1)
        def _():
            poll("w01", 0)

        return carry

    def attend_own(i, carry):
        b = jnp.where(t == 0, hb - 1 - i, hb + i)
        at = pl.multiple_of((b - t * hb) * QB, QB)
        for g, value in enumerate(attend(b)):
            joined[t, pl.ds(at, QB), g * LANES:(g + 1) * LANES] = value

        @pl.when(i == 1)
        def _():
            poll("w00", *range(3, Z))

        @pl.when(i == jnp.where((z == 0) | (z == Z - 1), 3, 2))
        def _():
            poll("w11", 2)
        return carry

    lax.fori_loop(0, hb, attend_other, 0)
    lax.fori_loop(0, hb, attend_own, 0)
    whole_pool = remote(pool_send, joined.at[T + cross], ex_send.at[0], ex_recv.at[0], s, cross)
    whole_att = remote(att_send, joined.at[cross], ex_send.at[1], ex_recv.at[1], s, cross)
    whole_pool.wait_recv()

    def columns(n, half, start, count):
        at = pl.ds(pl.multiple_of(start, wide), count)
        return jnp.concatenate([wfull[2 * n, half, at, :], wfull[2 * n + 1, half, at, :]], axis=1)

    at_rim = (z == 0) | (z == Z - 1)

    def near():
        poll("w01r", 1)
        poll("w11r", 1)

    def second():
        poll("w01", 2)
        poll("w10", 2)

    def pair_of(p):
        q = jnp.where(at_rim & ((p == 1) | (p == 2)), 3 - p, p)
        zz = sum(((z // bit + q // bit) % 2) * bit for bit in [2 ** k for k in range(Z.bit_length() - 1)])
        return [zz * 2 + y, zz * 2 + 1 - y]

    def pair_wait(pair):
        some = wfull.at[pl.ds(0, 2)]
        remote(some, some, wo_send.at[2], wp_recv.at[pair[0] // 2], partner, t).wait_recv()

    def pair_columns(pair, half, start, count):
        return jnp.concatenate([columns(n, half, start, count) for n in pair], axis=1)

    def store(n, total):
        out[:, pl.ds(pl.multiple_of(n * 2 * LANES, 2 * LANES), 2 * LANES)] = total.astype(jnp.bfloat16)

    def most(p, carry):
        @pl.when(p == 1)
        def _():
            pl.when(at_rim)(second)
            pl.when(jnp.logical_not(at_rim))(near)
        pair = pair_of(p)
        pair_wait(pair)
        left = jnp.concatenate([joined[t]] + [joined[T + k] for k in range(T)], axis=1)
        right = jnp.concatenate([pair_columns(pair, 0, t * wide, wide), pair_columns(pair, 1, 0, T * wide)], axis=0)
        total = jnp.dot(left, right, preferred_element_type=jnp.float32)
        acc[pair[0]] = total[:, :2 * LANES]
        acc[pair[1]] = total[:, 2 * LANES:]
        return carry

    def last(p, carry):
        pair = pair_of(p)
        total = jnp.dot(
            joined[cross], pair_columns(pair, 0, cross * wide, wide), preferred_element_type=jnp.float32
        )
        store(pair[0], acc[pair[0]] + total[:, :2 * LANES])
        store(pair[1], acc[pair[1]] + total[:, 2 * LANES:])
        return carry

    def whole(p, carry):
        @pl.when(p == split)
        def _():
            poll("w10", 1)
            poll("w11", 1)
            poll("w01", 1)
            poll("w01", *range(3, Z))
            poll("w10", *range(3, Z))
            poll("w11", *range(3, Z))
        pair = pair_of(p)
        pair_wait(pair)
        left = jnp.concatenate([joined[k] for k in range(2 * T)], axis=1)
        right = jnp.concatenate([pair_columns(pair, half, 0, T * wide) for half in range(T)], axis=0)
        total = jnp.dot(left, right, preferred_element_type=jnp.float32)
        store(pair[0], total[:, :2 * LANES])
        store(pair[1], total[:, 2 * LANES:])
        return carry

    split = Z // 2
    lax.fori_loop(0, split, most, 0)
    pl.when(at_rim)(near)
    pl.when(jnp.logical_not(at_rim))(second)
    whole_att.wait_recv()
    lax.fori_loop(0, split, last, 0)
    lax.fori_loop(split, Z, whole, 0)

    def sent(ref, sem):
        remote(ref, ref, sem, halo_recv.at[0], partner, t).wait_send()

    for cond, make in halo_tok + halo_kv:
        @pl.when(cond)
        def _(make=make):
            make().wait_send()
    whole_pool.wait_send()
    whole_att.wait_send()
    sent(kvw.at[pl.ds(0, 4 * Z - 1)], kv_send.at[0])
    sent(wfull.at[s], wo_send.at[2])
    sent(wfull.at[pl.ds(0, 3 * Z - 1)], wo_send.at[0])
    for at in range(Z):
        inside = lambda k: 0 <= k < Z
        edge = (0, Z - 1)
        count = sum(inside(at + h) for h in hop)
        count += sum(inside(at + h) and (abs(h) > 1 or inside(at + 2 * h)) for h in hop)
        count += 2 * sum(inside(at + d) and inside(at - d // abs(d)) for d in far if 2 <= abs(d) < Z - 1)
        for h in (1, -1):
            if inside(at + h):
                count += (at in edge or at + h in edge) + (at in edge)

        @pl.when(z == at)
        def _(count=count):
            sent(wfull.at[pl.ds(0, count // 2)], wo_send.at[1])


def body(mesh, tokens, norm_gain, w_query, w_key, w_value, w_pool_in, sink_logit, pool_scale, w_out):
    S = lax.axis_size("sp")
    T = lax.axis_size("tp")
    rows, width = tokens.shape
    local_heads = w_query.shape[1] // HEAD
    fits = (
        S % 4 == 0 and S > 4 and S & (S - 1) == 0 and T == 2
        and w_out.shape[1] == LANES and w_key.shape == (LANES, LANES) and w_value.shape == w_key.shape
        and w_query.shape[1] % LANES == 0 and w_pool_in.shape[1] % LANES == 0
        and w_query.shape[1] == w_pool_in.shape[1]
        and local_heads == QH // KVH and rows % (2 * CHUNK) == 0
        and width == S * LANES and LANES % S == 0
    )
    if not fits:
        return plain_body(
            tokens, norm_gain, w_query, w_key, w_value, w_pool_in, sink_logit, pool_scale, w_out
        )
    tables = rope_tables(S * rows)
    blocks = rows // QB
    half = rows // T
    Z = S // 4
    reach = POOL_SPANS[-1] // 2
    wide = w_query.shape[1]
    vmem = pl.BlockSpec(memory_space=pltpu.VMEM)
    hbm = pl.BlockSpec(memory_space=pltpu.HBM)
    dma = pltpu.SemaphoreType.DMA
    bf = jnp.bfloat16
    return pl.pallas_call(
        functools.partial(mixer_kernel, (S, T)),
        out_shape=pltpu.VMEM((half, S * w_out.shape[1]), bf),
        in_specs=[hbm] * 13,
        out_specs=vmem,
        scratch_shapes=[
            pltpu.VMEM((2, reach, width), bf),
            pltpu.VMEM((width // LANES, LANES), jnp.float32),
            pltpu.VMEM((1, wide), jnp.float32),
            pltpu.SMEM(sink_logit.shape, jnp.float32),
            pltpu.VMEM((QB, LANES), jnp.float32),
            pltpu.VMEM((QB, LANES), jnp.float32),
            pltpu.VMEM((rows, width), bf),
            pltpu.VMEM(w_query.shape, bf),
            pltpu.VMEM(w_pool_in.shape, bf),
            pltpu.VMEM((width, 2 * wide), bf),
            pltpu.VMEM((rows, LANES), jnp.float32),
            pltpu.VMEM((rows, LANES), jnp.float32),
            pltpu.VMEM((2,) + w_key.shape, bf),
            pltpu.VMEM((S, LANES, LANES), bf),
            pltpu.VMEM((S, T) + w_out.shape, bf),
            pltpu.VMEM((blocks, local_heads * QB, LANES), bf),
            pltpu.VMEM((rows + 2 * WINDOW, LANES), bf),
            pltpu.VMEM((rows + 2 * reach, wide), jnp.float32),
            pltpu.VMEM((half, wide), bf),
            pltpu.VMEM((half, wide), bf),
            pltpu.VMEM((2 * T, half, wide), bf),
            pltpu.VMEM((S // 2, half, 2 * LANES), jnp.float32),
            pltpu.VMEM((blocks, LANES), jnp.float32),
            pltpu.VMEM((blocks, LANES), jnp.float32),
            dma((rows // CHUNK,)),
            dma((12,)),
            dma((1,)),
            dma((3,)),
            dma((3,)),
            dma((S // 2, T)),
            dma((Z,)),
            dma((4,)),
            dma((4,)),
            dma((2,)),
            dma((2,)),
        ],
        compiler_params=pltpu.CompilerParams(
            collective_id=0, has_side_effects=True, vmem_limit_bytes=VMEM_LIMIT
        ),
    )(
        tokens, norm_gain.reshape(width // LANES, LANES), w_query, w_key, w_value, w_pool_in, sink_logit, pool_scale[None, :], w_out, *tables
    )


def solution(mesh):
    in_specs = (
        P("sp", None),
        P(),
        P(None, "tp"),
        P("sp", None),
        P("sp", None),
        P(None, "tp"),
        P("tp"),
        P("tp"),
        P("tp", "sp"),
    )
    out_specs = P(("sp", "tp"), None)
    return jax.shard_map(functools.partial(body, mesh), mesh=mesh, in_specs=in_specs, out_specs=out_specs, check_vma=False)
```

```python
import functools

import jax
import jax.numpy as jnp
import numpy as np
from jax import lax
from jax.experimental import pallas as pl
from jax.experimental.pallas import tpu as pltpu
from jax.sharding import PartitionSpec as P

HEAD = 64
QH = 8
KVH = 2
POOL_CH = 128
WINDOW = 128
QB = 128


NEG_BIG = -1e30
POOL_SPANS = (2, 4, 8, 16)


def extended(block, sides, width):
    for axis, dim in sides:
        count = lax.axis_size(axis)
        forward = [(i, i + 1) for i in range(count - 1)]
        backward = [(target, source) for source, target in forward]
        low = lax.ppermute(
            lax.slice_in_dim(block, block.shape[dim] - width, None, axis=dim), axis, forward
        )
        high = lax.ppermute(lax.slice_in_dim(block, 0, width, axis=dim), axis, backward)
        block = jnp.concatenate([low, block, high], axis=dim)
    return block


def layer_normed(tokens, norm_gain):
    values = tokens.astype(jnp.float32)
    center = jnp.mean(values, axis=-1, keepdims=True)
    spread = jnp.mean(jnp.square(values - center), axis=-1, keepdims=True)
    return ((values - center) * lax.rsqrt(spread + 1e-06) * norm_gain).astype(jnp.bfloat16)


def rotate(values, positions):
    half = HEAD // 2
    inverse = 10000.0 ** (-jnp.arange(half, dtype=jnp.float32) / half)
    angles = positions[:, None] * inverse[None, :]
    cosine = jnp.cos(angles)[:, None, :]
    sine = jnp.sin(angles)[:, None, :]
    first = values[..., :half]
    second = values[..., half:]
    return jnp.concatenate(
        [first * cosine - second * sine, first * sine + second * cosine], axis=-1
    )


def plain_body(tokens, norm_gain, w_query, w_key, w_value, w_pool_in, sink_logit, pool_scale, w_out):
    local_rows = tokens.shape[0]
    seq_total = local_rows * lax.axis_size("sp")
    offset = lax.axis_index("sp") * local_rows
    tp_place = lax.axis_index("tp")
    local_heads = w_query.shape[1] // HEAD
    local_pool = w_pool_in.shape[1]
    reach = POOL_SPANS[-1] // 2
    normed = layer_normed(tokens, norm_gain)
    positions = (offset + jnp.arange(local_rows)).astype(jnp.float32)
    query = rotate(
        jnp.dot(normed, w_query, preferred_element_type=jnp.float32).reshape(
            local_rows, local_heads, HEAD
        ),
        positions,
    ).astype(jnp.bfloat16)
    key_head = tp_place * local_heads // (QH // KVH)
    key_cols = lax.dynamic_slice_in_dim(w_key, key_head * HEAD, HEAD, 1)
    value_cols = lax.dynamic_slice_in_dim(w_value, key_head * HEAD, HEAD, 1)
    key_sum = jnp.dot(
        normed,
        lax.all_gather(key_cols, "sp", axis=0, tiled=True),
        preferred_element_type=jnp.float32,
    )
    value_sum = jnp.dot(
        normed,
        lax.all_gather(value_cols, "sp", axis=0, tiled=True),
        preferred_element_type=jnp.float32,
    )
    key = rotate(key_sum[:, None, :], positions)[:, 0, :].astype(jnp.bfloat16)
    value = value_sum.astype(jnp.bfloat16)
    key_value = jnp.concatenate([key, value], axis=1)
    pool_in = jnp.dot(normed, w_pool_in, preferred_element_type=jnp.float32).astype(jnp.bfloat16)
    widened = extended(jnp.concatenate([key_value, pool_in], axis=1), (("sp", 0),), WINDOW)
    kv_wide = widened[:, : 2 * HEAD]
    pool_wide = widened[WINDOW - reach : WINDOW + local_rows + reach, 2 * HEAD :]
    span = QB + 2 * WINDOW
    sink_here = sink_logit[:, None, None]
    results = []
    for block in range(local_rows // QB):
        queries = query[block * QB : (block + 1) * QB]
        keys = kv_wide[block * QB : block * QB + span, :HEAD]
        values = kv_wide[block * QB : block * QB + span, HEAD:]
        scores = jnp.einsum(
            "ihd,jd->hij", queries, keys, preferred_element_type=jnp.float32
        ) * HEAD ** (-0.5)
        query_pos = offset + block * QB + jnp.arange(QB)
        key_pos = offset + block * QB - WINDOW + jnp.arange(span)
        valid = (
            (jnp.abs(query_pos[:, None] - key_pos[None, :]) <= WINDOW)
            & (key_pos[None, :] >= 0)
            & (key_pos[None, :] < seq_total)
        )
        scores = jnp.where(valid, scores, NEG_BIG)
        highest = jnp.maximum(jnp.max(scores, axis=-1, keepdims=True), sink_here)
        expo = jnp.where(valid, jnp.exp(scores - highest), 0.0)
        total = jnp.sum(expo, axis=-1, keepdims=True) + jnp.exp(sink_here - highest)
        weights = (expo / total).astype(jnp.bfloat16)
        result = jnp.einsum("hij,jd->ihd", weights, values, preferred_element_type=jnp.float32)
        results.append(result.reshape(QB, local_heads * HEAD).astype(jnp.bfloat16))
    attended = jnp.concatenate(results, axis=0)
    pool_vals = pool_wide.astype(jnp.float32)
    window_sum = pool_vals
    global_pos = offset + jnp.arange(local_rows)
    channel = tp_place * local_pool + jnp.arange(local_pool)
    window_group = channel // POOL_CH
    measured = jnp.zeros((local_rows, local_pool), jnp.float32)
    stride = 1
    for index, width in enumerate(POOL_SPANS):
        window_sum = window_sum[:-stride] + window_sum[stride:]
        stride = width
        sums = window_sum[reach - width // 2 : reach - width // 2 + local_rows]
        counted = (
            jnp.minimum(global_pos + width // 2, seq_total)
            - jnp.maximum(global_pos - width // 2, 0)
        ).astype(jnp.float32)
        measured = measured + jnp.where(
            window_group[None, :] == index, sums / counted[:, None], 0.0
        )
    pooled = ((measured - pool_vals[reach : reach + local_rows]) * pool_scale).astype(jnp.bfloat16)
    attended_rows, pooled_rows = (
        lax.all_to_all(attended, "tp", split_axis=0, concat_axis=1, tiled=True),
        lax.all_to_all(pooled, "tp", split_axis=0, concat_axis=1, tiled=True),
    )
    joined = jnp.concatenate([attended_rows, pooled_rows], axis=1)
    out_rows_all = lax.all_gather(w_out, "tp", axis=0, tiled=True)
    projected = jnp.dot(
        joined,
        lax.all_gather(out_rows_all, "sp", axis=1, tiled=True),
        preferred_element_type=jnp.float32,
    )
    return projected.astype(jnp.bfloat16)


LANES = 128
CHUNK = 256
VMEM_LIMIT = 60 * 1024 * 1024
MESH = pl.DeviceIdType.MESH


def rope_tables(rows_total):
    half = HEAD // 2
    inverse = np.tile(10000.0 ** (-np.arange(half, dtype=np.float64) / half), LANES // half)[None, :]
    sign = np.where(np.arange(LANES) % HEAD < half, -1.0, 1.0)[None, :]
    inner = np.arange(QB, dtype=np.float64)[:, None] * inverse
    starts = (QB * np.arange(rows_total // QB, dtype=np.float64))[:, None] * inverse
    tables = (np.cos(inner), np.sin(inner) * sign, np.cos(starts), np.sin(starts) * sign)
    return [jnp.asarray(table.astype(np.float32)) for table in tables]


def mixer_kernel(
    places, tokens, gain, w_query, w_key, w_value, w_pool, sink, scale, w_out, cos_in, sin_in, cos_all, sin_all,
    out,
    tok_halo, gain_v, scale_v, sink_v, cos_v, sin_v, tok, wq, wp, wqp, scale_at, shift_at, kv_in, kvw, wfull, qs, kv, pool, pool_send, att_send, joined, acc, cos_at, sin_at,
    tok_sem, own_sem, kv_send, kv_recv, wo_send, wo_recv, wp_recv, halo_send, halo_recv, ex_send, ex_recv,
):
    S, T = places
    Z = S // 4
    s = lax.axis_index("sp")
    t = lax.axis_index("tp")
    rows = tokens.shape[0]
    width = tokens.shape[1]
    blocks = rows // QB
    hb = blocks // 2
    chunks = rows // CHUNK
    local_heads = w_query.shape[1] // HEAD
    groups = w_query.shape[1] // LANES
    pgroups = w_pool.shape[1] // LANES
    reach = POOL_SPANS[-1] // 2
    offset = s * rows
    total_rows = S * rows
    c = s % 2
    y = (s // 2) % 2
    z = s // 4
    partner = s + 1 - 2 * c
    yflip = s + 2 - 4 * y
    after = (s + 1) % S
    before = (s + S - 1) % S
    cross = 1 - t
    far = [d for k in range(1, Z) for d in (k, -k)]

    def remote(a, b, send, recv, to_s, to_t):
        return pltpu.make_async_remote_copy(
            src_ref=a, dst_ref=b, send_sem=send, recv_sem=recv,
            device_id={"sp": to_s, "tp": to_t}, device_id_type=MESH,
        )

    def chunk_at(i):
        return pl.multiple_of(jnp.where(t == 0, chunks - 1 - i, i) * CHUNK, CHUNK)

    def tok_copy(i):
        at = pl.ds(chunk_at(i), CHUNK)
        return pltpu.make_async_copy(tokens.at[at], tok.at[at], tok_sem.at[i])

    own_copies = [
        pltpu.make_async_copy(gain, gain_v, own_sem.at[7]),
        pltpu.make_async_copy(w_key, kv_in.at[0], own_sem.at[0]),
        pltpu.make_async_copy(w_value, kv_in.at[1], own_sem.at[1]),
        pltpu.make_async_copy(w_out, wfull.at[s, t], own_sem.at[2]),
        pltpu.make_async_copy(w_query, wq, own_sem.at[3]),
        pltpu.make_async_copy(w_pool, wp, own_sem.at[4]),
        pltpu.make_async_copy(cos_all.at[pl.ds(pl.multiple_of(s * blocks, blocks), blocks)], cos_at, own_sem.at[5]),
        pltpu.make_async_copy(sin_all.at[pl.ds(pl.multiple_of(s * blocks, blocks), blocks)], sin_at, own_sem.at[6]),
        pltpu.make_async_copy(cos_in, cos_v, own_sem.at[8]),
        pltpu.make_async_copy(sin_in, sin_v, own_sem.at[9]),
        pltpu.make_async_copy(scale, scale_v, own_sem.at[10]),
        pltpu.make_async_copy(sink, sink_v, own_sem.at[11]),
    ]
    barrier = pltpu.get_barrier_semaphore()
    greet = [(((z + d) % Z) * 4 + s % 4, t) for d in range(1, Z)]
    greet += [(yflip, t), (after, t), (before, t), (s, cross), (yflip, cross)]
    for to_s, to_t in greet:
        pl.semaphore_signal(barrier, inc=1, device_id={"sp": to_s, "tp": to_t}, device_id_type=MESH)
    for copy in own_copies[:6]:
        copy.start()
    tok_copy(0).start()
    for copy in own_copies[6:]:
        copy.start()
    for i in range(1, chunks):
        tok_copy(i).start()

    lane = lax.broadcasted_iota(jnp.int32, (QB, LANES), 1)
    low_half = lane < HEAD
    first_half = lane % HEAD < HEAD // 2

    own_copies[0].wait()
    gains = jnp.transpose(jnp.concatenate([gain_v[...]] * (LANES // gain.shape[0]), axis=0))

    def gain_column(b):
        return pltpu.roll(gains, (LANES - b) % LANES, 1)[:, :1]

    own_copies[1].wait()
    own_copies[2].wait()
    key_head = t * local_heads // (QH // KVH)
    key_in = kv_in[0].astype(jnp.float32)
    value_in = kv_in[1].astype(jnp.float32)
    key_cols = jnp.where(key_head == 0, key_in, pltpu.roll(key_in, HEAD, 1))
    value_cols = jnp.where(key_head == 0, pltpu.roll(value_in, HEAD, 1), value_in)
    kvw[s] = (jnp.where(low_half, key_cols, value_cols) * gain_column(s)).astype(jnp.bfloat16)
    own_copies[3].wait()

    def here(d):
        return (z + d >= 0) & (z + d < Z)

    def kv_copy(b, link, to):
        return lambda: remote(kvw.at[b], kvw.at[b], kv_send.at[0], kv_recv.at[link], to, t)

    def kv_wait(link, count):
        some = kvw.at[pl.ds(0, count)]
        remote(some, some, kv_send.at[0], kv_recv.at[link], partner, t).wait_recv()

    def wo_copy(b, half, group, to_s, to_t):
        return lambda: remote(wfull.at[b, half], wfull.at[b, half], wo_send.at[group], wo_recv.at[b // 2, half], to_s, to_t)

    def hand(b, half, group=0):
        return (None, lambda: remote(
            wfull.at[b, half], wfull.at[b, half], wo_send.at[group], wp_recv.at[b // 4], partner, t))

    hop = [2, -2, 1, -1]

    def at_z(d):
        return s + 4 * d

    def at_yz(d):
        return yflip + 4 * d

    def start_all(items):
        for cond, make in items:
            if cond is None:
                make().start()
            else:
                @pl.when(cond)
                def _(make=make):
                    make().start()

    def event(cond, arrival, items):
        def act():
            def inner():
                if arrival is not None:
                    arrival().wait_recv()
                start_all(items)
            if cond is None:
                inner()
            else:
                pl.when(cond)(inner)
        return act

    def onward(d):
        step = -1 if d > 0 else 1
        return step, here(step)

    ev = {}
    ev["kv_own"] = event(None, None,
        [(here(h), kv_copy(s, 0, at_z(h))) for h in far]
        + [(None, kv_copy(s, 1, yflip)), (None, kv_copy(s, 2, partner))])
    kv_to_y = [(here(d), kv_copy(at_z(d), 1, yflip)) for d in far]
    kv_to_p = [(here(d), kv_copy(at_z(d), 2, partner)) for d in far]
    kv_y_to_p = [(None, kv_copy(yflip, 2, partner))] + [(here(d), kv_copy(at_yz(d), 2, partner)) for d in far]

    ev["wo_own"] = event(None, None,
        [(None, wo_copy(s, t, 2, s, cross)), (z > 0, wo_copy(s, t, 0, yflip, t)), hand(s, t, 2)])
    ev["wo_own_y"] = event(None, None, [(z == 0, wo_copy(s, t, 0, yflip, t))])
    ahead = [(h, here(h) & here(2 * h) if abs(h) == 1 else here(h)) for h in hop if abs(h) < Z]
    ends = [(h, here(h) & jnp.logical_not(here(2 * h))) for h in hop if abs(h) == 1]
    ev["wo_own_z"] = event(None, None, [(ok, wo_copy(s, t, 1, at_z(h), t)) for h, ok in ahead])
    ev["wo_own_end"] = event(None, None, [(ok, wo_copy(s, t, 1, at_z(h), t)) for h, ok in ends])
    def rim(d):
        return here(d) & ((z == 0) | (z == Z - 1) | (z + d == 0) | (z + d == Z - 1))

    ev["wo_x"] = event(None, wo_copy(s, cross, 0, yflip, t),
        [(None, wo_copy(s, cross, 0, yflip, t)), hand(s, cross)]
        + [(rim(h), wo_copy(s, cross, 1, at_z(h), t)) for h in (1, -1)])
    ev["wo_d"] = event(None, wo_copy(yflip, cross, 0, partner, t),
        [(ok, wo_copy(yflip, cross, 1, at_z(h), t)) for h, ok in ahead] + [hand(yflip, cross)])
    def split_event(kind, d, arrival, items, at_rim=(), inner_only=()):
        if abs(d) == 1:
            ev[kind + "r", d] = event(rim(d), arrival, list(at_rim) + items)
            ev[kind, d] = event(here(d) & jnp.logical_not(rim(d)), arrival, list(inner_only) + items)
        else:
            ev[kind, d] = event(None if d == 0 else here(d), arrival, list(inner_only) + items)

    for d in far:
        step, fine = onward(d)
        relay = 2 <= abs(d) < Z - 1
        b = at_z(d)
        to_x = [(None, wo_copy(b, t, 0, s, cross))]
        items = [(None, wo_copy(b, t, 0, yflip, t)), hand(b, t)]
        if relay:
            served = here(d) & fine
            arrival = wo_copy(b, t, 0, s, cross)
            busy = (c == 0) & (y == 0) if step < 0 else (c == 1) & (y == 1)
            forward = [(None, wo_copy(b, t, 1, at_z(step), t))]
            ev["relay", d] = event(served & jnp.logical_not(busy), arrival, forward)
            ev["relay_late", d] = event(served & busy, arrival, forward)
            ev["served", d] = event(served, None, to_x + items)
            ev["w00", d] = event(here(d) & jnp.logical_not(fine), arrival, to_x + items)
        else:
            split_event("w00", d, wo_copy(b, t, 0, s, cross), items, inner_only=to_x)
        split_event("w10", d, wo_copy(b, cross, 0, partner, t), [hand(b, cross)],
            [((z == 0) | (z == Z - 1), wo_copy(b, cross, 1, yflip, t))])
        b = at_yz(d)
        items = [hand(b, cross)]
        if relay:
            items = [(fine, wo_copy(b, cross, 1, at_z(step), t))] + items
        split_event("w11", d, wo_copy(b, cross, 0, partner, t), items)
    for d in [0] + far:
        b = at_yz(d)
        split_event("w01", d, wo_copy(b, t, 0, partner, t), [hand(b, t)])

    def poll(kind, *distances):
        for k in distances:
            for d in ((k, -k) if k else (0,)):
                if abs(d) < Z:
                    ev[kind, d]()

    inner = s < S - 1
    outer = s > 0
    halo_tok = [
        (inner, lambda: remote(tokens.at[pl.ds(rows - reach, reach)], tok_halo.at[0], halo_send.at[0], halo_recv.at[0], after, t)),
        (outer, lambda: remote(tokens.at[pl.ds(0, reach)], tok_halo.at[1], halo_send.at[1], halo_recv.at[1], before, t)),
    ]
    halo_kv = [
        (inner, lambda: remote(kv.at[pl.ds(rows, WINDOW)], kv.at[pl.ds(0, WINDOW)], halo_send.at[2], halo_recv.at[2], after, t)),
        (outer, lambda: remote(kv.at[pl.ds(WINDOW, WINDOW)], kv.at[pl.ds(rows + WINDOW, WINDOW)], halo_send.at[3], halo_recv.at[3], before, t)),
    ]

    def halo_wait(pair):
        @pl.when(outer)
        def _():
            pair[0][1]().wait_recv()

        @pl.when(inner)
        def _():
            pair[1][1]().wait_recv()

    @pl.when(s == 0)
    def _():
        tok_halo[0] = jnp.zeros((reach, width), jnp.bfloat16)
        kv[0:WINDOW, :] = jnp.zeros((WINDOW, LANES), jnp.bfloat16)

    @pl.when(s == S - 1)
    def _():
        tok_halo[1] = jnp.zeros((reach, width), jnp.bfloat16)
        kv[rows + WINDOW:rows + 2 * WINDOW, :] = jnp.zeros((WINDOW, LANES), jnp.bfloat16)

    def begin():
        pl.semaphore_wait(barrier, len(greet))
        ev["kv_own"]()
        start_all(halo_tok)
        ev["wo_own"]()

    late = z > 0

    @pl.when(late)
    def _():
        begin()

    def rotated(values, b):
        ca = cos_at[pl.ds(b, 1), :]
        sa = sin_at[pl.ds(b, 1), :]
        ci = cos_v[...]
        si = sin_v[...]
        cosine = ca * ci - sa * si
        sine = sa * ci + ca * si
        swapped = jnp.where(
            first_half,
            pltpu.roll(values, LANES - HEAD // 2, 1),
            pltpu.roll(values, HEAD // 2, 1),
        )
        return values * cosine + swapped * sine

    for copy in own_copies[4:6]:
        copy.wait()
    wide = w_query.shape[1]

    def fold(b, carry):
        at = pl.ds(pl.multiple_of(b * LANES, LANES), LANES)
        column = gain_column(b)
        sums = []
        for k, part in enumerate((wq, wp)):
            scaled = (part[at, :].astype(jnp.float32) * column).astype(jnp.bfloat16)
            wqp[at, k * wide:(k + 1) * wide] = scaled
            sums.append(jnp.sum(scaled.astype(jnp.float32).reshape(LANES // 8, 8, wide), axis=0))
        return carry + jnp.concatenate(sums, axis=1)

    folded = lax.fori_loop(0, width // LANES, fold, jnp.zeros((8, 2 * wide), jnp.float32), unroll=2)
    total_qp = jnp.sum(folded, axis=0, keepdims=True)

    for copy in own_copies[6:]:
        copy.wait()
    LN = 16
    hc = chunks // 2

    def pooled(b, g):
        cols = slice(g * LANES, (g + 1) * LANES)
        length = QB + 2 * reach
        values = pool[pl.ds(pl.multiple_of(b * QB, QB), length), cols]
        index = (t * (pgroups * LANES) + g * LANES) // POOL_CH
        running = values
        stride = 1
        picked = jnp.zeros((QB, LANES), jnp.float32)
        wide = 0
        for k, span in enumerate(POOL_SPANS):
            running = running + pltpu.roll(running, length - stride, 0)
            stride = span
            shift = reach - span // 2
            sums = (pltpu.roll(running, length - shift, 0) if shift else running)[:QB]
            picked = jnp.where(index == k, sums, picked)
            wide = jnp.where(index == k, span // 2, wide)
        pos = offset + b * QB + lax.broadcasted_iota(jnp.int32, (QB, LANES), 0)
        counted = (jnp.minimum(pos + wide, total_rows) - jnp.maximum(pos - wide, 0)).astype(jnp.float32)
        return ((picked / counted - values[reach:reach + QB]) * scale_v[:, cols]).astype(jnp.bfloat16)


    def ex_pool(n):
        at = pl.ds(pl.multiple_of(n * QB, QB), QB)
        return remote(pool_send.at[at], joined.at[T + t, at], ex_send.at[0], ex_recv.at[0], s, cross)

    def ex_att(n):
        at = pl.ds(pl.multiple_of(n * QB, QB), QB)
        return remote(att_send.at[at], joined.at[t, at], ex_send.at[1], ex_recv.at[1], s, cross)

    def send_pooled(n):
        for g in range(pgroups):
            pool_send[pl.ds(pl.multiple_of(n * QB, QB), QB), g * LANES:(g + 1) * LANES] = pooled(cross * hb + n, g)
        ex_pool(n).start()

    def moments(rows_in):
        values = rows_in.astype(jnp.float32)
        center = jnp.sum(values, axis=1, keepdims=True) * (1.0 / width)
        moved = values - center
        spread = jnp.sum(moved * moved, axis=1, keepdims=True) * (1.0 / width)
        inverse = lax.rsqrt(spread + 1e-06)
        return inverse, center * inverse

    def project(i, carry):
        base = chunk_at(i)
        tok_copy(i).wait()
        raw = jnp.dot(tok[pl.ds(base, CHUNK), :], wqp[...], preferred_element_type=jnp.float32)
        scales = []
        shifts = []
        for r in range(CHUNK // LN):
            at = pl.ds(pl.multiple_of(base + r * LN, LN), LN)
            inverse, shifted = moments(tok[at, :])
            scales.append(inverse)
            shifts.append(shifted)
        rstd = jnp.broadcast_to(jnp.concatenate(scales, axis=0), (CHUNK, LANES))
        drop = jnp.broadcast_to(jnp.concatenate(shifts, axis=0), (CHUNK, LANES))
        scale_at[pl.ds(base, CHUNK), :] = rstd
        shift_at[pl.ds(base, CHUNK), :] = drop

        def normal(k, g):
            at = slice(k * QB, (k + 1) * QB)
            cols = slice(g * LANES, (g + 1) * LANES)
            return raw[at, cols] * rstd[at] - drop[at] * total_qp[:, cols]

        for k in range(CHUNK // QB):
            b = base // QB + k
            for g in range(groups):
                turned = rotated(normal(k, g), b) * HEAD ** (-0.5)
                qs[b, pl.ds(2 * g * QB, QB), :] = jnp.where(low_half, turned, 0.0).astype(jnp.bfloat16)
                qs[b, pl.ds((2 * g + 1) * QB, QB), :] = jnp.where(
                    low_half, pltpu.roll(turned, HEAD, 1), 0.0
                ).astype(jnp.bfloat16)
            for g in range(pgroups):
                pool[pl.ds(pl.multiple_of(reach + base + k * QB, 8), QB), g * LANES:(g + 1) * LANES] = (
                    normal(k, groups + g).astype(jnp.bfloat16).astype(jnp.float32)
                )

        @pl.when((i == 0) & (z == 0))
        def _():
            begin()

        @pl.when(i == 1)
        def _():
            ev["wo_own_z"]()

        @pl.when(i == jnp.where((z == 0) | (z == Z - 1), hc, hc - 1))
        def _():
            kv_wait(0, Z - 1)
            start_all(kv_to_y)
            start_all(kv_to_p)

        @pl.when(i == hc - 1)
        def _():
            for n in range(1, hb - 1):
                send_pooled(n)

        @pl.when(i == hc)
        def _():
            send_pooled(jnp.where(t == 0, 0, hb - 1))
            ev["wo_own_end"]()

        @pl.when(i == jnp.where(z == 0, chunks - 1, hc))
        def _():
            ev["wo_x"]()
            ev["wo_own_y"]()

        return carry

    lax.fori_loop(0, chunks, project, 0)

    halo_wait(halo_tok)
    edge = jnp.concatenate([tok_halo[0], tok_halo[1]], axis=0)
    edge_scale, edge_shift = moments(edge)
    edge_pool = (
        jnp.dot(edge, wqp[:, wide:], preferred_element_type=jnp.float32) * edge_scale - edge_shift * total_qp[:, wide:]
    ).astype(jnp.bfloat16).astype(jnp.float32)
    pool[0:reach, :] = edge_pool[:reach]
    pool[rows + reach:rows + 2 * reach, :] = edge_pool[reach:]

    def pool_own(i, carry):
        n = jnp.where(t == 0, i, hb - 1 - i)
        for g in range(pgroups):
            joined[T + t, pl.ds(pl.multiple_of(n * QB, QB), QB), g * LANES:(g + 1) * LANES] = pooled(t * hb + n, g)
        return carry

    send_pooled(jnp.where(t == 0, hb - 1, 0))
    lax.fori_loop(0, hb, pool_own, 0)
    kv_wait(1, Z)
    start_all(kv_y_to_p)
    kv_wait(2, 2 * Z)
    poll("relay", 2)

    def gather_sum(b, carry):
        return carry + jnp.sum(kvw[b].astype(jnp.float32).reshape(LANES // 8, 8, LANES), axis=0)

    total_kv = jnp.sum(
        lax.fori_loop(0, S, gather_sum, jnp.zeros((8, LANES), jnp.float32), unroll=4), axis=0, keepdims=True
    )

    def key_value(i):
        base = i * CHUNK
        both = jnp.dot(
            tok[pl.ds(base, CHUNK), :], kvw[...].reshape(width, LANES), preferred_element_type=jnp.float32
        )
        both = both * scale_at[pl.ds(base, CHUNK), :] - shift_at[pl.ds(base, CHUNK), :] * total_kv
        for k in range(CHUNK // QB):
            piece = both[k * QB:(k + 1) * QB, :]
            turned = rotated(piece, i * (CHUNK // QB) + k)
            kv[pl.ds(WINDOW + base + k * QB, QB), :] = jnp.where(low_half, turned, piece).astype(jnp.bfloat16)

    key_value(0)
    key_value(chunks - 1)
    start_all(halo_kv)
    def early_relays():
        poll("relay_late", 2)
        poll("served", 2)
        poll("w00", 2)
        ev["wo_d"]()
        poll("w00r", 1)
        poll("w00", 1)

    early_relays()
    for i in range(1, chunks - 1):
        key_value(i)
    span = QB + 2 * WINDOW
    row_id = lax.broadcasted_iota(jnp.int32, (QB, span), 0)
    col_id = lax.broadcasted_iota(jnp.int32, (QB, span), 1)

    def attend(b):
        context = kv[pl.ds(pl.multiple_of(b * QB, QB), span), :]
        scores = lax.dot_general(
            qs[b], context, (((1,), (1,)), ((), ())), preferred_element_type=jnp.float32
        )
        start = offset + b * QB
        lowest = jnp.maximum(row_id, WINDOW - start)
        highest_col = jnp.minimum(row_id + 2 * WINDOW, total_rows - 1 - start + WINDOW)
        valid = (col_id >= lowest) & (col_id <= highest_col)
        expos = []
        norms = []
        for h in range(local_heads):
            part = jnp.where(valid, scores[h * QB:(h + 1) * QB], NEG_BIG)
            top = jnp.maximum(jnp.max(part, axis=1, keepdims=True), sink_v[h])
            expo = jnp.exp(part - top)
            norms.append(1.0 / (jnp.sum(expo, axis=1, keepdims=True) + jnp.exp(sink_v[h] - top)))
            expos.append(expo.astype(jnp.bfloat16))
        result = jnp.dot(jnp.concatenate(expos, axis=0), context, preferred_element_type=jnp.float32)
        heads = [result[h * QB:(h + 1) * QB] * norms[h] for h in range(local_heads)]
        return [
            jnp.where(low_half, pltpu.roll(heads[2 * g], HEAD, 1), heads[2 * g + 1]).astype(jnp.bfloat16)
            for g in range(groups)
        ]


    def attend_other(i, carry):
        @pl.when(i == hb - 1)
        def _():
            halo_wait(halo_kv)
        b = jnp.where(t == 0, hb + i, hb - 1 - i)
        n = b - cross * hb
        at = pl.multiple_of(n * QB, QB)
        for g, value in enumerate(attend(b)):
            att_send[pl.ds(at, QB), g * LANES:(g + 1) * LANES] = value
        ex_att(n).start()

        @pl.when(i == 0)
        def _():
            poll("w10r", 1)

        @pl.when(i == 1)
        def _():
            poll("w01", 0)

        return carry

    def attend_own(i, carry):
        b = jnp.where(t == 0, hb - 1 - i, hb + i)
        at = pl.multiple_of((b - t * hb) * QB, QB)
        for g, value in enumerate(attend(b)):
            joined[t, pl.ds(at, QB), g * LANES:(g + 1) * LANES] = value

        @pl.when(i == 2)
        def _():
            poll("w00", *range(3, Z))

        @pl.when(i == jnp.where((z == 0) | (z == Z - 1), 3, 2))
        def _():
            poll("w11", 2)
        return carry

    lax.fori_loop(0, hb, attend_other, 0)
    lax.fori_loop(0, hb, attend_own, 0)
    whole_pool = remote(pool_send, joined.at[T + cross], ex_send.at[0], ex_recv.at[0], s, cross)
    whole_att = remote(att_send, joined.at[cross], ex_send.at[1], ex_recv.at[1], s, cross)
    whole_pool.wait_recv()

    def columns(n, half, start, count):
        at = pl.ds(pl.multiple_of(start, wide), count)
        return jnp.concatenate([wfull[2 * n, half, at, :], wfull[2 * n + 1, half, at, :]], axis=1)

    at_rim = (z == 0) | (z == Z - 1)

    def near():
        poll("w01r", 1)
        poll("w11r", 1)

    def second():
        poll("w01", 2)
        poll("w10", 2)

    def pair_of(p):
        q = jnp.where(at_rim & ((p == 1) | (p == 2)), 3 - p, p)
        zz = sum(((z // bit + q // bit) % 2) * bit for bit in [2 ** k for k in range(Z.bit_length() - 1)])
        return [zz * 2 + y, zz * 2 + 1 - y]

    def pair_wait(pair):
        some = wfull.at[pl.ds(0, 2)]
        remote(some, some, wo_send.at[2], wp_recv.at[pair[0] // 2], partner, t).wait_recv()

    def pair_columns(pair, half, start, count):
        return jnp.concatenate([columns(n, half, start, count) for n in pair], axis=1)

    def store(n, total):
        out[:, pl.ds(pl.multiple_of(n * 2 * LANES, 2 * LANES), 2 * LANES)] = total.astype(jnp.bfloat16)

    def most(p, carry):
        @pl.when(p == 1)
        def _():
            pl.when(at_rim)(second)
            pl.when(jnp.logical_not(at_rim))(near)
        pair = pair_of(p)
        pair_wait(pair)
        left = jnp.concatenate([joined[t]] + [joined[T + k] for k in range(T)], axis=1)
        right = jnp.concatenate([pair_columns(pair, 0, t * wide, wide), pair_columns(pair, 1, 0, T * wide)], axis=0)
        total = jnp.dot(left, right, preferred_element_type=jnp.float32)
        acc[pair[0]] = total[:, :2 * LANES]
        acc[pair[1]] = total[:, 2 * LANES:]
        return carry

    def last(p, carry):
        pair = pair_of(p)
        total = jnp.dot(
            joined[cross], pair_columns(pair, 0, cross * wide, wide), preferred_element_type=jnp.float32
        )
        store(pair[0], acc[pair[0]] + total[:, :2 * LANES])
        store(pair[1], acc[pair[1]] + total[:, 2 * LANES:])
        return carry

    def whole(p, carry):
        @pl.when(p == split)
        def _():
            poll("w10", 1)
            poll("w11", 1)
            poll("w01", 1)
            poll("w01", *range(3, Z))
            poll("w10", *range(3, Z))
            poll("w11", *range(3, Z))
        pair = pair_of(p)
        pair_wait(pair)
        left = jnp.concatenate([joined[k] for k in range(2 * T)], axis=1)
        right = jnp.concatenate([pair_columns(pair, half, 0, T * wide) for half in range(T)], axis=0)
        total = jnp.dot(left, right, preferred_element_type=jnp.float32)
        store(pair[0], total[:, :2 * LANES])
        store(pair[1], total[:, 2 * LANES:])
        return carry

    split = Z // 2
    lax.fori_loop(0, split, most, 0)
    pl.when(at_rim)(near)
    pl.when(jnp.logical_not(at_rim))(second)
    whole_att.wait_recv()
    lax.fori_loop(0, split, last, 0)
    lax.fori_loop(split, Z, whole, 0)

    def sent(ref, sem):
        remote(ref, ref, sem, halo_recv.at[0], partner, t).wait_send()

    for cond, make in halo_tok + halo_kv:
        @pl.when(cond)
        def _(make=make):
            make().wait_send()
    whole_pool.wait_send()
    whole_att.wait_send()
    sent(kvw.at[pl.ds(0, 4 * Z - 1)], kv_send.at[0])
    sent(wfull.at[s], wo_send.at[2])
    sent(wfull.at[pl.ds(0, 3 * Z - 1)], wo_send.at[0])
    for at in range(Z):
        inside = lambda k: 0 <= k < Z
        edge = (0, Z - 1)
        count = sum(inside(at + h) for h in hop)
        count += sum(inside(at + h) and (abs(h) > 1 or inside(at + 2 * h)) for h in hop)
        count += 2 * sum(inside(at + d) and inside(at - d // abs(d)) for d in far if 2 <= abs(d) < Z - 1)
        for h in (1, -1):
            if inside(at + h):
                count += (at in edge or at + h in edge) + (at in edge)

        @pl.when(z == at)
        def _(count=count):
            sent(wfull.at[pl.ds(0, count // 2)], wo_send.at[1])


def body(mesh, tokens, norm_gain, w_query, w_key, w_value, w_pool_in, sink_logit, pool_scale, w_out):
    S = lax.axis_size("sp")
    T = lax.axis_size("tp")
    rows, width = tokens.shape
    local_heads = w_query.shape[1] // HEAD
    fits = (
        S % 4 == 0 and S > 4 and S & (S - 1) == 0 and T == 2
        and w_out.shape[1] == LANES and w_key.shape == (LANES, LANES) and w_value.shape == w_key.shape
        and w_query.shape[1] % LANES == 0 and w_pool_in.shape[1] % LANES == 0
        and w_query.shape[1] == w_pool_in.shape[1]
        and local_heads == QH // KVH and rows % (2 * CHUNK) == 0
        and width == S * LANES and LANES % S == 0
    )
    if not fits:
        return plain_body(
            tokens, norm_gain, w_query, w_key, w_value, w_pool_in, sink_logit, pool_scale, w_out
        )
    tables = rope_tables(S * rows)
    blocks = rows // QB
    half = rows // T
    Z = S // 4
    reach = POOL_SPANS[-1] // 2
    wide = w_query.shape[1]
    vmem = pl.BlockSpec(memory_space=pltpu.VMEM)
    hbm = pl.BlockSpec(memory_space=pltpu.HBM)
    dma = pltpu.SemaphoreType.DMA
    bf = jnp.bfloat16
    return pl.pallas_call(
        functools.partial(mixer_kernel, (S, T)),
        out_shape=pltpu.VMEM((half, S * w_out.shape[1]), bf),
        in_specs=[hbm] * 13,
        out_specs=vmem,
        scratch_shapes=[
            pltpu.VMEM((2, reach, width), bf),
            pltpu.VMEM((width // LANES, LANES), jnp.float32),
            pltpu.VMEM((1, wide), jnp.float32),
            pltpu.SMEM(sink_logit.shape, jnp.float32),
            pltpu.VMEM((QB, LANES), jnp.float32),
            pltpu.VMEM((QB, LANES), jnp.float32),
            pltpu.VMEM((rows, width), bf),
            pltpu.VMEM(w_query.shape, bf),
            pltpu.VMEM(w_pool_in.shape, bf),
            pltpu.VMEM((width, 2 * wide), bf),
            pltpu.VMEM((rows, LANES), jnp.float32),
            pltpu.VMEM((rows, LANES), jnp.float32),
            pltpu.VMEM((2,) + w_key.shape, bf),
            pltpu.VMEM((S, LANES, LANES), bf),
            pltpu.VMEM((S, T) + w_out.shape, bf),
            pltpu.VMEM((blocks, local_heads * QB, LANES), bf),
            pltpu.VMEM((rows + 2 * WINDOW, LANES), bf),
            pltpu.VMEM((rows + 2 * reach, wide), jnp.float32),
            pltpu.VMEM((half, wide), bf),
            pltpu.VMEM((half, wide), bf),
            pltpu.VMEM((2 * T, half, wide), bf),
            pltpu.VMEM((S // 2, half, 2 * LANES), jnp.float32),
            pltpu.VMEM((blocks, LANES), jnp.float32),
            pltpu.VMEM((blocks, LANES), jnp.float32),
            dma((rows // CHUNK,)),
            dma((12,)),
            dma((1,)),
            dma((3,)),
            dma((3,)),
            dma((S // 2, T)),
            dma((Z,)),
            dma((4,)),
            dma((4,)),
            dma((2,)),
            dma((2,)),
        ],
        compiler_params=pltpu.CompilerParams(
            collective_id=0, has_side_effects=True, vmem_limit_bytes=VMEM_LIMIT
        ),
    )(
        tokens, norm_gain.reshape(width // LANES, LANES), w_query, w_key, w_value, w_pool_in, sink_logit, pool_scale[None, :], w_out, *tables
    )


def solution(mesh):
    in_specs = (
        P("sp", None),
        P(),
        P(None, "tp"),
        P("sp", None),
        P("sp", None),
        P(None, "tp"),
        P("tp"),
        P("tp"),
        P("tp", "sp"),
    )
    out_specs = P(("sp", "tp"), None)
    return jax.shard_map(functools.partial(body, mesh), mesh=mesh, in_specs=in_specs, out_specs=out_specs, check_vma=False)
```

```python
import functools

import jax
import jax.numpy as jnp
import numpy as np
from jax import lax
from jax.experimental import pallas as pl
from jax.experimental.pallas import tpu as pltpu
from jax.sharding import PartitionSpec as P

HEAD = 64
QH = 8
KVH = 2
POOL_CH = 128
WINDOW = 128
QB = 128


NEG_BIG = -1e30
POOL_SPANS = (2, 4, 8, 16)


def extended(block, sides, width):
    for axis, dim in sides:
        count = lax.axis_size(axis)
        forward = [(i, i + 1) for i in range(count - 1)]
        backward = [(target, source) for source, target in forward]
        low = lax.ppermute(
            lax.slice_in_dim(block, block.shape[dim] - width, None, axis=dim), axis, forward
        )
        high = lax.ppermute(lax.slice_in_dim(block, 0, width, axis=dim), axis, backward)
        block = jnp.concatenate([low, block, high], axis=dim)
    return block


def layer_normed(tokens, norm_gain):
    values = tokens.astype(jnp.float32)
    center = jnp.mean(values, axis=-1, keepdims=True)
    spread = jnp.mean(jnp.square(values - center), axis=-1, keepdims=True)
    return ((values - center) * lax.rsqrt(spread + 1e-06) * norm_gain).astype(jnp.bfloat16)


def rotate(values, positions):
    half = HEAD // 2
    inverse = 10000.0 ** (-jnp.arange(half, dtype=jnp.float32) / half)
    angles = positions[:, None] * inverse[None, :]
    cosine = jnp.cos(angles)[:, None, :]
    sine = jnp.sin(angles)[:, None, :]
    first = values[..., :half]
    second = values[..., half:]
    return jnp.concatenate(
        [first * cosine - second * sine, first * sine + second * cosine], axis=-1
    )


def plain_body(tokens, norm_gain, w_query, w_key, w_value, w_pool_in, sink_logit, pool_scale, w_out):
    local_rows = tokens.shape[0]
    seq_total = local_rows * lax.axis_size("sp")
    offset = lax.axis_index("sp") * local_rows
    tp_place = lax.axis_index("tp")
    local_heads = w_query.shape[1] // HEAD
    local_pool = w_pool_in.shape[1]
    reach = POOL_SPANS[-1] // 2
    normed = layer_normed(tokens, norm_gain)
    positions = (offset + jnp.arange(local_rows)).astype(jnp.float32)
    query = rotate(
        jnp.dot(normed, w_query, preferred_element_type=jnp.float32).reshape(
            local_rows, local_heads, HEAD
        ),
        positions,
    ).astype(jnp.bfloat16)
    key_head = tp_place * local_heads // (QH // KVH)
    key_cols = lax.dynamic_slice_in_dim(w_key, key_head * HEAD, HEAD, 1)
    value_cols = lax.dynamic_slice_in_dim(w_value, key_head * HEAD, HEAD, 1)
    key_sum = jnp.dot(
        normed,
        lax.all_gather(key_cols, "sp", axis=0, tiled=True),
        preferred_element_type=jnp.float32,
    )
    value_sum = jnp.dot(
        normed,
        lax.all_gather(value_cols, "sp", axis=0, tiled=True),
        preferred_element_type=jnp.float32,
    )
    key = rotate(key_sum[:, None, :], positions)[:, 0, :].astype(jnp.bfloat16)
    value = value_sum.astype(jnp.bfloat16)
    key_value = jnp.concatenate([key, value], axis=1)
    pool_in = jnp.dot(normed, w_pool_in, preferred_element_type=jnp.float32).astype(jnp.bfloat16)
    widened = extended(jnp.concatenate([key_value, pool_in], axis=1), (("sp", 0),), WINDOW)
    kv_wide = widened[:, : 2 * HEAD]
    pool_wide = widened[WINDOW - reach : WINDOW + local_rows + reach, 2 * HEAD :]
    span = QB + 2 * WINDOW
    sink_here = sink_logit[:, None, None]
    results = []
    for block in range(local_rows // QB):
        queries = query[block * QB : (block + 1) * QB]
        keys = kv_wide[block * QB : block * QB + span, :HEAD]
        values = kv_wide[block * QB : block * QB + span, HEAD:]
        scores = jnp.einsum(
            "ihd,jd->hij", queries, keys, preferred_element_type=jnp.float32
        ) * HEAD ** (-0.5)
        query_pos = offset + block * QB + jnp.arange(QB)
        key_pos = offset + block * QB - WINDOW + jnp.arange(span)
        valid = (
            (jnp.abs(query_pos[:, None] - key_pos[None, :]) <= WINDOW)
            & (key_pos[None, :] >= 0)
            & (key_pos[None, :] < seq_total)
        )
        scores = jnp.where(valid, scores, NEG_BIG)
        highest = jnp.maximum(jnp.max(scores, axis=-1, keepdims=True), sink_here)
        expo = jnp.where(valid, jnp.exp(scores - highest), 0.0)
        total = jnp.sum(expo, axis=-1, keepdims=True) + jnp.exp(sink_here - highest)
        weights = (expo / total).astype(jnp.bfloat16)
        result = jnp.einsum("hij,jd->ihd", weights, values, preferred_element_type=jnp.float32)
        results.append(result.reshape(QB, local_heads * HEAD).astype(jnp.bfloat16))
    attended = jnp.concatenate(results, axis=0)
    pool_vals = pool_wide.astype(jnp.float32)
    window_sum = pool_vals
    global_pos = offset + jnp.arange(local_rows)
    channel = tp_place * local_pool + jnp.arange(local_pool)
    window_group = channel // POOL_CH
    measured = jnp.zeros((local_rows, local_pool), jnp.float32)
    stride = 1
    for index, width in enumerate(POOL_SPANS):
        window_sum = window_sum[:-stride] + window_sum[stride:]
        stride = width
        sums = window_sum[reach - width // 2 : reach - width // 2 + local_rows]
        counted = (
            jnp.minimum(global_pos + width // 2, seq_total)
            - jnp.maximum(global_pos - width // 2, 0)
        ).astype(jnp.float32)
        measured = measured + jnp.where(
            window_group[None, :] == index, sums / counted[:, None], 0.0
        )
    pooled = ((measured - pool_vals[reach : reach + local_rows]) * pool_scale).astype(jnp.bfloat16)
    attended_rows, pooled_rows = (
        lax.all_to_all(attended, "tp", split_axis=0, concat_axis=1, tiled=True),
        lax.all_to_all(pooled, "tp", split_axis=0, concat_axis=1, tiled=True),
    )
    joined = jnp.concatenate([attended_rows, pooled_rows], axis=1)
    out_rows_all = lax.all_gather(w_out, "tp", axis=0, tiled=True)
    projected = jnp.dot(
        joined,
        lax.all_gather(out_rows_all, "sp", axis=1, tiled=True),
        preferred_element_type=jnp.float32,
    )
    return projected.astype(jnp.bfloat16)


LANES = 128
CHUNK = 256
VMEM_LIMIT = 60 * 1024 * 1024
MESH = pl.DeviceIdType.MESH


def rope_tables(rows_total):
    half = HEAD // 2
    inverse = np.tile(10000.0 ** (-np.arange(half, dtype=np.float64) / half), LANES // half)[None, :]
    sign = np.where(np.arange(LANES) % HEAD < half, -1.0, 1.0)[None, :]
    inner = np.arange(QB, dtype=np.float64)[:, None] * inverse
    starts = (QB * np.arange(rows_total // QB, dtype=np.float64))[:, None] * inverse
    tables = (np.cos(inner), np.sin(inner) * sign, np.cos(starts), np.sin(starts) * sign)
    return [jnp.asarray(table.astype(np.float32)) for table in tables]


def mixer_kernel(
    places, tokens, gain, w_query, w_key, w_value, w_pool, sink, scale, w_out, cos_in, sin_in, cos_all, sin_all,
    out,
    tok_halo, gain_v, scale_v, sink_v, cos_v, sin_v, tok, wq, wp, wqp, scale_at, shift_at, kv_in, kvw, wfull, qs, kv, pool, pool_send, att_send, joined, acc, cos_at, sin_at,
    tok_sem, own_sem, kv_send, kv_recv, wo_send, wo_recv, wp_recv, halo_send, halo_recv, ex_send, ex_recv,
):
    S, T = places
    Z = S // 4
    s = lax.axis_index("sp")
    t = lax.axis_index("tp")
    rows = tokens.shape[0]
    width = tokens.shape[1]
    blocks = rows // QB
    hb = blocks // 2
    chunks = rows // CHUNK
    local_heads = w_query.shape[1] // HEAD
    groups = w_query.shape[1] // LANES
    pgroups = w_pool.shape[1] // LANES
    reach = POOL_SPANS[-1] // 2
    offset = s * rows
    total_rows = S * rows
    c = s % 2
    y = (s // 2) % 2
    z = s // 4
    partner = s + 1 - 2 * c
    yflip = s + 2 - 4 * y
    after = (s + 1) % S
    before = (s + S - 1) % S
    cross = 1 - t
    far = [d for k in range(1, Z) for d in (k, -k)]

    def remote(a, b, send, recv, to_s, to_t):
        return pltpu.make_async_remote_copy(
            src_ref=a, dst_ref=b, send_sem=send, recv_sem=recv,
            device_id={"sp": to_s, "tp": to_t}, device_id_type=MESH,
        )

    def chunk_at(i):
        return pl.multiple_of(jnp.where(t == 0, chunks - 1 - i, i) * CHUNK, CHUNK)

    def tok_copy(i):
        at = pl.ds(chunk_at(i), CHUNK)
        return pltpu.make_async_copy(tokens.at[at], tok.at[at], tok_sem.at[i])

    own_copies = [
        pltpu.make_async_copy(gain, gain_v, own_sem.at[7]),
        pltpu.make_async_copy(w_key, kv_in.at[0], own_sem.at[0]),
        pltpu.make_async_copy(w_value, kv_in.at[1], own_sem.at[1]),
        pltpu.make_async_copy(w_out, wfull.at[s, t], own_sem.at[2]),
        pltpu.make_async_copy(w_query, wq, own_sem.at[3]),
        pltpu.make_async_copy(w_pool, wp, own_sem.at[4]),
        pltpu.make_async_copy(cos_all.at[pl.ds(pl.multiple_of(s * blocks, blocks), blocks)], cos_at, own_sem.at[5]),
        pltpu.make_async_copy(sin_all.at[pl.ds(pl.multiple_of(s * blocks, blocks), blocks)], sin_at, own_sem.at[6]),
        pltpu.make_async_copy(cos_in, cos_v, own_sem.at[8]),
        pltpu.make_async_copy(sin_in, sin_v, own_sem.at[9]),
        pltpu.make_async_copy(scale, scale_v, own_sem.at[10]),
        pltpu.make_async_copy(sink, sink_v, own_sem.at[11]),
    ]
    barrier = pltpu.get_barrier_semaphore()
    greet = [(((z + d) % Z) * 4 + s % 4, t) for d in range(1, Z)]
    greet += [(yflip, t), (after, t), (before, t), (s, cross)]
    for to_s, to_t in greet:
        pl.semaphore_signal(barrier, inc=1, device_id={"sp": to_s, "tp": to_t}, device_id_type=MESH)
    for copy in own_copies[:6]:
        copy.start()
    tok_copy(0).start()
    for copy in own_copies[6:]:
        copy.start()
    for i in range(1, chunks):
        tok_copy(i).start()

    lane = lax.broadcasted_iota(jnp.int32, (QB, LANES), 1)
    low_half = lane < HEAD
    first_half = lane % HEAD < HEAD // 2

    own_copies[0].wait()
    gains = jnp.transpose(jnp.concatenate([gain_v[...]] * (LANES // gain.shape[0]), axis=0))

    def gain_column(b):
        return pltpu.roll(gains, (LANES - b) % LANES, 1)[:, :1]

    own_copies[1].wait()
    own_copies[2].wait()
    key_head = t * local_heads // (QH // KVH)
    key_in = kv_in[0].astype(jnp.float32)
    value_in = kv_in[1].astype(jnp.float32)
    key_cols = jnp.where(key_head == 0, key_in, pltpu.roll(key_in, HEAD, 1))
    value_cols = jnp.where(key_head == 0, pltpu.roll(value_in, HEAD, 1), value_in)
    kvw[s] = (jnp.where(low_half, key_cols, value_cols) * gain_column(s)).astype(jnp.bfloat16)
    own_copies[3].wait()

    def here(d):
        return (z + d >= 0) & (z + d < Z)

    def kv_copy(b, link, to):
        return lambda: remote(kvw.at[b], kvw.at[b], kv_send.at[0], kv_recv.at[link], to, t)

    def kv_wait(link, count):
        some = kvw.at[pl.ds(0, count)]
        remote(some, some, kv_send.at[0], kv_recv.at[link], partner, t).wait_recv()

    def wo_copy(b, half, group, to_s, to_t):
        return lambda: remote(wfull.at[b, half], wfull.at[b, half], wo_send.at[group], wo_recv.at[b // 2, half], to_s, to_t)

    def hand(b, half, group=0):
        return (None, lambda: remote(
            wfull.at[b, half], wfull.at[b, half], wo_send.at[group], wp_recv.at[b // 4], partner, t))

    hop = [2, -2, 1, -1]

    def at_z(d):
        return s + 4 * d

    def at_yz(d):
        return yflip + 4 * d

    def start_all(items):
        for cond, make in items:
            if cond is None:
                make().start()
            else:
                @pl.when(cond)
                def _(make=make):
                    make().start()

    def event(cond, arrival, items):
        def act():
            def inner():
                if arrival is not None:
                    arrival().wait_recv()
                start_all(items)
            if cond is None:
                inner()
            else:
                pl.when(cond)(inner)
        return act

    def onward(d):
        step = -1 if d > 0 else 1
        return step, here(step)

    ev = {}
    ev["kv_own"] = event(None, None,
        [(here(h), kv_copy(s, 0, at_z(h))) for h in far]
        + [(None, kv_copy(s, 1, yflip)), (None, kv_copy(s, 2, partner))])
    kv_to_y = [(here(d), kv_copy(at_z(d), 1, yflip)) for d in far]
    kv_to_p = [(here(d), kv_copy(at_z(d), 2, partner)) for d in far]
    kv_y_to_p = [(None, kv_copy(yflip, 2, partner))] + [(here(d), kv_copy(at_yz(d), 2, partner)) for d in far]

    ev["wo_own"] = event(None, None,
        [(None, wo_copy(s, t, 2, s, cross)), (z > 0, wo_copy(s, t, 0, yflip, t)), hand(s, t, 2)])
    ev["wo_own_y"] = event(None, None, [(z == 0, wo_copy(s, t, 0, yflip, t))])
    ahead = [(h, here(h) & here(2 * h) if abs(h) == 1 else here(h)) for h in hop if abs(h) < Z]
    ends = [(h, here(h) & jnp.logical_not(here(2 * h))) for h in hop if abs(h) == 1]
    ev["wo_own_z"] = event(None, None, [(ok, wo_copy(s, t, 1, at_z(h), t)) for h, ok in ahead])
    ev["wo_own_end"] = event(None, None, [(ok, wo_copy(s, t, 1, at_z(h), t)) for h, ok in ends])
    def rim(d):
        return here(d) & ((z == 0) | (z == Z - 1) | (z + d == 0) | (z + d == Z - 1))

    ev["wo_x"] = event(None, wo_copy(s, cross, 0, yflip, t),
        [(None, wo_copy(s, cross, 0, yflip, t)), hand(s, cross)]
        + [(rim(h), wo_copy(s, cross, 1, at_z(h), t)) for h in (1, -1)])
    ev["wo_d"] = event(None, wo_copy(yflip, cross, 0, partner, t),
        [(ok, wo_copy(yflip, cross, 1, at_z(h), t)) for h, ok in ahead] + [hand(yflip, cross)])
    def split_event(kind, d, arrival, items, at_rim=(), inner_only=()):
        if abs(d) == 1:
            ev[kind + "r", d] = event(rim(d), arrival, list(at_rim) + items)
            ev[kind, d] = event(here(d) & jnp.logical_not(rim(d)), arrival, list(inner_only) + items)
        else:
            ev[kind, d] = event(None if d == 0 else here(d), arrival, list(inner_only) + items)

    for d in far:
        step, fine = onward(d)
        relay = 2 <= abs(d) < Z - 1
        b = at_z(d)
        to_x = [(None, wo_copy(b, t, 0, s, cross))]
        items = [(None, wo_copy(b, t, 0, yflip, t)), hand(b, t)]
        if relay:
            to_x = [(fine, wo_copy(b, t, 1, at_z(step), t))] + to_x
        split_event("w00", d, wo_copy(b, t, 0, s, cross), items, inner_only=to_x)
        split_event("w10", d, wo_copy(b, cross, 0, partner, t), [hand(b, cross)],
            [((z == 0) | (z == Z - 1), wo_copy(b, cross, 1, yflip, t))])
        b = at_yz(d)
        items = [hand(b, cross)]
        if relay:
            items = [(fine, wo_copy(b, cross, 1, at_z(step), t))] + items
        split_event("w11", d, wo_copy(b, cross, 0, partner, t), items)
    for d in [0] + far:
        b = at_yz(d)
        split_event("w01", d, wo_copy(b, t, 0, partner, t), [hand(b, t)])

    def poll(kind, *distances):
        for k in distances:
            for d in ((k, -k) if k else (0,)):
                if abs(d) < Z:
                    ev[kind, d]()

    inner = s < S - 1
    outer = s > 0
    halo_tok = [
        (inner, lambda: remote(tokens.at[pl.ds(rows - reach, reach)], tok_halo.at[0], halo_send.at[0], halo_recv.at[0], after, t)),
        (outer, lambda: remote(tokens.at[pl.ds(0, reach)], tok_halo.at[1], halo_send.at[1], halo_recv.at[1], before, t)),
    ]
    halo_kv = [
        (inner, lambda: remote(kv.at[pl.ds(rows, WINDOW)], kv.at[pl.ds(0, WINDOW)], halo_send.at[2], halo_recv.at[2], after, t)),
        (outer, lambda: remote(kv.at[pl.ds(WINDOW, WINDOW)], kv.at[pl.ds(rows + WINDOW, WINDOW)], halo_send.at[3], halo_recv.at[3], before, t)),
    ]

    def halo_wait(pair):
        @pl.when(outer)
        def _():
            pair[0][1]().wait_recv()

        @pl.when(inner)
        def _():
            pair[1][1]().wait_recv()

    @pl.when(s == 0)
    def _():
        tok_halo[0] = jnp.zeros((reach, width), jnp.bfloat16)
        kv[0:WINDOW, :] = jnp.zeros((WINDOW, LANES), jnp.bfloat16)

    @pl.when(s == S - 1)
    def _():
        tok_halo[1] = jnp.zeros((reach, width), jnp.bfloat16)
        kv[rows + WINDOW:rows + 2 * WINDOW, :] = jnp.zeros((WINDOW, LANES), jnp.bfloat16)

    def begin():
        pl.semaphore_wait(barrier, len(greet))
        ev["kv_own"]()
        start_all(halo_tok)
        ev["wo_own"]()

    late = z > 0

    @pl.when(late)
    def _():
        begin()

    def rotated(values, b):
        ca = cos_at[pl.ds(b, 1), :]
        sa = sin_at[pl.ds(b, 1), :]
        ci = cos_v[...]
        si = sin_v[...]
        cosine = ca * ci - sa * si
        sine = sa * ci + ca * si
        swapped = jnp.where(
            first_half,
            pltpu.roll(values, LANES - HEAD // 2, 1),
            pltpu.roll(values, HEAD // 2, 1),
        )
        return values * cosine + swapped * sine

    for copy in own_copies[4:6]:
        copy.wait()
    wide = w_query.shape[1]

    def fold(b, carry):
        at = pl.ds(pl.multiple_of(b * LANES, LANES), LANES)
        column = gain_column(b)
        sums = []
        for k, part in enumerate((wq, wp)):
            scaled = (part[at, :].astype(jnp.float32) * column).astype(jnp.bfloat16)
            wqp[at, k * wide:(k + 1) * wide] = scaled
            sums.append(jnp.sum(scaled.astype(jnp.float32).reshape(LANES // 8, 8, wide), axis=0))
        return carry + jnp.concatenate(sums, axis=1)

    folded = lax.fori_loop(0, width // LANES, fold, jnp.zeros((8, 2 * wide), jnp.float32), unroll=2)
    total_qp = jnp.sum(folded, axis=0, keepdims=True)

    for copy in own_copies[6:]:
        copy.wait()
    LN = 16
    hc = chunks // 2

    def pooled(b, g):
        cols = slice(g * LANES, (g + 1) * LANES)
        length = QB + 2 * reach
        values = pool[pl.ds(pl.multiple_of(b * QB, QB), length), cols]
        index = (t * (pgroups * LANES) + g * LANES) // POOL_CH
        running = values
        stride = 1
        picked = jnp.zeros((QB, LANES), jnp.float32)
        wide = 0
        for k, span in enumerate(POOL_SPANS):
            running = running + pltpu.roll(running, length - stride, 0)
            stride = span
            shift = reach - span // 2
            sums = (pltpu.roll(running, length - shift, 0) if shift else running)[:QB]
            picked = jnp.where(index == k, sums, picked)
            wide = jnp.where(index == k, span // 2, wide)
        pos = offset + b * QB + lax.broadcasted_iota(jnp.int32, (QB, LANES), 0)
        counted = (jnp.minimum(pos + wide, total_rows) - jnp.maximum(pos - wide, 0)).astype(jnp.float32)
        return ((picked / counted - values[reach:reach + QB]) * scale_v[:, cols]).astype(jnp.bfloat16)


    def ex_pool(n):
        at = pl.ds(pl.multiple_of(n * QB, QB), QB)
        return remote(pool_send.at[at], joined.at[T + t, at], ex_send.at[0], ex_recv.at[0], s, cross)

    def ex_att(n):
        at = pl.ds(pl.multiple_of(n * QB, QB), QB)
        return remote(att_send.at[at], joined.at[t, at], ex_send.at[1], ex_recv.at[1], s, cross)

    def send_pooled(n):
        for g in range(pgroups):
            pool_send[pl.ds(pl.multiple_of(n * QB, QB), QB), g * LANES:(g + 1) * LANES] = pooled(cross * hb + n, g)
        ex_pool(n).start()

    def moments(rows_in):
        values = rows_in.astype(jnp.float32)
        center = jnp.sum(values, axis=1, keepdims=True) * (1.0 / width)
        moved = values - center
        spread = jnp.sum(moved * moved, axis=1, keepdims=True) * (1.0 / width)
        inverse = lax.rsqrt(spread + 1e-06)
        return inverse, center * inverse

    def project(i, carry):
        base = chunk_at(i)
        tok_copy(i).wait()
        raw = jnp.dot(tok[pl.ds(base, CHUNK), :], wqp[...], preferred_element_type=jnp.float32)
        scales = []
        shifts = []
        for r in range(CHUNK // LN):
            at = pl.ds(pl.multiple_of(base + r * LN, LN), LN)
            inverse, shifted = moments(tok[at, :])
            scales.append(inverse)
            shifts.append(shifted)
        rstd = jnp.broadcast_to(jnp.concatenate(scales, axis=0), (CHUNK, LANES))
        drop = jnp.broadcast_to(jnp.concatenate(shifts, axis=0), (CHUNK, LANES))
        scale_at[pl.ds(base, CHUNK), :] = rstd
        shift_at[pl.ds(base, CHUNK), :] = drop

        def normal(k, g):
            at = slice(k * QB, (k + 1) * QB)
            cols = slice(g * LANES, (g + 1) * LANES)
            return raw[at, cols] * rstd[at] - drop[at] * total_qp[:, cols]

        for k in range(CHUNK // QB):
            b = base // QB + k
            for g in range(groups):
                turned = rotated(normal(k, g), b) * HEAD ** (-0.5)
                qs[b, pl.ds(2 * g * QB, QB), :] = jnp.where(low_half, turned, 0.0).astype(jnp.bfloat16)
                qs[b, pl.ds((2 * g + 1) * QB, QB), :] = jnp.where(
                    low_half, pltpu.roll(turned, HEAD, 1), 0.0
                ).astype(jnp.bfloat16)
            for g in range(pgroups):
                pool[pl.ds(pl.multiple_of(reach + base + k * QB, 8), QB), g * LANES:(g + 1) * LANES] = (
                    normal(k, groups + g).astype(jnp.bfloat16).astype(jnp.float32)
                )

        @pl.when((i == 0) & (z == 0))
        def _():
            begin()

        @pl.when(i == jnp.where(z == 0, 1, 0))
        def _():
            ev["wo_own_z"]()

        @pl.when(i == hc - 1)
        def _():
            for n in range(1, hb - 1):
                send_pooled(n)

        @pl.when(i == hc)
        def _():
            send_pooled(jnp.where(t == 0, 0, hb - 1))
            kv_wait(0, Z - 1)
            start_all(kv_to_y)
            start_all(kv_to_p)
            ev["wo_own_end"]()

        @pl.when(i == jnp.where(z == 0, chunks - 1, hc))
        def _():
            ev["wo_x"]()
            ev["wo_own_y"]()

        return carry

    lax.fori_loop(0, chunks, project, 0)

    halo_wait(halo_tok)
    edge = jnp.concatenate([tok_halo[0], tok_halo[1]], axis=0)
    edge_scale, edge_shift = moments(edge)
    edge_pool = (
        jnp.dot(edge, wqp[:, wide:], preferred_element_type=jnp.float32) * edge_scale - edge_shift * total_qp[:, wide:]
    ).astype(jnp.bfloat16).astype(jnp.float32)
    pool[0:reach, :] = edge_pool[:reach]
    pool[rows + reach:rows + 2 * reach, :] = edge_pool[reach:]

    def pool_own(i, carry):
        n = jnp.where(t == 0, i, hb - 1 - i)
        for g in range(pgroups):
            joined[T + t, pl.ds(pl.multiple_of(n * QB, QB), QB), g * LANES:(g + 1) * LANES] = pooled(t * hb + n, g)
        return carry

    send_pooled(jnp.where(t == 0, hb - 1, 0))
    lax.fori_loop(0, hb, pool_own, 0)
    kv_wait(1, Z)
    start_all(kv_y_to_p)
    kv_wait(2, 2 * Z)

    def gather_sum(b, carry):
        return carry + jnp.sum(kvw[b].astype(jnp.float32).reshape(LANES // 8, 8, LANES), axis=0)

    total_kv = jnp.sum(
        lax.fori_loop(0, S, gather_sum, jnp.zeros((8, LANES), jnp.float32), unroll=4), axis=0, keepdims=True
    )

    def key_value(i):
        base = i * CHUNK
        both = jnp.dot(
            tok[pl.ds(base, CHUNK), :], kvw[...].reshape(width, LANES), preferred_element_type=jnp.float32
        )
        both = both * scale_at[pl.ds(base, CHUNK), :] - shift_at[pl.ds(base, CHUNK), :] * total_kv
        for k in range(CHUNK // QB):
            piece = both[k * QB:(k + 1) * QB, :]
            turned = rotated(piece, i * (CHUNK // QB) + k)
            kv[pl.ds(WINDOW + base + k * QB, QB), :] = jnp.where(low_half, turned, piece).astype(jnp.bfloat16)

    key_value(0)
    key_value(chunks - 1)
    start_all(halo_kv)
    def early_relays():
        poll("w00", 2)
        ev["wo_d"]()
        poll("w00r", 1)
        poll("w00", 1)

    early_relays()
    for i in range(1, chunks - 1):
        key_value(i)
    span = QB + 2 * WINDOW
    row_id = lax.broadcasted_iota(jnp.int32, (QB, span), 0)
    col_id = lax.broadcasted_iota(jnp.int32, (QB, span), 1)

    def attend(b):
        context = kv[pl.ds(pl.multiple_of(b * QB, QB), span), :]
        scores = lax.dot_general(
            qs[b], context, (((1,), (1,)), ((), ())), preferred_element_type=jnp.float32
        )
        start = offset + b * QB
        lowest = jnp.maximum(row_id, WINDOW - start)
        highest_col = jnp.minimum(row_id + 2 * WINDOW, total_rows - 1 - start + WINDOW)
        valid = (col_id >= lowest) & (col_id <= highest_col)
        expos = []
        norms = []
        for h in range(local_heads):
            part = jnp.where(valid, scores[h * QB:(h + 1) * QB], NEG_BIG)
            top = jnp.maximum(jnp.max(part, axis=1, keepdims=True), sink_v[h])
            expo = jnp.exp(part - top)
            norms.append(1.0 / (jnp.sum(expo, axis=1, keepdims=True) + jnp.exp(sink_v[h] - top)))
            expos.append(expo.astype(jnp.bfloat16))
        result = jnp.dot(jnp.concatenate(expos, axis=0), context, preferred_element_type=jnp.float32)
        heads = [result[h * QB:(h + 1) * QB] * norms[h] for h in range(local_heads)]
        return [
            jnp.where(low_half, pltpu.roll(heads[2 * g], HEAD, 1), heads[2 * g + 1]).astype(jnp.bfloat16)
            for g in range(groups)
        ]


    def attend_other(i, carry):
        @pl.when(i == hb - 1)
        def _():
            halo_wait(halo_kv)
        b = jnp.where(t == 0, hb + i, hb - 1 - i)
        n = b - cross * hb
        at = pl.multiple_of(n * QB, QB)
        for g, value in enumerate(attend(b)):
            att_send[pl.ds(at, QB), g * LANES:(g + 1) * LANES] = value
        ex_att(n).start()

        @pl.when(i == 0)
        def _():
            poll("w10r", 1)

        @pl.when(i == 1)
        def _():
            poll("w01", 0)

        return carry

    def attend_own(i, carry):
        b = jnp.where(t == 0, hb - 1 - i, hb + i)
        at = pl.multiple_of((b - t * hb) * QB, QB)
        for g, value in enumerate(attend(b)):
            joined[t, pl.ds(at, QB), g * LANES:(g + 1) * LANES] = value

        @pl.when(i == 1)
        def _():
            poll("w00", *range(3, Z))

        @pl.when(i == jnp.where((z == 0) | (z == Z - 1), 3, 2))
        def _():
            poll("w11", 2)
        return carry

    lax.fori_loop(0, hb, attend_other, 0)
    lax.fori_loop(0, hb, attend_own, 0)
    whole_pool = remote(pool_send, joined.at[T + cross], ex_send.at[0], ex_recv.at[0], s, cross)
    whole_att = remote(att_send, joined.at[cross], ex_send.at[1], ex_recv.at[1], s, cross)
    whole_pool.wait_recv()

    def columns(n, half, start, count):
        at = pl.ds(pl.multiple_of(start, wide), count)
        return jnp.concatenate([wfull[2 * n, half, at, :], wfull[2 * n + 1, half, at, :]], axis=1)

    at_rim = (z == 0) | (z == Z - 1)

    def near():
        poll("w01r", 1)
        poll("w11r", 1)

    def second():
        poll("w01", 2)
        poll("w10", 2)

    def pair_of(p):
        q = jnp.where(at_rim & ((p == 1) | (p == 2)), 3 - p, p)
        zz = sum(((z // bit + q // bit) % 2) * bit for bit in [2 ** k for k in range(Z.bit_length() - 1)])
        return [zz * 2 + y, zz * 2 + 1 - y]

    def pair_wait(pair):
        some = wfull.at[pl.ds(0, 2)]
        remote(some, some, wo_send.at[2], wp_recv.at[pair[0] // 2], partner, t).wait_recv()

    def pair_columns(pair, half, start, count):
        return jnp.concatenate([columns(n, half, start, count) for n in pair], axis=1)

    def store(n, total):
        out[:, pl.ds(pl.multiple_of(n * 2 * LANES, 2 * LANES), 2 * LANES)] = total.astype(jnp.bfloat16)

    def most(p, carry):
        @pl.when(p == 1)
        def _():
            pl.when(at_rim)(second)
            pl.when(jnp.logical_not(at_rim))(near)
        pair = pair_of(p)
        pair_wait(pair)
        left = jnp.concatenate([joined[t]] + [joined[T + k] for k in range(T)], axis=1)
        right = jnp.concatenate([pair_columns(pair, 0, t * wide, wide), pair_columns(pair, 1, 0, T * wide)], axis=0)
        total = jnp.dot(left, right, preferred_element_type=jnp.float32)
        acc[pair[0]] = total[:, :2 * LANES]
        acc[pair[1]] = total[:, 2 * LANES:]
        return carry

    def last(p, carry):
        pair = pair_of(p)
        total = jnp.dot(
            joined[cross], pair_columns(pair, 0, cross * wide, wide), preferred_element_type=jnp.float32
        )
        store(pair[0], acc[pair[0]] + total[:, :2 * LANES])
        store(pair[1], acc[pair[1]] + total[:, 2 * LANES:])
        return carry

    def whole(p, carry):
        @pl.when(p == split)
        def _():
            poll("w10", 1)
            poll("w11", 1)
            poll("w01", 1)
            poll("w01", *range(3, Z))
            poll("w10", *range(3, Z))
            poll("w11", *range(3, Z))
        pair = pair_of(p)
        pair_wait(pair)
        left = jnp.concatenate([joined[k] for k in range(2 * T)], axis=1)
        right = jnp.concatenate([pair_columns(pair, half, 0, T * wide) for half in range(T)], axis=0)
        total = jnp.dot(left, right, preferred_element_type=jnp.float32)
        store(pair[0], total[:, :2 * LANES])
        store(pair[1], total[:, 2 * LANES:])
        return carry

    split = Z // 2
    lax.fori_loop(0, split, most, 0)
    pl.when(at_rim)(near)
    pl.when(jnp.logical_not(at_rim))(second)
    whole_att.wait_recv()
    lax.fori_loop(0, split, last, 0)
    lax.fori_loop(split, Z, whole, 0)

    def sent(ref, sem):
        remote(ref, ref, sem, halo_recv.at[0], partner, t).wait_send()

    for cond, make in halo_tok + halo_kv:
        @pl.when(cond)
        def _(make=make):
            make().wait_send()
    whole_pool.wait_send()
    whole_att.wait_send()
    sent(kvw.at[pl.ds(0, 4 * Z - 1)], kv_send.at[0])
    sent(wfull.at[s], wo_send.at[2])
    sent(wfull.at[pl.ds(0, 3 * Z - 1)], wo_send.at[0])
    for at in range(Z):
        inside = lambda k: 0 <= k < Z
        edge = (0, Z - 1)
        count = sum(inside(at + h) for h in hop)
        count += sum(inside(at + h) and (abs(h) > 1 or inside(at + 2 * h)) for h in hop)
        count += 2 * sum(inside(at + d) and inside(at - d // abs(d)) for d in far if 2 <= abs(d) < Z - 1)
        for h in (1, -1):
            if inside(at + h):
                count += (at in edge or at + h in edge) + (at in edge)

        @pl.when(z == at)
        def _(count=count):
            sent(wfull.at[pl.ds(0, count // 2)], wo_send.at[1])


def body(mesh, tokens, norm_gain, w_query, w_key, w_value, w_pool_in, sink_logit, pool_scale, w_out):
    S = lax.axis_size("sp")
    T = lax.axis_size("tp")
    rows, width = tokens.shape
    local_heads = w_query.shape[1] // HEAD
    fits = (
        S % 4 == 0 and S > 4 and S & (S - 1) == 0 and T == 2
        and w_out.shape[1] == LANES and w_key.shape == (LANES, LANES) and w_value.shape == w_key.shape
        and w_query.shape[1] % LANES == 0 and w_pool_in.shape[1] % LANES == 0
        and w_query.shape[1] == w_pool_in.shape[1]
        and local_heads == QH // KVH and rows % (2 * CHUNK) == 0
        and width == S * LANES and LANES % S == 0
    )
    if not fits:
        return plain_body(
            tokens, norm_gain, w_query, w_key, w_value, w_pool_in, sink_logit, pool_scale, w_out
        )
    tables = rope_tables(S * rows)
    blocks = rows // QB
    half = rows // T
    Z = S // 4
    reach = POOL_SPANS[-1] // 2
    wide = w_query.shape[1]
    vmem = pl.BlockSpec(memory_space=pltpu.VMEM)
    hbm = pl.BlockSpec(memory_space=pltpu.HBM)
    dma = pltpu.SemaphoreType.DMA
    bf = jnp.bfloat16
    return pl.pallas_call(
        functools.partial(mixer_kernel, (S, T)),
        out_shape=pltpu.VMEM((half, S * w_out.shape[1]), bf),
        in_specs=[hbm] * 13,
        out_specs=vmem,
        scratch_shapes=[
            pltpu.VMEM((2, reach, width), bf),
            pltpu.VMEM((width // LANES, LANES), jnp.float32),
            pltpu.VMEM((1, wide), jnp.float32),
            pltpu.SMEM(sink_logit.shape, jnp.float32),
            pltpu.VMEM((QB, LANES), jnp.float32),
            pltpu.VMEM((QB, LANES), jnp.float32),
            pltpu.VMEM((rows, width), bf),
            pltpu.VMEM(w_query.shape, bf),
            pltpu.VMEM(w_pool_in.shape, bf),
            pltpu.VMEM((width, 2 * wide), bf),
            pltpu.VMEM((rows, LANES), jnp.float32),
            pltpu.VMEM((rows, LANES), jnp.float32),
            pltpu.VMEM((2,) + w_key.shape, bf),
            pltpu.VMEM((S, LANES, LANES), bf),
            pltpu.VMEM((S, T) + w_out.shape, bf),
            pltpu.VMEM((blocks, local_heads * QB, LANES), bf),
            pltpu.VMEM((rows + 2 * WINDOW, LANES), bf),
            pltpu.VMEM((rows + 2 * reach, wide), jnp.float32),
            pltpu.VMEM((half, wide), bf),
            pltpu.VMEM((half, wide), bf),
            pltpu.VMEM((2 * T, half, wide), bf),
            pltpu.VMEM((S // 2, half, 2 * LANES), jnp.float32),
            pltpu.VMEM((blocks, LANES), jnp.float32),
            pltpu.VMEM((blocks, LANES), jnp.float32),
            dma((rows // CHUNK,)),
            dma((12,)),
            dma((1,)),
            dma((3,)),
            dma((3,)),
            dma((S // 2, T)),
            dma((Z,)),
            dma((4,)),
            dma((4,)),
            dma((2,)),
            dma((2,)),
        ],
        compiler_params=pltpu.CompilerParams(
            collective_id=0, has_side_effects=True, vmem_limit_bytes=VMEM_LIMIT
        ),
    )(
        tokens, norm_gain.reshape(width // LANES, LANES), w_query, w_key, w_value, w_pool_in, sink_logit, pool_scale[None, :], w_out, *tables
    )


def solution(mesh):
    in_specs = (
        P("sp", None),
        P(),
        P(None, "tp"),
        P("sp", None),
        P("sp", None),
        P(None, "tp"),
        P("tp"),
        P("tp"),
        P("tp", "sp"),
    )
    out_specs = P(("sp", "tp"), None)
    return jax.shard_map(functools.partial(body, mesh), mesh=mesh, in_specs=in_specs, out_specs=out_specs, check_vma=False)
```
